32 devices in a mesh: sp: 8 (over z, core), tp: 4 (over y, x).
Axes of the slice: x: 2, y: 2, z: 4, core: 2. Of those that a mesh axis runs over, the one named last changes fastest.
Arguments:
- query_rows: bfloat16 [4096, 1024], P('sp', 'tp'), may hold values from -128 to 128
- key_rows: bfloat16 [4096, 1024], P('sp', 'tp'), may hold values from -4 to 4
- value_rows: bfloat16 [4096, 1024], P('sp', 'tp'), may hold values from -6 to 6
- cum_gates: float32 [4096, 16], P('sp', 'tp'), may hold values from -4098 to 0, as said below
- residual: bfloat16 [4096, 2048], P('sp', 'tp'), may hold values from -64 to 64
- output_weight: bfloat16 [1024, 2048], P(None, 'tp'), may hold values from -0.1875 to 0.1875
- norm_gain: bfloat16 [2048], replicated, may hold values from 0.099609375 to 1.8984375
- expert_index: int32 [4096, 2], P('sp'), may hold values from 0 to 7, all different within a row; in each aligned block of 512 rows (0 to 511, 512 to 1023, ...) at most 256 rows name the same one
- route_weights: float32 [4096, 2], P('sp'), may hold values from 0.2 to 1
- gate_weight: bfloat16 [8, 2048, 2048], P('sp', None, 'tp'), may hold values from -2 to 2
- up_weight: bfloat16 [8, 2048, 2048], P('sp', None, 'tp'), may hold values from -2 to 2
- down_weight: bfloat16 [8, 2048, 2048], P('sp', None, 'tp'), may hold values from -0.125 to 0.125
Outputs:
- layer_out: bfloat16 [4096, 2048], P('sp', 'tp')
The draws below stay inside these ranges and needn't reach their ends.
Inputs may be any that keep to these rules, and one draw needn't show every extreme that they name: `cum_gates`: each head's values never rise along positions. `expert_index`: each token names 2 different experts. In the 512 tokens of one index of sp no expert is named more than 256 times, and in some index's tokens some expert is named exactly 256 times.
All inputs are finite; a program needn't handle non-finite values.
Results may differ from the reference program's by a relative error of at most 0.01.
Values may be sent and summed in bfloat16 or wider, within the bound.
A program may use at most 64 MiB of HBM per device.

```python
import math
import jax
import jax.numpy as jnp
import numpy as np
from jax import lax

D = 2048
HEAD_TOTAL = 16
HEAD_DIM = 64
ATT = 1024
FF = 2048
EXPERTS = 8
TOPK = 2
ROWS = 512
SEQUENCE_LENGTH = 4096
CAP = 256


def attention_pair(key):
    base = jax.random.fold_in(key, 101)
    first_key, second_key = jax.random.split(base, 2)
    shape = (SEQUENCE_LENGTH, HEAD_TOTAL, HEAD_DIM)
    key_part = jnp.clip(jax.random.normal(first_key, shape, jnp.float32), -4.0, 4.0)
    query_part = jnp.clip(3.0 * jax.random.normal(second_key, shape, jnp.float32), -12.0, 12.0)
    return (query_part.reshape(SEQUENCE_LENGTH, HEAD_TOTAL * HEAD_DIM), key_part.reshape(SEQUENCE_LENGTH, HEAD_TOTAL * HEAD_DIM))


def draw_query_rows(key, part):
    return attention_pair(key)[0].astype(jnp.bfloat16)


def draw_key_rows(key, part):
    return attention_pair(key)[1].astype(jnp.bfloat16)


def draw_cum_gates(key, part):
    base = jax.random.fold_in(key, 202)
    ordering, ranking, texture, token_positions, depths = jax.random.split(base, 5)
    order = jax.random.permutation(ordering, HEAD_TOTAL)
    sluggish_decay = order >= HEAD_TOTAL // 2
    rough = jax.random.uniform(texture, (SEQUENCE_LENGTH, HEAD_TOTAL), jnp.float32, 0.4, 1.6)
    blocks = SEQUENCE_LENGTH // ROWS
    ladder = jax.random.permutation(ranking, blocks).astype(jnp.float32) / max(blocks - 1, 1)
    factor = jnp.repeat(0.5 * 4.0 ** ladder, ROWS)
    rate = jnp.where(sluggish_decay, 0.8 / SEQUENCE_LENGTH, 1.0 / min(40.0, ROWS / 2.0))
    forget_steps = -factor[:, None] * rate[None, :] * rough
    spike_position = jax.random.randint(token_positions, (HEAD_TOTAL, 2), 0, SEQUENCE_LENGTH)
    decay_drops = jax.random.uniform(depths, (HEAD_TOTAL, 2), jnp.float32, math.log(0.5), math.log(0.8))
    head_ordinal = jnp.broadcast_to(jnp.arange(HEAD_TOTAL, dtype=jnp.int32)[:, None], (HEAD_TOTAL, 2))
    spike_events = jnp.zeros((SEQUENCE_LENGTH, HEAD_TOTAL), jnp.float32).at[spike_position, head_ordinal].add(decay_drops * sluggish_decay[:, None].astype(jnp.float32))
    return jnp.cumsum(forget_steps + spike_events, axis=0)


def draw_residual(key, part):
    base = jax.random.fold_in(key, 303)
    values_key = jax.random.fold_in(base, 0)
    place = jnp.arange(D, dtype=jnp.float32) / D - 0.5
    noise = jnp.clip(jax.random.normal(values_key, (SEQUENCE_LENGTH, D), jnp.float32), -6.0, 6.0)
    rising = jnp.exp(math.log(3.0) * place)
    return (noise * rising[None, :]).astype(jnp.bfloat16)


def expert_matrix(key, salt):
    base = jax.random.fold_in(key, salt)
    values_key, column_key = jax.random.split(base, 2)
    shape = (EXPERTS, D, FF)
    noise = jnp.clip(jax.random.normal(values_key, shape, jnp.float32), -6.0, 6.0)
    column = jnp.exp(jax.random.uniform(column_key, (EXPERTS, 1, FF), jnp.float32, 0.0, math.log(3.0)))
    return jnp.clip(noise * column / math.sqrt(D), -2.0, 2.0).astype(jnp.bfloat16)


def draw_gate_weight(key, part):
    return expert_matrix(key, 404)


def draw_up_weight(key, part):
    return expert_matrix(key, 505)


def levels(key, extent, cuts, least, largest):
    factor_of, own = 1.0, jax.random.fold_in(key, 6)
    for position, shards_of in cuts:
        steps = jnp.exp(jax.random.uniform(jax.random.fold_in(own, position), (shards_of,), jnp.float32, least / len(cuts), largest / len(cuts)))
        factor_of = factor_of * jnp.repeat(steps, extent[position] // shards_of).reshape([-1 if axis == position else 1 for axis in range(len(extent))])
    return factor_of


def shared_out(rng, own, number, rows, count, top, most, slope):
    order = jax.random.permutation(rng, count)
    crowded, ordinary = portions_of(count, rows * top, most, slope, True), portions_of(count, rows * top, most, slope, False)
    places = jnp.arange(count)

    def named(lengths, offset_by):
        used = int((lengths > 0).sum())
        fixed = max(1, used // 4)
        passed = fixed + (places - fixed + offset_by * (used - fixed)) % max(1, count - fixed)
        return jnp.zeros((count,), jnp.int32).at[order[jnp.where(places < fixed, places, passed)]].set(jnp.asarray(lengths, jnp.int32))

    lengths = jnp.where(number % 4 == 0, named(crowded, number // 4), named(ordinary, number - number // 4 - 1))
    mixed = jax.random.permutation(jax.random.fold_in(own, 3), count)
    source_of, taker = mixed[0:count // 2 * 2:2], mixed[1:count // 2 * 2:2]
    margin = jnp.minimum(lengths[source_of] - 1, most - lengths[taker]) // 2
    margin = jnp.where((source_of == order[0]) | (taker == order[0]) | (lengths[taker] == 0), 0, jnp.maximum(margin, 0))
    passed = jax.random.randint(jax.random.fold_in(own, 4), (count // 2,), 0, 1 << 20) % (margin + 1)
    lengths = lengths.at[source_of].add(-passed).at[taker].add(passed)
    members = jnp.searchsorted(jnp.cumsum(lengths), jnp.arange(rows * top), side="right").astype(jnp.int32)
    table = members.reshape(top, rows).T
    table = table[jax.random.permutation(jax.random.fold_in(own, 1), rows)]
    offset_by = jax.random.randint(jax.random.fold_in(own, 2), (rows, 1), 0, top)
    return jnp.take_along_axis(table, (jnp.arange(top)[None, :] + offset_by) % top, axis=1)


def portions_of(number_of, total, limit, lean, full):
    portions = [(1 << 20) // math.isqrt(standing ** lean) + 1 for standing in range(1, number_of + 1)]
    largest = limit if full else min(limit, max(-(-total // number_of), total * portions[0] // sum(portions)))
    least = 1 if total - largest >= number_of - 1 else 0
    counts, spare = [largest] + [least] * (number_of - 1), total - largest - least * (number_of - 1)
    while spare > 0:
        free = [i for i in range(1, number_of) if counts[i] < largest] or [i for i in range(1, number_of) if counts[i] < limit]
        mass, budget = sum([portions[i] for i in free]), spare
        for i in free:
            extra = min(limit - counts[i], max(1, budget * portions[i] // mass), spare)
            counts[i] = counts[i] + extra
            spare = spare - extra
    return np.array(counts)


def normal_values(rng, dims, spread, most, pieces=(), held_as=jnp.bfloat16):
    level = levels(rng, dims, pieces, -0.22, 0.18) if pieces else 1.0
    values = jax.random.normal(rng, dims, jnp.float32) * spread * level
    return jnp.minimum(jnp.maximum(values, -most), most).astype(held_as)


def setup_inputs(seed: int = 0) -> dict:
    streams_of = jax.random.split(jax.random.key(seed), 13)
    query_rows = draw_query_rows(jax.random.fold_in(streams_of[12], 71), 0)
    key_rows = draw_key_rows(jax.random.fold_in(streams_of[12], 71), 0)
    value_rows = normal_values(streams_of[2], (SEQUENCE_LENGTH, ATT), 1.0, 6.0, ((0, 8), (1, 4)))
    cum_gates = draw_cum_gates(jax.random.fold_in(streams_of[12], 71), 0)
    residual = draw_residual(jax.random.fold_in(streams_of[12], 71), 0)
    output_weight = normal_values(streams_of[5], (ATT, D), ATT ** -0.5, 0.1875, ((1, 4),))
    norm_gain = jnp.clip(1.0 + 0.18 * jax.random.normal(streams_of[6], (D,), jnp.float32), 0.099609375, 1.8984375).astype(jnp.bfloat16)
    expert_index_keys = jax.random.split(jax.random.fold_in(streams_of[7], 1), SEQUENCE_LENGTH // ROWS)
    expert_index_turns = jax.random.permutation(jax.random.fold_in(streams_of[7], 3), SEQUENCE_LENGTH // ROWS)
    expert_index = jax.vmap(lambda own, number: shared_out(jax.random.fold_in(streams_of[7], 2), own, number, ROWS, EXPERTS, TOPK, CAP, 2))(expert_index_keys, expert_index_turns).reshape((SEQUENCE_LENGTH, TOPK))
    route_weights = jnp.clip(0.2 + 0.8 * jax.random.uniform(streams_of[8], (SEQUENCE_LENGTH, TOPK), jnp.float32) ** levels(streams_of[8], (SEQUENCE_LENGTH, TOPK), ((0, 8),), -0.2, 0.2), 0.2, 1.0)
    gate_weight = draw_gate_weight(jax.random.fold_in(streams_of[12], 71), 0)
    up_weight = draw_up_weight(jax.random.fold_in(streams_of[12], 71), 0)
    down_weight = normal_values(streams_of[11], (EXPERTS, FF, D), FF ** -0.5, 0.125, ((0, 8), (2, 4)))
    return dict(query_rows=query_rows, key_rows=key_rows, value_rows=value_rows, cum_gates=cum_gates, residual=residual, output_weight=output_weight, norm_gain=norm_gain, expert_index=expert_index, route_weights=route_weights, gate_weight=gate_weight, up_weight=up_weight, down_weight=down_weight)


NORM_EPS = 1e-06
CLAMP_LIMIT = 7.0
SILU_ALPHA = 1.702

def attend(query_rows, key_rows, value_rows, cum_gates):
    length = query_rows.shape[0]
    heads = cum_gates.shape[1]
    head_size = query_rows.shape[1] // heads
    queries = query_rows.reshape(length, heads, head_size)
    key_heads = key_rows.reshape(length, heads, head_size).astype(jnp.float32)
    value_heads = value_rows.reshape(length, heads, head_size).astype(jnp.float32)
    block = math.gcd(length, 512)
    positions = jnp.arange(length, dtype=jnp.int32)

    def one_block(number):
        start = number * block
        query_block = lax.dynamic_slice_in_dim(queries, start, block, 0).astype(jnp.float32)
        query_gates = lax.dynamic_slice_in_dim(cum_gates, start, block, 0)
        scores = jnp.einsum('qhd,khd->hqk', query_block, key_heads) * head_size ** (-0.5)
        scores = scores + query_gates.T[:, :, None] - cum_gates.T[:, None, :]
        query_place = start + jnp.arange(block, dtype=jnp.int32)
        allowed = positions[None, :] <= query_place[:, None]
        scores = jnp.where(allowed[None], scores, -jnp.inf)
        top = lax.optimization_barrier(jnp.max(scores, axis=-1, keepdims=True))
        raised = jnp.exp(scores - top)
        total = lax.optimization_barrier(jnp.sum(raised, axis=-1))
        weights = raised.astype(jnp.bfloat16).astype(jnp.float32)
        summed = jnp.einsum('hqk,khd->qhd', weights, value_heads)
        return (summed / total.T[:, :, None]).astype(jnp.bfloat16).reshape(block, heads * head_size)
    return lax.map(one_block, jnp.arange(length // block, dtype=jnp.int32)).reshape(length, heads * head_size)

def expert_rows(rows, gate_part, up_part, down_part):
    gate_input = jnp.dot(rows, gate_part, preferred_element_type=jnp.float32)
    linear_input = jnp.dot(rows, up_part, preferred_element_type=jnp.float32)
    gate_cut = jnp.minimum(gate_input, CLAMP_LIMIT)
    linear_cut = jnp.clip(linear_input, -CLAMP_LIMIT, CLAMP_LIMIT)
    activated = (gate_cut * jax.nn.sigmoid(SILU_ALPHA * gate_cut) * (linear_cut + 1.0)).astype(jnp.bfloat16)
    return jnp.dot(activated, down_part, preferred_element_type=jnp.float32).astype(jnp.bfloat16)

def reference(query_rows, key_rows, value_rows, cum_gates, residual, output_weight, norm_gain, expert_index, route_weights, gate_weight, up_weight, down_weight):
    attended = attend(query_rows, key_rows, value_rows, cum_gates)
    mixed = (residual.astype(jnp.float32) + jnp.dot(attended, output_weight, preferred_element_type=jnp.float32)).astype(jnp.bfloat16)
    wide = mixed.astype(jnp.float32)
    factor = lax.rsqrt(lax.optimization_barrier(jnp.mean(wide * wide, axis=-1, keepdims=True)) + NORM_EPS)
    normed = (wide * factor * norm_gain.astype(jnp.float32)).astype(jnp.bfloat16)
    experts = gate_weight.shape[0]
    blocks = SEQUENCE_LENGTH // ROWS
    chosen = expert_index.reshape(blocks, ROWS * TOPK)
    matches = (chosen[:, :, None] == jnp.arange(experts, dtype=jnp.int32)[None, None, :]).astype(jnp.int32)
    rank = lax.optimization_barrier(jnp.sum((jnp.cumsum(matches, axis=1) - matches) * matches, axis=2))
    slot = jnp.arange(blocks, dtype=jnp.int32)[:, None] * CAP + rank
    owner = jnp.arange(blocks * ROWS * TOPK, dtype=jnp.int32).reshape(blocks, ROWS * TOPK) // TOPK
    table = jnp.full((experts, blocks * CAP), SEQUENCE_LENGTH, jnp.int32).at[chosen, slot].set(owner)
    padded = jnp.concatenate([normed, jnp.zeros((1, D), normed.dtype)], axis=0)

    def one_expert(number):
        rows = padded[table[number]]
        return expert_rows(rows, gate_weight[number], up_weight[number], down_weight[number])
    outputs = lax.map(one_expert, jnp.arange(experts, dtype=jnp.int32))
    picked = outputs[chosen, slot].reshape(SEQUENCE_LENGTH, TOPK, D).astype(jnp.float32)
    blended = lax.optimization_barrier(jnp.sum(route_weights[:, :, None] * picked, axis=1))
    return (mixed.astype(jnp.float32) + blended).astype(jnp.bfloat16)
```

```python
import functools
import math

import jax
import jax.numpy as jnp
from jax import lax
from jax.experimental import pallas as pl
from jax.experimental.pallas import tpu as pltpu
from jax.sharding import PartitionSpec as P

NORM_EPS = 1e-06
CLAMP_LIMIT = 7.0
SILU_ALPHA = 1.702
CHUNKS = 1


def normalize(rows, norm_gain):
    wide = rows.astype(jnp.float32)
    factor = lax.rsqrt(jnp.mean(wide * wide, axis=-1, keepdims=True) + NORM_EPS)
    return (wide * factor * norm_gain.astype(jnp.float32)).astype(jnp.bfloat16)


def attend_kernel(heads, q_ref, kv_ref, gates_ref, out_ref, masked_q, top, total, summed):
    rows, width = q_ref.shape
    head_size = width // heads
    lanes = min(width, 128)
    tile = math.gcd(rows, 256)
    tiles = rows // tile
    me = lax.axis_index("sp")
    scale = head_size ** (-0.5)
    lane = lax.broadcasted_iota(jnp.int32, (rows, lanes), 1)
    for h in range(heads):
        group, inside = divmod(h * head_size, lanes)
        part = q_ref[:, group * lanes : (group + 1) * lanes].astype(jnp.float32) * scale
        keep = (lane >= inside) & (lane < inside + head_size)
        masked_q[h] = jnp.where(keep, part, 0.0).astype(jnp.bfloat16)
    top[...] = jnp.full(top.shape, -1e30, jnp.float32)
    total[...] = jnp.zeros(total.shape, jnp.float32)
    summed[...] = jnp.zeros(summed.shape, jnp.float32)

    def block(number, diagonal):
        base = pl.multiple_of(number * rows, rows)
        for h in range(heads):
            group = h * head_size // lanes
            keys = kv_ref[pl.ds(base, rows), group * lanes : (group + 1) * lanes]
            values = kv_ref[pl.ds(base, rows), width + group * lanes : width + (group + 1) * lanes]
            gates = gates_ref[number, h : h + 1, :]
            for t in range(tiles):
                span = slice(t * tile, (t + 1) * tile)
                count = (t + 1) * tile if diagonal else rows
                scores = lax.dot_general(
                    masked_q[h, span],
                    keys[:count],
                    (((1,), (1,)), ((), ())),
                    preferred_element_type=jnp.float32,
                )
                scores = scores - gates[:, :count]
                if diagonal:
                    row = lax.broadcasted_iota(jnp.int32, (tile, count), 0) + t * tile
                    col = lax.broadcasted_iota(jnp.int32, (tile, count), 1)
                    scores = jnp.where(col <= row, scores, -jnp.inf)
                old = top[h, span]
                new = jnp.maximum(old, jnp.max(scores, axis=1, keepdims=True))
                raised = jnp.exp(scores - new[:, :1])
                shrink = jnp.exp(old - new)
                part = raised[:, :128]
                for c in range(128, count, 128):
                    part = part + raised[:, c : c + 128]
                top[h, span] = new
                total[h, span] = total[h, span] * shrink + part
                product = lax.dot_general(
                    raised.astype(jnp.bfloat16),
                    values[:count],
                    (((1,), (0,)), ((), ())),
                    preferred_element_type=jnp.float32,
                )
                summed[h, span] = summed[h, span] * shrink[:, :lanes] + product

    def step(number, carry):
        block(number, False)
        return carry

    lax.fori_loop(0, me, step, 0)
    block(me, True)
    for g in range(width // lanes):
        result = jnp.zeros((rows, lanes), jnp.float32)
        for h in range(heads):
            if h * head_size // lanes == g:
                inside = h * head_size % lanes
                keep = (lane >= inside) & (lane < inside + head_size)
                whole = jnp.sum(total[h], axis=1, keepdims=True)
                result = jnp.where(keep, summed[h] / whole, result)
        out_ref[:, g * lanes : (g + 1) * lanes] = result.astype(out_ref.dtype)


def attend_local(query_rows, kv_all, gates_all):
    rows, width = query_rows.shape
    groups, heads, _ = gates_all.shape
    lanes = min(width, 128)
    return pl.pallas_call(
        functools.partial(attend_kernel, heads),
        out_shape=jax.ShapeDtypeStruct((rows, width), jnp.bfloat16),
        in_specs=[pl.BlockSpec(memory_space=pltpu.VMEM)] * 3,
        out_specs=pl.BlockSpec(memory_space=pltpu.VMEM),
        scratch_shapes=[
            pltpu.VMEM((heads, rows, lanes), jnp.bfloat16),
            pltpu.VMEM((heads, rows, 128), jnp.float32),
            pltpu.VMEM((heads, rows, 128), jnp.float32),
            pltpu.VMEM((heads, rows, lanes), jnp.float32),
        ],
        compiler_params=pltpu.CompilerParams(vmem_limit_bytes=48 * 2**20),
        cost_estimate=pl.CostEstimate(
            flops=4 * rows * rows * groups * width * 4,
            bytes_accessed=4 * rows * groups * width,
            transcendentals=rows * rows * groups * heads,
        ),
    )(query_rows, kv_all, gates_all)


def half_of(core, tp):
    return (1 - core) * (tp // 2) + core * (tp % 2)


def partner_of(core, tp):
    return (1 - core) * ((tp + 2) % 4) + core * (tp + 1 - 2 * (tp % 2))


def layer_kernel(
    heads,
    groups,
    q_ref,
    k_ref,
    v_ref,
    gates_ref,
    weight_ref,
    residual_ref,
    index_row_ref,
    index_col_ref,
    route_ref,
    gain_ref,
    gate_ref,
    up_ref,
    down_ref,
    out_ref,
    place_row_ref,
    place_col_ref,
    mixed_ref,
    keys_all,
    values_all,
    gates_all,
    masked_q,
    top,
    total,
    summed,
    attended,
    outbox,
    full,
    act,
    made,
    returned,
    blended,
    gate_all,
    up_all,
    down_all,
    wide_rows,
    next_send,
    next_recv,
    side_send,
    side_recv,
    tp_send,
    tp_recv,
    weight_send,
    weight_recv,
    load_sem,
    down_send,
    down_recv,
    out_send,
    out_recv,
    one_send,
    one_recv,
    two_send,
    two_recv,
    back_send,
    back_recv,
):
    rows, width = q_ref.shape
    head_size = width // heads
    lanes = min(width, 128)
    tile = math.gcd(rows, 256)
    tiles = rows // tile
    sp = lax.axis_index("sp")
    tp = lax.axis_index("tp")
    chip = sp // 2
    core = sp % 2
    chips = groups // 2
    sibling = sp + 1 - 2 * core
    beside = tp + 1 - 2 * (tp % 2)
    across = (tp + 2) % 4
    mesh_id = pl.DeviceIdType.MESH
    scale = head_size ** (-0.5)

    def copies(number, own, device, send_sem, recv_sem):
        made = []
        for n, (mine, held) in enumerate(
            ((k_ref, keys_all), (v_ref, values_all), (gates_ref, gates_all))
        ):
            made.append(
                pltpu.make_async_remote_copy(
                    src_ref=mine if own else held.at[number],
                    dst_ref=held.at[number],
                    send_sem=send_sem.at[number, n],
                    recv_sem=recv_sem.at[number, n],
                    device_id=device,
                    device_id_type=mesh_id,
                )
            )
        return made

    def onward(number, own=False):
        return copies(number, own, ((sp + 2) % groups, tp), next_send, next_recv)

    def sideways(number, own=False):
        return copies(number, own, (sibling, tp), side_send, side_recv)

    def direct(which):
        return pltpu.make_async_remote_copy(
            src_ref=attended.at[tp],
            dst_ref=attended.at[tp],
            send_sem=tp_send.at[which],
            recv_sem=tp_recv.at[which],
            device_id=(sp, beside if which == 0 else across),
            device_id_type=mesh_id,
        )

    def relay(which):
        owner = beside if which == 0 else across
        part = attended.at[owner, pl.ds(which * (rows // 2), rows // 2)]
        return pltpu.make_async_remote_copy(
            src_ref=part,
            dst_ref=part,
            send_sem=tp_send.at[2 + which],
            recv_sem=tp_recv.at[2 + which],
            device_id=(sp, across if which == 0 else beside),
            device_id_type=mesh_id,
        )

    topk = route_ref.shape[1]
    half, columns = outbox.shape[2:]
    capacity = 2 * half
    shards = full.shape[1]
    mine = half_of(core, tp)
    pair = partner_of(core, tp)
    peer = partner_of(1 - core, tp)
    owners = (tp, pair, peer, (beside + 2) % 4)

    def partner(number):
        found, bit = 0, 1
        while bit < groups:
            found = found + bit * (((sp // bit) % 2 + (number // bit) % 2) % 2)
            bit *= 2
        return found

    def send(src, dst, send_sem, recv_sem, device):
        return pltpu.make_async_remote_copy(
            src_ref=src,
            dst_ref=dst,
            send_sem=send_sem,
            recv_sem=recv_sem,
            device_id=device,
            device_id_type=pl.DeviceIdType.MESH,
        )

    def dispatch(i, which):
        group = partner(i)
        target = tp if which == 0 else partner_of(group % 2, tp)
        return send(
            outbox.at[i, which],
            full.at[i, which],
            out_send.at[i, which],
            out_recv.at[i, which],
            (group, target),
        )

    def exchange(i, held, send_sem, recv_sem):
        return send(
            held.at[i, pl.ds(0, 2)],
            held.at[i, pl.ds(2, 2)],
            send_sem.at[i],
            recv_sem.at[i],
            (sp, peer),
        )

    def give_back(i, which):
        target = tp if which == 0 else pair
        return send(
            made.at[i, which],
            returned.at[i, mine],
            back_send.at[i, which],
            back_recv.at[i, mine],
            (partner(i), target),
        )

    def arrive_back(i, which):
        return send(
            made.at[i, 0],
            returned.at[i, which],
            back_send.at[i, 0],
            back_recv.at[i, which],
            (sp, pair),
        )

    loads = []
    for n, (src, dst) in enumerate(
        ((gate_ref, gate_all.at[0]), (up_ref, up_all.at[0]), (down_ref, down_all.at[0]))
    ):
        loads.append(pltpu.make_async_copy(src, dst, load_sem.at[n]))
    for load in loads:
        load.start()

    barrier = pltpu.get_barrier_semaphore()
    for i in range(1, groups):
        pl.semaphore_signal(
            barrier, inc=1, device_id=(partner(i), tp), device_id_type=pl.DeviceIdType.MESH
        )
        pl.semaphore_signal(
            barrier,
            inc=1,
            device_id=(partner(i), partner_of(partner(i) % 2, tp)),
            device_id_type=pl.DeviceIdType.MESH,
        )
        pl.semaphore_signal(
            barrier, inc=1, device_id=(partner(i), pair), device_id_type=pl.DeviceIdType.MESH
        )
    for other in (pair, peer):
        pl.semaphore_signal(
            barrier, inc=1, device_id=(sp, other), device_id_type=pl.DeviceIdType.MESH
        )
    pl.semaphore_wait(barrier, 3 * groups - 1)

    down_copy = send(down_ref, down_all.at[1], down_send, down_recv, (sp, pair))

    weight_copies = [
        pltpu.make_async_remote_copy(
            src_ref=src,
            dst_ref=dst,
            send_sem=weight_send.at[n],
            recv_sem=weight_recv.at[n],
            device_id=(sp, pair),
            device_id_type=mesh_id,
        )
        for n, (src, dst) in enumerate(((gate_ref, gate_all.at[1]), (up_ref, up_all.at[1])))
    ]

    @pl.when(chip < chips - 1)
    def _():
        for copy in onward(sp, True):
            copy.start()

    @pl.when(core == 0)
    def _():
        for copy in sideways(sp, True):
            copy.start()

    for copy in weight_copies:
        copy.start()

    first = lax.broadcasted_iota(jnp.int32, (rows, rows), 0)
    second = lax.broadcasted_iota(jnp.int32, (rows, rows), 1)
    number = lax.broadcasted_iota(jnp.int32, (rows, 128), 1)
    named = jnp.zeros((rows, 128), jnp.float32)
    for k in range(topk):
        named = named + jnp.where(number == index_col_ref[:, k : k + 1], 1.0, 0.0)
    before = jnp.dot(
        jnp.where(second < first, 1.0, 0.0).astype(jnp.bfloat16),
        named.astype(jnp.bfloat16),
        preferred_element_type=jnp.float32,
    )
    for k in range(topk):
        expert = index_col_ref[:, k : k + 1]
        rank = jnp.sum(jnp.where(number == expert, before, 0.0), axis=1, keepdims=True)
        place_col_ref[:, k : k + 1] = expert * capacity + rank.astype(jnp.int32)
    number = lax.broadcasted_iota(jnp.int32, (128, rows), 0)
    named = jnp.zeros((128, rows), jnp.float32)
    for k in range(topk):
        named = named + jnp.where(number == index_row_ref[k : k + 1, :], 1.0, 0.0)
    before = jnp.dot(
        named.astype(jnp.bfloat16),
        jnp.where(first < second, 1.0, 0.0).astype(jnp.bfloat16),
        preferred_element_type=jnp.float32,
    )
    for k in range(topk):
        expert = index_row_ref[k : k + 1, :]
        rank = jnp.sum(jnp.where(number == expert, before, 0.0), axis=0, keepdims=True)
        place_row_ref[k : k + 1, :] = expert * capacity + rank.astype(jnp.int32)

    lane = lax.broadcasted_iota(jnp.int32, (rows, lanes), 1)
    for h in range(heads):
        group, inside = divmod(h * head_size, lanes)
        part = q_ref[:, group * lanes : (group + 1) * lanes].astype(jnp.float32) * scale
        keep = (lane >= inside) & (lane < inside + head_size)
        masked_q[h] = jnp.where(keep, part, 0.0).astype(jnp.bfloat16)
    top[...] = jnp.full(top.shape, -1e30, jnp.float32)
    total[...] = jnp.zeros(total.shape, jnp.float32)
    summed[...] = jnp.zeros(summed.shape, jnp.float32)

    def block(key_block, value_block, gate_block, diagonal):
        for h in range(heads):
            group = h * head_size // lanes
            keys = key_block[:, group * lanes : (group + 1) * lanes]
            values = value_block[:, group * lanes : (group + 1) * lanes]
            gates = gate_block[h : h + 1, :]
            for t in range(tiles):
                span = slice(t * tile, (t + 1) * tile)
                count = (t + 1) * tile if diagonal else rows
                scores = lax.dot_general(
                    masked_q[h, span],
                    keys[:count],
                    (((1,), (1,)), ((), ())),
                    preferred_element_type=jnp.float32,
                )
                scores = scores - gates[:, :count]
                if diagonal:
                    row = lax.broadcasted_iota(jnp.int32, (tile, count), 0) + t * tile
                    col = lax.broadcasted_iota(jnp.int32, (tile, count), 1)
                    scores = jnp.where(col <= row, scores, -jnp.inf)
                old = top[h, span]
                new = jnp.maximum(old, jnp.max(scores, axis=1, keepdims=True))
                raised = jnp.exp(scores - new[:, :1])
                shrink = jnp.exp(old - new)
                part = raised[:, :128]
                for c in range(128, count, 128):
                    part = part + raised[:, c : c + 128]
                top[h, span] = new
                total[h, span] = total[h, span] * shrink + part
                product = lax.dot_general(
                    raised.astype(jnp.bfloat16),
                    values[:count],
                    (((1,), (0,)), ((), ())),
                    preferred_element_type=jnp.float32,
                )
                summed[h, span] = summed[h, span] * shrink[:, :lanes] + product

    block(k_ref, v_ref, gates_ref, True)

    def ring_step(d, carry):
        mine = sp - 2 * (d // 2)
        other = sibling - 2 * (d // 2)

        @pl.when((d % 2 == 0) & (d >= 2))
        def _():
            for copy in onward(mine):
                copy.wait_recv()

            @pl.when(chip < chips - 1)
            def _():
                for copy in onward(mine):
                    copy.start()

            for copy in sideways(mine):
                copy.start()

        @pl.when(d % 2 == 1)
        def _():
            for copy in sideways(other):
                copy.wait_recv()

        now = mine * (1 - d % 2) + other * (d % 2)
        block(keys_all.at[now], values_all.at[now], gates_all.at[now], False)
        return carry

    lax.fori_loop(2 - core, 2 * chip + 2, ring_step, 0)

    for g in range(width // lanes):
        result = jnp.zeros((rows, lanes), jnp.float32)
        for h in range(heads):
            if h * head_size // lanes == g:
                inside = h * head_size % lanes
                keep = (lane >= inside) & (lane < inside + head_size)
                whole = jnp.sum(total[h], axis=1, keepdims=True)
                result = jnp.where(keep, summed[h] / whole, result)
        attended[tp, :, g * lanes : (g + 1) * lanes] = result.astype(jnp.bfloat16)
    direct(0).start()
    direct(1).start()
    down_copy.start()

    def projected(owner):
        return jnp.dot(
            attended[owner],
            weight_ref[pl.ds(pl.multiple_of(owner * width, width), width), :],
            preferred_element_type=jnp.float32,
        )

    mixed = residual_ref[...].astype(jnp.float32) + projected(tp)
    for which, owner in ((0, beside), (1, across)):
        direct(which).wait_recv()
        relay(which).start()
        mixed = mixed + projected(owner)
    relay(0).wait_recv()
    relay(1).wait_recv()
    mixed_ref[...] = (mixed + projected((beside + 2) % 4)).astype(mixed_ref.dtype)

    def rows_for(i):
        flip = half_of(partner(i) % 2, tp)
        place = lax.broadcasted_iota(jnp.int32, (capacity, rows), 0) + flip * half
        numbers = jnp.where(place >= capacity, place - capacity, place) + i * capacity
        taken = numbers == place_row_ref[0:1, :]
        for k in range(1, topk):
            taken = taken | (numbers == place_row_ref[k : k + 1, :])
        return jnp.dot(
            jnp.where(taken, 1.0, 0.0).astype(jnp.bfloat16),
            mixed_ref[...],
            preferred_element_type=jnp.float32,
        ).astype(jnp.bfloat16)

    first = rows_for(0)
    full[0, 0] = first[:half]
    outbox[0, 1] = first[half:]
    dispatch(0, 1).start()

    def fill(i, carry):
        made_rows = rows_for(i)
        outbox[i, 0] = made_rows[:half]
        outbox[i, 1] = made_rows[half:]
        dispatch(i, 0).start()
        dispatch(i, 1).start()
        return carry

    lax.fori_loop(1, groups, fill, 0)
    blended[...] = mixed_ref[...].astype(jnp.float32)
    for load in loads:
        load.wait()
    for copy in weight_copies:
        copy.wait_recv()

    def hidden(i):
        square = jnp.zeros((half, 1), jnp.float32)
        for j in range(shards):
            wide = full[i, j].astype(jnp.float32)
            square = square + jnp.sum(wide * wide, axis=1, keepdims=True)
        factor = lax.rsqrt(square / (shards * columns) + NORM_EPS)
        for j in range(shards):
            span = pl.ds(pl.multiple_of(owners[j] * columns, columns), columns)
            gain = gain_ref[0:1, span].astype(jnp.float32)
            wide_rows[:, span] = (full[i, j].astype(jnp.float32) * factor * gain).astype(
                jnp.bfloat16
            )
        for c in range(2):
            gate_input = jnp.dot(
                wide_rows[...], gate_all[c], preferred_element_type=jnp.float32
            )
            linear_input = jnp.dot(wide_rows[...], up_all[c], preferred_element_type=jnp.float32)
            gate_cut = jnp.minimum(gate_input, CLAMP_LIMIT)
            linear_cut = jnp.clip(linear_input, -CLAMP_LIMIT, CLAMP_LIMIT)
            act[i, c] = (
                gate_cut * jax.nn.sigmoid(SILU_ALPHA * gate_cut) * (linear_cut + 1.0)
            ).astype(jnp.bfloat16)

    def output_rows(i, c):
        return jnp.dot(
            wide_rows[...], down_all[c], preferred_element_type=jnp.float32
        ).astype(jnp.bfloat16)

    def step(i, carry):
        @pl.when(i < groups)
        def _():
            @pl.when(i > 0)
            def _():
                dispatch(i, 0).wait_recv()

            dispatch(i, 1).wait_recv()
            exchange(i, full, one_send, one_recv).start()

        @pl.when((i >= 1) & (i < groups + 1))
        def _():
            exchange(i - 1, full, one_send, one_recv).wait_recv()
            hidden(i - 1)
            exchange(i - 1, act, two_send, two_recv).start()

        @pl.when((i >= 2) & (i < groups + 2))
        def _():
            b = i - 2

            @pl.when(b == 0)
            def _():
                down_copy.wait_recv()

            exchange(b, act, two_send, two_recv).wait_recv()
            for j in range(shards):
                span = pl.ds(pl.multiple_of(owners[j] * columns, columns), columns)
                wide_rows[:, span] = act[b, j]
            made[b, 1] = output_rows(b, 1)
            give_back(b, 1).start()
            result = output_rows(b, 0)

            @pl.when(b == 0)
            def _():
                returned[0, mine] = result

            @pl.when(b > 0)
            def _():
                made[b, 0] = result
                give_back(b, 0).start()

        @pl.when(i >= 3)
        def _():
            b = i - 3

            @pl.when(b == 0)
            def _():
                arrive_back(0, 1 - mine).wait_recv()

            @pl.when(b > 0)
            def _():
                arrive_back(b, 0).wait_recv()
                arrive_back(b, 1).wait_recv()

            numbers = lax.broadcasted_iota(jnp.int32, (rows, capacity), 1) + b * capacity
            added = blended[...]
            rows_back = returned[b].reshape(capacity, columns)
            for k in range(topk):
                taken = jnp.where(numbers == place_col_ref[:, k : k + 1], 1.0, 0.0)
                picked = jnp.dot(
                    taken.astype(jnp.bfloat16), rows_back, preferred_element_type=jnp.float32
                )
                added = added + route_ref[:, k : k + 1] * picked
            blended[...] = added

        return carry

    lax.fori_loop(0, groups + 3, step, 0)
    out_ref[...] = blended[...].astype(out_ref.dtype)

    def settle(i, carry):
        @pl.when(i > 0)
        def _():
            dispatch(i, 0).wait_send()
            give_back(i, 0).wait_send()

        dispatch(i, 1).wait_send()
        give_back(i, 1).wait_send()
        exchange(i, full, one_send, one_recv).wait_send()
        exchange(i, act, two_send, two_recv).wait_send()
        return carry

    lax.fori_loop(0, groups, settle, 0)
    down_copy.wait_send()

    for which in range(2):
        direct(which).wait_send()
        relay(which).wait_send()

    @pl.when(chip < chips - 1)
    def _():
        for copy in onward(sp, True):
            copy.wait_send()

    @pl.when(core == 0)
    def _():
        for copy in sideways(sp, True):
            copy.wait_send()

    def settle_ring(d, carry):
        @pl.when(chip < chips - 1)
        def _():
            for copy in onward(sp - 2 * d):
                copy.wait_send()

        for copy in sideways(sp - 2 * d):
            copy.wait_send()
        return carry

    lax.fori_loop(1, chip + 1, settle_ring, 0)
    for copy in weight_copies:
        copy.wait_send()


def layer_fused(
    query_rows,
    key_rows,
    value_rows,
    gates,
    output_weight,
    residual,
    index,
    route_weights,
    norm_gain,
    gate_weight,
    up_weight,
    down_weight,
    capacity,
):
    rows, width = query_rows.shape
    columns = residual.shape[1]
    heads = gates.shape[0]
    groups = lax.axis_size("sp")
    shards = lax.axis_size("tp")
    lanes = min(width, 128)
    depth, units = gate_weight.shape
    half = capacity // 2
    dma = pltpu.SemaphoreType.DMA
    return pl.pallas_call(
        functools.partial(layer_kernel, heads, groups),
        out_shape=jax.ShapeDtypeStruct(residual.shape, jnp.bfloat16),
        in_specs=[pl.BlockSpec(memory_space=pltpu.VMEM)] * 10
        + [pl.BlockSpec(memory_space=pl.ANY)] * 3,
        out_specs=pl.BlockSpec(memory_space=pltpu.VMEM),
        scratch_shapes=[
            pltpu.VMEM(index.shape[::-1], jnp.int32),
            pltpu.VMEM(index.shape, jnp.int32),
            pltpu.VMEM((rows, columns), jnp.bfloat16),
            pltpu.VMEM((groups, rows, width), jnp.bfloat16),
            pltpu.VMEM((groups, rows, width), jnp.bfloat16),
            pltpu.VMEM((groups, heads, rows), jnp.float32),
            pltpu.VMEM((heads, rows, lanes), jnp.bfloat16),
            pltpu.VMEM((heads, rows, 128), jnp.float32),
            pltpu.VMEM((heads, rows, 128), jnp.float32),
            pltpu.VMEM((heads, rows, lanes), jnp.float32),
            pltpu.VMEM((4, rows, width), jnp.bfloat16),
            pltpu.VMEM((groups, 2, half, columns), jnp.bfloat16),
            pltpu.VMEM((groups, shards, half, columns), jnp.bfloat16),
            pltpu.VMEM((groups, shards, half, units), jnp.bfloat16),
            pltpu.VMEM((groups, 2, half, columns), jnp.bfloat16),
            pltpu.VMEM((groups, 2, half, columns), jnp.bfloat16),
            pltpu.VMEM((rows, columns), jnp.float32),
            pltpu.VMEM((2, depth, units), jnp.bfloat16),
            pltpu.VMEM((2, depth, units), jnp.bfloat16),
            pltpu.VMEM((2, shards * units, columns), jnp.bfloat16),
            pltpu.VMEM((half, shards * columns), jnp.bfloat16),
            dma((groups, 3)),
            dma((groups, 3)),
            dma((groups, 3)),
            dma((groups, 3)),
            dma((4,)),
            dma((4,)),
            dma((2,)),
            dma((2,)),
            dma((3,)),
            dma(()),
            dma(()),
            dma((groups, 2)),
            dma((groups, 2)),
            dma((groups,)),
            dma((groups,)),
            dma((groups,)),
            dma((groups,)),
            dma((groups, 2)),
            dma((groups, 2)),
        ],
        compiler_params=pltpu.CompilerParams(
            collective_id=1, has_side_effects=True, vmem_limit_bytes=60 * 2**20
        ),
    )(
        query_rows,
        key_rows,
        value_rows,
        gates,
        output_weight,
        residual,
        index.T,
        index,
        route_weights,
        norm_gain.reshape(1, -1),
        gate_weight,
        up_weight,
        down_weight,
    )


def body(
    query_rows,
    key_rows,
    value_rows,
    cum_gates,
    residual,
    output_weight,
    norm_gain,
    expert_index,
    route_weights,
    gate_weight,
    up_weight,
    down_weight,
):
    rows, columns = residual.shape
    topk = expert_index.shape[1]
    local_experts = gate_weight.shape[0]
    groups = lax.axis_size("sp")
    experts = local_experts * groups
    capacity = 2 * rows * topk // experts
    heads = cum_gates.shape[1]

    if lax.axis_size("tp") == 4 and local_experts == 1 and groups in (4, 8):
        index = expert_index ^ lax.axis_index("sp")
        return layer_fused(
            query_rows,
            key_rows,
            value_rows,
            cum_gates.T,
            output_weight,
            residual,
            index,
            route_weights,
            norm_gain,
            gate_weight[0],
            up_weight[0],
            down_weight[0],
            capacity,
        )

    both = jnp.concatenate([key_rows, value_rows], axis=1)
    kv_all = lax.all_gather(both, "sp", axis=0, tiled=True)
    gates_all = lax.all_gather(cum_gates.T, "sp", axis=0, tiled=False)

    chosen = expert_index.reshape(rows * topk)
    matches = (chosen[:, None] == jnp.arange(experts, dtype=jnp.int32)[None, :]).astype(jnp.int32)
    rank = jnp.sum((jnp.cumsum(matches, axis=0) - matches) * matches, axis=1)
    chosen, rank, gates_all = lax.optimization_barrier((chosen, rank, gates_all))

    attended = attend_local(query_rows, kv_all, gates_all)
    projected = jnp.dot(
        lax.all_gather(attended, "tp", axis=1, tiled=True),
        output_weight,
        preferred_element_type=jnp.float32,
    )
    mixed = (residual.astype(jnp.float32) + projected).astype(jnp.bfloat16)

    chunks = math.gcd(capacity, CHUNKS)
    piece = capacity // chunks
    places = chosen * piece + rank % piece
    inside = rank // piece
    blended = jnp.zeros((rows, columns), jnp.float32)
    for c in range(chunks):
        place = jnp.where(inside == c, places, -1).reshape(rows, topk)
        numbers = jnp.arange(experts * piece, dtype=jnp.int32)
        taken = numbers[:, None] == place[:, 0][None, :]
        for k in range(1, topk):
            taken = taken | (numbers[:, None] == place[:, k][None, :])
        outgoing = jnp.dot(
            taken.astype(jnp.bfloat16), mixed, preferred_element_type=jnp.float32
        ).astype(jnp.bfloat16)
        arrived = lax.all_to_all(
            outgoing.reshape(experts, piece, columns), "sp", split_axis=0, concat_axis=0, tiled=True
        )
        grouped = arrived.reshape(groups, local_experts, piece, columns)
        normed = normalize(lax.all_gather(grouped, "tp", axis=3, tiled=True), norm_gain)
        gate_input = jnp.einsum(
            "seid,edf->seif", normed, gate_weight, preferred_element_type=jnp.float32
        )
        linear_input = jnp.einsum(
            "seid,edf->seif", normed, up_weight, preferred_element_type=jnp.float32
        )
        gate_cut = jnp.minimum(gate_input, CLAMP_LIMIT)
        linear_cut = jnp.clip(linear_input, -CLAMP_LIMIT, CLAMP_LIMIT)
        activated = (gate_cut * jax.nn.sigmoid(SILU_ALPHA * gate_cut) * (linear_cut + 1.0)).astype(
            jnp.bfloat16
        )
        produced = jnp.einsum(
            "seif,efc->seic",
            lax.all_gather(activated, "tp", axis=3, tiled=True),
            down_weight,
            preferred_element_type=jnp.float32,
        ).astype(jnp.bfloat16)
        returned = lax.all_to_all(
            produced.reshape(experts, piece, columns), "sp", split_axis=0, concat_axis=0, tiled=True
        ).reshape(experts * piece, columns)
        for k in range(topk):
            picked = jnp.dot(
                (place[:, k][:, None] == numbers[None, :]).astype(jnp.bfloat16),
                returned,
                preferred_element_type=jnp.float32,
            )
            blended = blended + route_weights[:, k : k + 1] * picked
    return (mixed.astype(jnp.float32) + blended).astype(jnp.bfloat16)


def solution(mesh):
    placed = (
        P("sp", "tp"),
        P("sp", "tp"),
        P("sp", "tp"),
        P("sp", "tp"),
        P("sp", "tp"),
        P(None, "tp"),
        P(),
        P("sp", None),
        P("sp", None),
        P("sp", None, "tp"),
        P("sp", None, "tp"),
        P("sp", None, "tp"),
    )
    return jax.shard_map(body, mesh=mesh, in_specs=placed, out_specs=P("sp", "tp"), check_vma=False)
```

```python
import functools
import math

import jax
import jax.numpy as jnp
from jax import lax
from jax.experimental import pallas as pl
from jax.experimental.pallas import tpu as pltpu
from jax.sharding import PartitionSpec as P

NORM_EPS = 1e-06
CLAMP_LIMIT = 7.0
SILU_ALPHA = 1.702
CHUNKS = 1


def normalize(rows, norm_gain):
    wide = rows.astype(jnp.float32)
    factor = lax.rsqrt(jnp.mean(wide * wide, axis=-1, keepdims=True) + NORM_EPS)
    return (wide * factor * norm_gain.astype(jnp.float32)).astype(jnp.bfloat16)


def attend_kernel(heads, q_ref, kv_ref, gates_ref, out_ref, masked_q, top, total, summed):
    rows, width = q_ref.shape
    head_size = width // heads
    lanes = min(width, 128)
    tile = math.gcd(rows, 256)
    tiles = rows // tile
    me = lax.axis_index("sp")
    scale = head_size ** (-0.5)
    lane = lax.broadcasted_iota(jnp.int32, (rows, lanes), 1)
    for h in range(heads):
        group, inside = divmod(h * head_size, lanes)
        part = q_ref[:, group * lanes : (group + 1) * lanes].astype(jnp.float32) * scale
        keep = (lane >= inside) & (lane < inside + head_size)
        masked_q[h] = jnp.where(keep, part, 0.0).astype(jnp.bfloat16)
    top[...] = jnp.full(top.shape, -1e30, jnp.float32)
    total[...] = jnp.zeros(total.shape, jnp.float32)
    summed[...] = jnp.zeros(summed.shape, jnp.float32)

    def block(number, diagonal):
        base = pl.multiple_of(number * rows, rows)
        for h in range(heads):
            group = h * head_size // lanes
            keys = kv_ref[pl.ds(base, rows), group * lanes : (group + 1) * lanes]
            values = kv_ref[pl.ds(base, rows), width + group * lanes : width + (group + 1) * lanes]
            gates = gates_ref[number, h : h + 1, :]
            for t in range(tiles):
                span = slice(t * tile, (t + 1) * tile)
                count = (t + 1) * tile if diagonal else rows
                scores = lax.dot_general(
                    masked_q[h, span],
                    keys[:count],
                    (((1,), (1,)), ((), ())),
                    preferred_element_type=jnp.float32,
                )
                scores = scores - gates[:, :count]
                if diagonal:
                    row = lax.broadcasted_iota(jnp.int32, (tile, count), 0) + t * tile
                    col = lax.broadcasted_iota(jnp.int32, (tile, count), 1)
                    scores = jnp.where(col <= row, scores, -jnp.inf)
                old = top[h, span]
                new = jnp.maximum(old, jnp.max(scores, axis=1, keepdims=True))
                raised = jnp.exp(scores - new[:, :1])
                shrink = jnp.exp(old - new)
                part = raised[:, :128]
                for c in range(128, count, 128):
                    part = part + raised[:, c : c + 128]
                top[h, span] = new
                total[h, span] = total[h, span] * shrink + part
                product = lax.dot_general(
                    raised.astype(jnp.bfloat16),
                    values[:count],
                    (((1,), (0,)), ((), ())),
                    preferred_element_type=jnp.float32,
                )
                summed[h, span] = summed[h, span] * shrink[:, :lanes] + product

    def step(number, carry):
        block(number, False)
        return carry

    lax.fori_loop(0, me, step, 0)
    block(me, True)
    for g in range(width // lanes):
        result = jnp.zeros((rows, lanes), jnp.float32)
        for h in range(heads):
            if h * head_size // lanes == g:
                inside = h * head_size % lanes
                keep = (lane >= inside) & (lane < inside + head_size)
                whole = jnp.sum(total[h], axis=1, keepdims=True)
                result = jnp.where(keep, summed[h] / whole, result)
        out_ref[:, g * lanes : (g + 1) * lanes] = result.astype(out_ref.dtype)


def attend_local(query_rows, kv_all, gates_all):
    rows, width = query_rows.shape
    groups, heads, _ = gates_all.shape
    lanes = min(width, 128)
    return pl.pallas_call(
        functools.partial(attend_kernel, heads),
        out_shape=jax.ShapeDtypeStruct((rows, width), jnp.bfloat16),
        in_specs=[pl.BlockSpec(memory_space=pltpu.VMEM)] * 3,
        out_specs=pl.BlockSpec(memory_space=pltpu.VMEM),
        scratch_shapes=[
            pltpu.VMEM((heads, rows, lanes), jnp.bfloat16),
            pltpu.VMEM((heads, rows, 128), jnp.float32),
            pltpu.VMEM((heads, rows, 128), jnp.float32),
            pltpu.VMEM((heads, rows, lanes), jnp.float32),
        ],
        compiler_params=pltpu.CompilerParams(vmem_limit_bytes=48 * 2**20),
        cost_estimate=pl.CostEstimate(
            flops=4 * rows * rows * groups * width * 4,
            bytes_accessed=4 * rows * groups * width,
            transcendentals=rows * rows * groups * heads,
        ),
    )(query_rows, kv_all, gates_all)


def half_of(core, tp):
    return (1 - core) * (tp // 2) + core * (tp % 2)


def partner_of(core, tp):
    return (1 - core) * ((tp + 2) % 4) + core * (tp + 1 - 2 * (tp % 2))


def layer_kernel(
    heads,
    groups,
    q_ref,
    k_ref,
    v_ref,
    gates_ref,
    weight_ref,
    residual_ref,
    index_row_ref,
    index_col_ref,
    route_ref,
    gain_ref,
    gate_ref,
    up_ref,
    down_ref,
    out_ref,
    place_row_ref,
    place_col_ref,
    mixed_ref,
    kv_out,
    q_out,
    kv_all,
    q_all,
    gates_all,
    gate_pair,
    packed,
    heads_in,
    masked_q,
    top,
    total,
    summed,
    attended,
    outbox,
    full,
    act,
    made,
    returned,
    blended,
    gate_all,
    up_all,
    down_all,
    wide_rows,
    kv_send,
    side_send,
    kv_recv,
    q_send,
    q_recv,
    head_send,
    head_recv,
    tp_send,
    tp_recv,
    weight_send,
    weight_recv,
    load_sem,
    down_send,
    down_recv,
    out_send,
    out_recv,
    one_send,
    one_recv,
    two_send,
    two_recv,
    back_send,
    back_recv,
):
    rows, width = q_ref.shape
    head_size = width // heads
    lanes = min(width, 128)
    tile = math.gcd(rows, 256)
    tiles = rows // tile
    sp = lax.axis_index("sp")
    tp = lax.axis_index("tp")
    chip = sp // 2
    core = sp % 2
    chips = groups // 2
    sibling = sp + 1 - 2 * core
    beside = tp + 1 - 2 * (tp % 2)
    across = (tp + 2) % 4
    mesh_id = pl.DeviceIdType.MESH
    scale = head_size ** (-0.5)
    lead = (sp + chip) % 2

    def direct(which):
        return pltpu.make_async_remote_copy(
            src_ref=attended.at[tp],
            dst_ref=attended.at[tp],
            send_sem=tp_send.at[which],
            recv_sem=tp_recv.at[which],
            device_id=(sp, beside if which == 0 else across),
            device_id_type=mesh_id,
        )

    def relay(which):
        owner = beside if which == 0 else across
        part = attended.at[owner, pl.ds(which * (rows // 2), rows // 2)]
        return pltpu.make_async_remote_copy(
            src_ref=part,
            dst_ref=part,
            send_sem=tp_send.at[2 + which],
            recv_sem=tp_recv.at[2 + which],
            device_id=(sp, across if which == 0 else beside),
            device_id_type=mesh_id,
        )

    topk = route_ref.shape[1]
    half, columns = outbox.shape[2:]
    capacity = 2 * half
    shards = full.shape[1]
    mine = half_of(core, tp)
    pair = partner_of(core, tp)
    peer = partner_of(1 - core, tp)
    owners = (tp, pair, peer, (beside + 2) % 4)

    def partner(number):
        found, bit = 0, 1
        while bit < groups:
            found = found + bit * (((sp // bit) % 2 + (number // bit) % 2) % 2)
            bit *= 2
        return found

    def send(src, dst, send_sem, recv_sem, device):
        return pltpu.make_async_remote_copy(
            src_ref=src,
            dst_ref=dst,
            send_sem=send_sem,
            recv_sem=recv_sem,
            device_id=device,
            device_id_type=pl.DeviceIdType.MESH,
        )

    def spread(head):
        device = (2 * head + core, tp)
        return [
            send(src, dst.at[sp], kv_send.at[head, n], kv_recv.at[sp, n], device)
            for n, (src, dst) in enumerate(((kv_out.at[head], kv_all), (gates_ref, gates_all)))
        ]

    def sideways(number, own=False):
        return [
            send(src, dst.at[number], side_send.at[number, n], kv_recv.at[number, n], (sibling, tp))
            for n, (src, dst) in enumerate(
                (
                    (kv_all.at[number], kv_all),
                    (gates_ref if own else gates_all.at[number], gates_all),
                )
            )
        ]

    def ask(head):
        return send(
            q_out.at[head],
            q_all.at[chip],
            q_send.at[head],
            q_recv.at[chip],
            (2 * head + lead, tp),
        )

    def answer(slot):
        return send(
            packed.at[slot],
            heads_in.at[chip],
            head_send.at[slot],
            head_recv.at[chip],
            (2 * slot + (slot + core) % 2, tp),
        )

    def dispatch(i, which):
        group = partner(i)
        target = tp if which == 0 else partner_of(group % 2, tp)
        return send(
            outbox.at[i, which],
            full.at[i, which],
            out_send.at[i, which],
            out_recv.at[i, which],
            (group, target),
        )

    def exchange(i, held, send_sem, recv_sem):
        return send(
            held.at[i, pl.ds(0, 2)],
            held.at[i, pl.ds(2, 2)],
            send_sem.at[i],
            recv_sem.at[i],
            (sp, peer),
        )

    def give_back(i, which):
        target = tp if which == 0 else pair
        return send(
            made.at[i, which],
            returned.at[i, mine],
            back_send.at[i, which],
            back_recv.at[i, mine],
            (partner(i), target),
        )

    def arrive_back(i, which):
        return send(
            made.at[i, 0],
            returned.at[i, which],
            back_send.at[i, 0],
            back_recv.at[i, which],
            (sp, pair),
        )

    loads = []
    for n, (src, dst) in enumerate(
        ((gate_ref, gate_all.at[0]), (up_ref, up_all.at[0]), (down_ref, down_all.at[0]))
    ):
        loads.append(pltpu.make_async_copy(src, dst, load_sem.at[n]))
    for load in loads:
        load.start()

    barrier = pltpu.get_barrier_semaphore()
    for i in range(1, groups):
        pl.semaphore_signal(
            barrier, inc=1, device_id=(partner(i), tp), device_id_type=pl.DeviceIdType.MESH
        )
        pl.semaphore_signal(
            barrier,
            inc=1,
            device_id=(partner(i), partner_of(partner(i) % 2, tp)),
            device_id_type=pl.DeviceIdType.MESH,
        )
        pl.semaphore_signal(
            barrier, inc=1, device_id=(partner(i), pair), device_id_type=pl.DeviceIdType.MESH
        )
    for other in (pair, peer):
        pl.semaphore_signal(
            barrier, inc=1, device_id=(sp, other), device_id_type=pl.DeviceIdType.MESH
        )
    pl.semaphore_wait(barrier, 3 * groups - 1)

    down_copy = send(down_ref, down_all.at[1], down_send, down_recv, (sp, pair))

    weight_copies = [
        pltpu.make_async_remote_copy(
            src_ref=src,
            dst_ref=dst,
            send_sem=weight_send.at[n],
            recv_sem=weight_recv.at[n],
            device_id=(sp, pair),
            device_id_type=mesh_id,
        )
        for n, (src, dst) in enumerate(((gate_ref, gate_all.at[1]), (up_ref, up_all.at[1])))
    ]

    lane = lax.broadcasted_iota(jnp.int32, (rows, lanes), 1)
    low = lane < head_size
    short = rows // 2
    short_low = low[:short]

    def turned(wide):
        return pltpu.roll(wide, head_size, 1)

    for g in range(width // lanes):
        part = slice(g * lanes, (g + 1) * lanes)
        wide = q_ref[:, part].astype(jnp.float32) * scale
        tail = turned(wide[short:])
        q_out[2 * g] = jnp.where(short_low, wide[:short], tail).astype(jnp.bfloat16)
        q_out[2 * g + 1] = jnp.where(short_low, tail, wide[:short]).astype(jnp.bfloat16)
    for s in range(1, chips):
        ask(partner(2 * s) // 2).start()

    @pl.when(lead != core)
    def _():
        ask(chip).start()

    @pl.when(lead == core)
    def _():
        q_all[chip] = q_out[chip]

    for g in range(width // lanes):
        part = slice(g * lanes, (g + 1) * lanes)
        keys = k_ref[:, part].astype(jnp.float32)
        values = turned(v_ref[:, part].astype(jnp.float32))
        kv_out[2 * g] = jnp.where(low, keys, values).astype(jnp.bfloat16)
        kv_out[2 * g + 1] = jnp.where(low, values, keys).astype(jnp.bfloat16)
    for s in range(1, chips):
        for copy in spread(partner(2 * s) // 2):
            copy.start()
    kv_all[sp] = kv_out[chip]
    gates_all[sp] = gates_ref[...]
    for copy in sideways(sp, True):
        copy.start()
    for copy in weight_copies:
        copy.start()

    first = lax.broadcasted_iota(jnp.int32, (rows, rows), 0)
    second = lax.broadcasted_iota(jnp.int32, (rows, rows), 1)
    number = lax.broadcasted_iota(jnp.int32, (rows, 128), 1)
    named = jnp.zeros((rows, 128), jnp.float32)
    for k in range(topk):
        named = named + jnp.where(number == index_col_ref[:, k : k + 1], 1.0, 0.0)
    before = jnp.dot(
        jnp.where(second < first, 1.0, 0.0).astype(jnp.bfloat16),
        named.astype(jnp.bfloat16),
        preferred_element_type=jnp.float32,
    )
    for k in range(topk):
        expert = index_col_ref[:, k : k + 1]
        rank = jnp.sum(jnp.where(number == expert, before, 0.0), axis=1, keepdims=True)
        place_col_ref[:, k : k + 1] = expert * capacity + rank.astype(jnp.int32)
    number = lax.broadcasted_iota(jnp.int32, (128, rows), 0)
    named = jnp.zeros((128, rows), jnp.float32)
    for k in range(topk):
        named = named + jnp.where(number == index_row_ref[k : k + 1, :], 1.0, 0.0)
    before = jnp.dot(
        named.astype(jnp.bfloat16),
        jnp.where(first < second, 1.0, 0.0).astype(jnp.bfloat16),
        preferred_element_type=jnp.float32,
    )
    for k in range(topk):
        expert = index_row_ref[k : k + 1, :]
        rank = jnp.sum(jnp.where(number == expert, before, 0.0), axis=0, keepdims=True)
        place_row_ref[k : k + 1, :] = expert * capacity + rank.astype(jnp.int32)

    odd = chip % 2
    key_lane = (lane // head_size) == odd
    short_key = key_lane[:short]
    top[...] = jnp.full(top.shape, -1e30, jnp.float32)
    total[...] = jnp.zeros(total.shape, jnp.float32)
    summed[...] = jnp.zeros(summed.shape, jnp.float32)
    for n in range(chips):

        @pl.when((n != chip) | (lead != core))
        def _():
            send(
                q_out.at[0], q_all.at[n], q_send.at[0], q_recv.at[n], (sibling, tp)
            ).wait_recv()

        part = q_all[n].astype(jnp.float32)
        masked_q[n, :short] = jnp.where(short_key, part, 0.0).astype(jnp.bfloat16)
        masked_q[n, short:] = jnp.where(short_key, turned(part), 0.0).astype(jnp.bfloat16)

    def block(slot, number, offset):
        span_keys = 2 * rows
        for t in range(tiles):
            span = slice(t * tile, (t + 1) * tile)
            count = span_keys if offset is None else offset + (t + 1) * tile
            pair_kv = kv_all[pl.ds(2 * number, 2)].reshape(span_keys, lanes)[:count]
            scores = lax.dot_general(
                masked_q[slot, span],
                pair_kv,
                (((1,), (1,)), ((), ())),
                preferred_element_type=jnp.float32,
            )
            scores = scores - gate_pair[0:1, :count]
            if offset is not None:
                row = lax.broadcasted_iota(jnp.int32, (tile, count), 0) + t * tile + offset
                col = lax.broadcasted_iota(jnp.int32, (tile, count), 1)
                scores = jnp.where(col <= row, scores, -jnp.inf)
            old = top[slot, span]
            new = jnp.maximum(old, jnp.max(scores, axis=1, keepdims=True))
            raised = jnp.exp(scores - new[:, :1])
            shrink = jnp.exp(old - new)
            part = raised[:, :128]
            for c in range(128, count, 128):
                part = part + raised[:, c : c + 128]
            top[slot, span] = new
            total[slot, span] = total[slot, span] * shrink + part
            product = lax.dot_general(
                raised.astype(jnp.bfloat16),
                pair_kv,
                (((1,), (0,)), ((), ())),
                preferred_element_type=jnp.float32,
            )
            summed[slot, span] = summed[slot, span] * shrink[:, :lanes] + product

    def chip_step(s, carry):
        number = partner(2 * s) // 2
        near = 2 * number + core

        @pl.when(s > 0)
        def _():
            for copy in sideways(near):
                copy.wait_recv()
            for copy in sideways(near):
                copy.start()

        for copy in sideways(2 * number + 1 - core):
            copy.wait_recv()
        gate_pair[0:1, :rows] = gates_all[2 * number, pl.ds(chip, 1), :]
        gate_pair[0:1, rows:] = gates_all[2 * number + 1, pl.ds(chip, 1), :]

        @pl.when((number + core) % 2 == 0)
        def _():
            block(number, number, 0)

        @pl.when((number + core) % 2 == 1)
        def _():
            block(number, number, rows)

        def full_step(slot, inner):
            block(slot, number, None)
            return inner

        lax.fori_loop(number + 1, chips, full_step, 0)
        return carry

    lax.fori_loop(0, chips, chip_step, 0)

    for n in range(chips):
        result = summed[n] / jnp.sum(total[n], axis=1, keepdims=True)
        folded = jnp.where(short_key, turned(result[short:]), result[:short])
        packed[n] = folded.astype(jnp.bfloat16)

        @pl.when((n != chip) | (lead != core))
        def _():
            answer(n).start()

        @pl.when((n == chip) & (lead == core))
        def _():
            heads_in[chip] = packed[n]

    for n in range(chips):

        @pl.when((n != chip) | (lead != core))
        def _():
            send(
                packed.at[0], heads_in.at[n], head_send.at[0], head_recv.at[n], (sibling, tp)
            ).wait_recv()

    for g in range(width // lanes):
        even = heads_in[2 * g].astype(jnp.float32)
        uneven = heads_in[2 * g + 1].astype(jnp.float32)
        part = slice(g * lanes, (g + 1) * lanes)
        attended[tp, :short, part] = jnp.where(short_low, turned(even), turned(uneven)).astype(
            jnp.bfloat16
        )
        attended[tp, short:, part] = jnp.where(short_low, even, uneven).astype(jnp.bfloat16)
    direct(0).start()
    direct(1).start()
    down_copy.start()

    def projected(owner):
        return jnp.dot(
            attended[owner],
            weight_ref[pl.ds(pl.multiple_of(owner * width, width), width), :],
            preferred_element_type=jnp.float32,
        )

    mixed = residual_ref[...].astype(jnp.float32) + projected(tp)
    for which, owner in ((0, beside), (1, across)):
        direct(which).wait_recv()
        relay(which).start()
        mixed = mixed + projected(owner)
    relay(0).wait_recv()
    relay(1).wait_recv()
    mixed_ref[...] = (mixed + projected((beside + 2) % 4)).astype(mixed_ref.dtype)

    def rows_for(i):
        flip = half_of(partner(i) % 2, tp)
        place = lax.broadcasted_iota(jnp.int32, (capacity, rows), 0) + flip * half
        numbers = jnp.where(place >= capacity, place - capacity, place) + i * capacity
        taken = numbers == place_row_ref[0:1, :]
        for k in range(1, topk):
            taken = taken | (numbers == place_row_ref[k : k + 1, :])
        return jnp.dot(
            jnp.where(taken, 1.0, 0.0).astype(jnp.bfloat16),
            mixed_ref[...],
            preferred_element_type=jnp.float32,
        ).astype(jnp.bfloat16)

    first = rows_for(0)
    full[0, 0] = first[:half]
    outbox[0, 1] = first[half:]
    dispatch(0, 1).start()

    def fill(i, carry):
        made_rows = rows_for(i)
        outbox[i, 0] = made_rows[:half]
        outbox[i, 1] = made_rows[half:]
        dispatch(i, 0).start()
        dispatch(i, 1).start()
        return carry

    lax.fori_loop(1, groups, fill, 0)
    blended[...] = mixed_ref[...].astype(jnp.float32)
    for load in loads:
        load.wait()
    for copy in weight_copies:
        copy.wait_recv()

    def hidden(i):
        square = jnp.zeros((half, 1), jnp.float32)
        for j in range(shards):
            wide = full[i, j].astype(jnp.float32)
            square = square + jnp.sum(wide * wide, axis=1, keepdims=True)
        factor = lax.rsqrt(square / (shards * columns) + NORM_EPS)
        for j in range(shards):
            span = pl.ds(pl.multiple_of(owners[j] * columns, columns), columns)
            gain = gain_ref[0:1, span].astype(jnp.float32)
            wide_rows[:, span] = (full[i, j].astype(jnp.float32) * factor * gain).astype(
                jnp.bfloat16
            )
        for c in range(2):
            gate_input = jnp.dot(
                wide_rows[...], gate_all[c], preferred_element_type=jnp.float32
            )
            linear_input = jnp.dot(wide_rows[...], up_all[c], preferred_element_type=jnp.float32)
            gate_cut = jnp.minimum(gate_input, CLAMP_LIMIT)
            linear_cut = jnp.clip(linear_input, -CLAMP_LIMIT, CLAMP_LIMIT)
            act[i, c] = (
                gate_cut * jax.nn.sigmoid(SILU_ALPHA * gate_cut) * (linear_cut + 1.0)
            ).astype(jnp.bfloat16)

    def output_rows(i, c):
        return jnp.dot(
            wide_rows[...], down_all[c], preferred_element_type=jnp.float32
        ).astype(jnp.bfloat16)

    def step(i, carry):
        @pl.when(i < groups)
        def _():
            @pl.when(i > 0)
            def _():
                dispatch(i, 0).wait_recv()

            dispatch(i, 1).wait_recv()
            exchange(i, full, one_send, one_recv).start()

        @pl.when((i >= 1) & (i < groups + 1))
        def _():
            exchange(i - 1, full, one_send, one_recv).wait_recv()
            hidden(i - 1)
            exchange(i - 1, act, two_send, two_recv).start()

        @pl.when((i >= 2) & (i < groups + 2))
        def _():
            b = i - 2

            @pl.when(b == 0)
            def _():
                down_copy.wait_recv()

            exchange(b, act, two_send, two_recv).wait_recv()
            for j in range(shards):
                span = pl.ds(pl.multiple_of(owners[j] * columns, columns), columns)
                wide_rows[:, span] = act[b, j]
            made[b, 1] = output_rows(b, 1)
            give_back(b, 1).start()
            result = output_rows(b, 0)

            @pl.when(b == 0)
            def _():
                returned[0, mine] = result

            @pl.when(b > 0)
            def _():
                made[b, 0] = result
                give_back(b, 0).start()

        @pl.when(i >= 3)
        def _():
            b = i - 3

            @pl.when(b == 0)
            def _():
                arrive_back(0, 1 - mine).wait_recv()

            @pl.when(b > 0)
            def _():
                arrive_back(b, 0).wait_recv()
                arrive_back(b, 1).wait_recv()

            numbers = lax.broadcasted_iota(jnp.int32, (rows, capacity), 1) + b * capacity
            added = blended[...]
            rows_back = returned[b].reshape(capacity, columns)
            for k in range(topk):
                taken = jnp.where(numbers == place_col_ref[:, k : k + 1], 1.0, 0.0)
                picked = jnp.dot(
                    taken.astype(jnp.bfloat16), rows_back, preferred_element_type=jnp.float32
                )
                added = added + route_ref[:, k : k + 1] * picked
            blended[...] = added

        return carry

    lax.fori_loop(0, groups + 3, step, 0)
    out_ref[...] = blended[...].astype(out_ref.dtype)

    def settle(i, carry):
        @pl.when(i > 0)
        def _():
            dispatch(i, 0).wait_send()
            give_back(i, 0).wait_send()

        dispatch(i, 1).wait_send()
        give_back(i, 1).wait_send()
        exchange(i, full, one_send, one_recv).wait_send()
        exchange(i, act, two_send, two_recv).wait_send()
        return carry

    lax.fori_loop(0, groups, settle, 0)
    down_copy.wait_send()

    for which in range(2):
        direct(which).wait_send()
        relay(which).wait_send()

    for s in range(1, chips):
        ask(partner(2 * s) // 2).wait_send()
        for copy in spread(partner(2 * s) // 2):
            copy.wait_send()
        for copy in sideways(2 * (partner(2 * s) // 2) + core):
            copy.wait_send()
    for copy in sideways(sp, True):
        copy.wait_send()

    @pl.when(lead != core)
    def _():
        ask(chip).wait_send()

    for n in range(chips):

        @pl.when((n != chip) | (lead != core))
        def _():
            answer(n).wait_send()

    for copy in weight_copies:
        copy.wait_send()


def layer_fused(
    query_rows,
    key_rows,
    value_rows,
    gates,
    output_weight,
    residual,
    index,
    route_weights,
    norm_gain,
    gate_weight,
    up_weight,
    down_weight,
    capacity,
):
    rows, width = query_rows.shape
    columns = residual.shape[1]
    heads = gates.shape[0]
    groups = lax.axis_size("sp")
    shards = lax.axis_size("tp")
    lanes = min(width, 128)
    depth, units = gate_weight.shape
    half = capacity // 2
    dma = pltpu.SemaphoreType.DMA
    return pl.pallas_call(
        functools.partial(layer_kernel, heads, groups),
        out_shape=jax.ShapeDtypeStruct(residual.shape, jnp.bfloat16),
        in_specs=[pl.BlockSpec(memory_space=pltpu.VMEM)] * 10
        + [pl.BlockSpec(memory_space=pl.ANY)] * 3,
        out_specs=pl.BlockSpec(memory_space=pltpu.VMEM),
        scratch_shapes=[
            pltpu.VMEM(index.shape[::-1], jnp.int32),
            pltpu.VMEM(index.shape, jnp.int32),
            pltpu.VMEM((rows, columns), jnp.bfloat16),
            pltpu.VMEM((heads, rows, lanes), jnp.bfloat16),
            pltpu.VMEM((heads, rows // 2, lanes), jnp.bfloat16),
            pltpu.VMEM((groups, rows, lanes), jnp.bfloat16),
            pltpu.VMEM((heads, rows // 2, lanes), jnp.bfloat16),
            pltpu.VMEM((groups, heads, rows), jnp.float32),
            pltpu.VMEM((8, 2 * rows), jnp.float32),
            pltpu.VMEM((heads, rows // 2, lanes), jnp.bfloat16),
            pltpu.VMEM((heads, rows // 2, lanes), jnp.bfloat16),
            pltpu.VMEM((heads, rows, lanes), jnp.bfloat16),
            pltpu.VMEM((heads, rows, 128), jnp.float32),
            pltpu.VMEM((heads, rows, 128), jnp.float32),
            pltpu.VMEM((heads, rows, lanes), jnp.float32),
            pltpu.VMEM((4, rows, width), jnp.bfloat16),
            pltpu.VMEM((groups, 2, half, columns), jnp.bfloat16),
            pltpu.VMEM((groups, shards, half, columns), jnp.bfloat16),
            pltpu.VMEM((groups, shards, half, units), jnp.bfloat16),
            pltpu.VMEM((groups, 2, half, columns), jnp.bfloat16),
            pltpu.VMEM((groups, 2, half, columns), jnp.bfloat16),
            pltpu.VMEM((rows, columns), jnp.float32),
            pltpu.VMEM((2, depth, units), jnp.bfloat16),
            pltpu.VMEM((2, depth, units), jnp.bfloat16),
            pltpu.VMEM((2, shards * units, columns), jnp.bfloat16),
            pltpu.VMEM((half, shards * columns), jnp.bfloat16),
            dma((heads, 2)),
            dma((groups, 2)),
            dma((groups, 2)),
            dma((heads,)),
            dma((heads,)),
            dma((heads,)),
            dma((heads,)),
            dma((4,)),
            dma((4,)),
            dma((2,)),
            dma((2,)),
            dma((3,)),
            dma(()),
            dma(()),
            dma((groups, 2)),
            dma((groups, 2)),
            dma((groups,)),
            dma((groups,)),
            dma((groups,)),
            dma((groups,)),
            dma((groups, 2)),
            dma((groups, 2)),
        ],
        compiler_params=pltpu.CompilerParams(
            collective_id=1, has_side_effects=True, vmem_limit_bytes=60 * 2**20
        ),
    )(
        query_rows,
        key_rows,
        value_rows,
        gates,
        output_weight,
        residual,
        index.T,
        index,
        route_weights,
        norm_gain.reshape(1, -1),
        gate_weight,
        up_weight,
        down_weight,
    )


def body(
    query_rows,
    key_rows,
    value_rows,
    cum_gates,
    residual,
    output_weight,
    norm_gain,
    expert_index,
    route_weights,
    gate_weight,
    up_weight,
    down_weight,
):
    rows, columns = residual.shape
    topk = expert_index.shape[1]
    local_experts = gate_weight.shape[0]
    groups = lax.axis_size("sp")
    experts = local_experts * groups
    capacity = 2 * rows * topk // experts
    heads = cum_gates.shape[1]

    if (
        lax.axis_size("tp") == 4
        and local_experts == 1
        and groups == 8
        and heads == 4
        and query_rows.shape[1] == heads * 64
    ):
        index = expert_index ^ lax.axis_index("sp")
        return layer_fused(
            query_rows,
            key_rows,
            value_rows,
            cum_gates.T,
            output_weight,
            residual,
            index,
            route_weights,
            norm_gain,
            gate_weight[0],
            up_weight[0],
            down_weight[0],
            capacity,
        )

    both = jnp.concatenate([key_rows, value_rows], axis=1)
    kv_all = lax.all_gather(both, "sp", axis=0, tiled=True)
    gates_all = lax.all_gather(cum_gates.T, "sp", axis=0, tiled=False)

    chosen = expert_index.reshape(rows * topk)
    matches = (chosen[:, None] == jnp.arange(experts, dtype=jnp.int32)[None, :]).astype(jnp.int32)
    rank = jnp.sum((jnp.cumsum(matches, axis=0) - matches) * matches, axis=1)
    chosen, rank, gates_all = lax.optimization_barrier((chosen, rank, gates_all))

    attended = attend_local(query_rows, kv_all, gates_all)
    projected = jnp.dot(
        lax.all_gather(attended, "tp", axis=1, tiled=True),
        output_weight,
        preferred_element_type=jnp.float32,
    )
    mixed = (residual.astype(jnp.float32) + projected).astype(jnp.bfloat16)

    chunks = math.gcd(capacity, CHUNKS)
    piece = capacity // chunks
    places = chosen * piece + rank % piece
    inside = rank // piece
    blended = jnp.zeros((rows, columns), jnp.float32)
    for c in range(chunks):
        place = jnp.where(inside == c, places, -1).reshape(rows, topk)
        numbers = jnp.arange(experts * piece, dtype=jnp.int32)
        taken = numbers[:, None] == place[:, 0][None, :]
        for k in range(1, topk):
            taken = taken | (numbers[:, None] == place[:, k][None, :])
        outgoing = jnp.dot(
            taken.astype(jnp.bfloat16), mixed, preferred_element_type=jnp.float32
        ).astype(jnp.bfloat16)
        arrived = lax.all_to_all(
            outgoing.reshape(experts, piece, columns), "sp", split_axis=0, concat_axis=0, tiled=True
        )
        grouped = arrived.reshape(groups, local_experts, piece, columns)
        normed = normalize(lax.all_gather(grouped, "tp", axis=3, tiled=True), norm_gain)
        gate_input = jnp.einsum(
            "seid,edf->seif", normed, gate_weight, preferred_element_type=jnp.float32
        )
        linear_input = jnp.einsum(
            "seid,edf->seif", normed, up_weight, preferred_element_type=jnp.float32
        )
        gate_cut = jnp.minimum(gate_input, CLAMP_LIMIT)
        linear_cut = jnp.clip(linear_input, -CLAMP_LIMIT, CLAMP_LIMIT)
        activated = (gate_cut * jax.nn.sigmoid(SILU_ALPHA * gate_cut) * (linear_cut + 1.0)).astype(
            jnp.bfloat16
        )
        produced = jnp.einsum(
            "seif,efc->seic",
            lax.all_gather(activated, "tp", axis=3, tiled=True),
            down_weight,
            preferred_element_type=jnp.float32,
        ).astype(jnp.bfloat16)
        returned = lax.all_to_all(
            produced.reshape(experts, piece, columns), "sp", split_axis=0, concat_axis=0, tiled=True
        ).reshape(experts * piece, columns)
        for k in range(topk):
            picked = jnp.dot(
                (place[:, k][:, None] == numbers[None, :]).astype(jnp.bfloat16),
                returned,
                preferred_element_type=jnp.float32,
            )
            blended = blended + route_weights[:, k : k + 1] * picked
    return (mixed.astype(jnp.float32) + blended).astype(jnp.bfloat16)


def solution(mesh):
    placed = (
        P("sp", "tp"),
        P("sp", "tp"),
        P("sp", "tp"),
        P("sp", "tp"),
        P("sp", "tp"),
        P(None, "tp"),
        P(),
        P("sp", None),
        P("sp", None),
        P("sp", None, "tp"),
        P("sp", None, "tp"),
        P("sp", None, "tp"),
    )
    return jax.shard_map(body, mesh=mesh, in_specs=placed, out_specs=P("sp", "tp"), check_vma=False)
```

```python
import functools
import math

import jax
import jax.numpy as jnp
from jax import lax
from jax.experimental import pallas as pl
from jax.experimental.pallas import tpu as pltpu
from jax.sharding import PartitionSpec as P

NORM_EPS = 1e-06
CLAMP_LIMIT = 7.0
SILU_ALPHA = 1.702
CHUNKS = 1


def normalize(rows, norm_gain):
    wide = rows.astype(jnp.float32)
    factor = lax.rsqrt(jnp.mean(wide * wide, axis=-1, keepdims=True) + NORM_EPS)
    return (wide * factor * norm_gain.astype(jnp.float32)).astype(jnp.bfloat16)


def attend_kernel(heads, q_ref, kv_ref, gates_ref, out_ref, masked_q, top, total, summed):
    rows, width = q_ref.shape
    head_size = width // heads
    lanes = min(width, 128)
    tile = math.gcd(rows, 256)
    tiles = rows // tile
    me = lax.axis_index("sp")
    scale = head_size ** (-0.5)
    lane = lax.broadcasted_iota(jnp.int32, (rows, lanes), 1)
    for h in range(heads):
        group, inside = divmod(h * head_size, lanes)
        part = q_ref[:, group * lanes : (group + 1) * lanes].astype(jnp.float32) * scale
        keep = (lane >= inside) & (lane < inside + head_size)
        masked_q[h] = jnp.where(keep, part, 0.0).astype(jnp.bfloat16)
    top[...] = jnp.full(top.shape, -1e30, jnp.float32)
    total[...] = jnp.zeros(total.shape, jnp.float32)
    summed[...] = jnp.zeros(summed.shape, jnp.float32)

    def block(number, diagonal):
        base = pl.multiple_of(number * rows, rows)
        for h in range(heads):
            group = h * head_size // lanes
            keys = kv_ref[pl.ds(base, rows), group * lanes : (group + 1) * lanes]
            values = kv_ref[pl.ds(base, rows), width + group * lanes : width + (group + 1) * lanes]
            gates = gates_ref[number, h : h + 1, :]
            for t in range(tiles):
                span = slice(t * tile, (t + 1) * tile)
                count = (t + 1) * tile if diagonal else rows
                scores = lax.dot_general(
                    masked_q[h, span],
                    keys[:count],
                    (((1,), (1,)), ((), ())),
                    preferred_element_type=jnp.float32,
                )
                scores = scores - gates[:, :count]
                if diagonal:
                    row = lax.broadcasted_iota(jnp.int32, (tile, count), 0) + t * tile
                    col = lax.broadcasted_iota(jnp.int32, (tile, count), 1)
                    scores = jnp.where(col <= row, scores, -jnp.inf)
                old = top[h, span]
                new = jnp.maximum(old, jnp.max(scores, axis=1, keepdims=True))
                raised = jnp.exp(scores - new[:, :1])
                shrink = jnp.exp(old - new)
                part = raised[:, :128]
                for c in range(128, count, 128):
                    part = part + raised[:, c : c + 128]
                top[h, span] = new
                total[h, span] = total[h, span] * shrink + part
                product = lax.dot_general(
                    raised.astype(jnp.bfloat16),
                    values[:count],
                    (((1,), (0,)), ((), ())),
                    preferred_element_type=jnp.float32,
                )
                summed[h, span] = summed[h, span] * shrink[:, :lanes] + product

    def step(number, carry):
        block(number, False)
        return carry

    lax.fori_loop(0, me, step, 0)
    block(me, True)
    for g in range(width // lanes):
        result = jnp.zeros((rows, lanes), jnp.float32)
        for h in range(heads):
            if h * head_size // lanes == g:
                inside = h * head_size % lanes
                keep = (lane >= inside) & (lane < inside + head_size)
                whole = jnp.sum(total[h], axis=1, keepdims=True)
                result = jnp.where(keep, summed[h] / whole, result)
        out_ref[:, g * lanes : (g + 1) * lanes] = result.astype(out_ref.dtype)


def attend_local(query_rows, kv_all, gates_all):
    rows, width = query_rows.shape
    groups, heads, _ = gates_all.shape
    lanes = min(width, 128)
    return pl.pallas_call(
        functools.partial(attend_kernel, heads),
        out_shape=jax.ShapeDtypeStruct((rows, width), jnp.bfloat16),
        in_specs=[pl.BlockSpec(memory_space=pltpu.VMEM)] * 3,
        out_specs=pl.BlockSpec(memory_space=pltpu.VMEM),
        scratch_shapes=[
            pltpu.VMEM((heads, rows, lanes), jnp.bfloat16),
            pltpu.VMEM((heads, rows, 128), jnp.float32),
            pltpu.VMEM((heads, rows, 128), jnp.float32),
            pltpu.VMEM((heads, rows, lanes), jnp.float32),
        ],
        compiler_params=pltpu.CompilerParams(vmem_limit_bytes=48 * 2**20),
        cost_estimate=pl.CostEstimate(
            flops=4 * rows * rows * groups * width * 4,
            bytes_accessed=4 * rows * groups * width,
            transcendentals=rows * rows * groups * heads,
        ),
    )(query_rows, kv_all, gates_all)


def half_of(core, tp):
    return (1 - core) * (tp // 2) + core * (tp % 2)


def partner_of(core, tp):
    return (1 - core) * ((tp + 2) % 4) + core * (tp + 1 - 2 * (tp % 2))


def layer_kernel(
    heads,
    groups,
    q_ref,
    k_ref,
    v_ref,
    gates_ref,
    weight_ref,
    residual_ref,
    index_ref,
    route_ref,
    gain_ref,
    gate_ref,
    up_ref,
    down_ref,
    out_ref,
    place_row_ref,
    facts,
    facts_col,
    gain_row,
    mixed_ref,
    kv_out,
    q_out,
    kv_all,
    q_all,
    gates_all,
    gate_pair,
    packed,
    heads_in,
    masked_q,
    top,
    total,
    summed,
    attended,
    outbox,
    full,
    act,
    made,
    returned,
    blended,
    gate_all,
    up_all,
    down_all,
    wide_rows,
    kv_send,
    side_send,
    kv_recv,
    q_send,
    q_recv,
    head_send,
    head_recv,
    tp_send,
    tp_recv,
    weight_send,
    weight_recv,
    load_sem,
    down_send,
    down_recv,
    out_send,
    out_recv,
    one_send,
    one_recv,
    two_send,
    two_recv,
    back_send,
    back_recv,
):
    rows, width = q_ref.shape
    head_size = width // heads
    lanes = min(width, 128)
    tile = math.gcd(rows, 256)
    tiles = rows // tile
    sp = lax.axis_index("sp")
    tp = lax.axis_index("tp")
    chip = sp // 2
    core = sp % 2
    chips = groups // 2
    sibling = sp + 1 - 2 * core
    beside = tp + 1 - 2 * (tp % 2)
    across = (tp + 2) % 4
    mesh_id = pl.DeviceIdType.MESH
    scale = head_size ** (-0.5)
    lead = (sp + chip) % 2

    def direct(which):
        return pltpu.make_async_remote_copy(
            src_ref=attended.at[tp],
            dst_ref=attended.at[tp],
            send_sem=tp_send.at[which],
            recv_sem=tp_recv.at[which],
            device_id=(sp, beside if which == 0 else across),
            device_id_type=mesh_id,
        )

    def relay(which):
        owner = beside if which == 0 else across
        part = attended.at[owner, pl.ds(which * (rows // 2), rows // 2)]
        return pltpu.make_async_remote_copy(
            src_ref=part,
            dst_ref=part,
            send_sem=tp_send.at[2 + which],
            recv_sem=tp_recv.at[2 + which],
            device_id=(sp, across if which == 0 else beside),
            device_id_type=mesh_id,
        )

    topk = route_ref.shape[0]
    half, columns = outbox.shape[2:]
    capacity = 2 * half
    shards = full.shape[1]
    mine = half_of(core, tp)
    pair = partner_of(core, tp)
    peer = partner_of(1 - core, tp)
    owners = (tp, pair, peer, (beside + 2) % 4)

    def partner(number):
        found, bit = 0, 1
        while bit < groups:
            found = found + bit * (((sp // bit) % 2 + (number // bit) % 2) % 2)
            bit *= 2
        return found

    def send(src, dst, send_sem, recv_sem, device):
        return pltpu.make_async_remote_copy(
            src_ref=src,
            dst_ref=dst,
            send_sem=send_sem,
            recv_sem=recv_sem,
            device_id=device,
            device_id_type=pl.DeviceIdType.MESH,
        )

    def spread(head):
        device = (2 * head + core, tp)
        return [
            send(src, dst.at[sp], kv_send.at[head, n], kv_recv.at[sp, n], device)
            for n, (src, dst) in enumerate(((kv_out.at[head], kv_all), (gates_ref, gates_all)))
        ]

    def sideways(number, own=False):
        return [
            send(src, dst.at[number], side_send.at[number, n], kv_recv.at[number, n], (sibling, tp))
            for n, (src, dst) in enumerate(
                (
                    (kv_all.at[number], kv_all),
                    (gates_ref if own else gates_all.at[number], gates_all),
                )
            )
        ]

    def ask(head):
        return send(
            q_out.at[head],
            q_all.at[chip],
            q_send.at[head],
            q_recv.at[chip],
            (2 * head + lead, tp),
        )

    def answer(slot):
        return send(
            packed.at[slot],
            heads_in.at[chip],
            head_send.at[slot],
            head_recv.at[chip],
            (2 * slot + (slot + core) % 2, tp),
        )

    def dispatch(i, which):
        group = partner(i)
        target = tp if which == 0 else partner_of(group % 2, tp)
        return send(
            outbox.at[i, which],
            full.at[i, which],
            out_send.at[i, which],
            out_recv.at[i, which],
            (group, target),
        )

    def exchange(i, held, send_sem, recv_sem):
        return send(
            held.at[i, pl.ds(0, 2)],
            held.at[i, pl.ds(2, 2)],
            send_sem.at[i],
            recv_sem.at[i],
            (sp, peer),
        )

    def give_back(i, which):
        target = tp if which == 0 else pair
        return send(
            made.at[i, which],
            returned.at[i, mine],
            back_send.at[i, which],
            back_recv.at[i, mine],
            (partner(i), target),
        )

    def arrive_back(i, which):
        return send(
            made.at[i, 0],
            returned.at[i, which],
            back_send.at[i, 0],
            back_recv.at[i, which],
            (sp, pair),
        )

    loads = []
    for n, (src, dst) in enumerate(
        ((gate_ref, gate_all.at[0]), (up_ref, up_all.at[0]), (down_ref, down_all.at[0]))
    ):
        loads.append(pltpu.make_async_copy(src, dst, load_sem.at[n]))
    for load in loads:
        load.start()

    barrier = pltpu.get_barrier_semaphore()
    for i in range(1, groups):
        pl.semaphore_signal(
            barrier, inc=1, device_id=(partner(i), tp), device_id_type=pl.DeviceIdType.MESH
        )
        pl.semaphore_signal(
            barrier,
            inc=1,
            device_id=(partner(i), partner_of(partner(i) % 2, tp)),
            device_id_type=pl.DeviceIdType.MESH,
        )
        pl.semaphore_signal(
            barrier, inc=1, device_id=(partner(i), pair), device_id_type=pl.DeviceIdType.MESH
        )
    for other in (pair, peer):
        pl.semaphore_signal(
            barrier, inc=1, device_id=(sp, other), device_id_type=pl.DeviceIdType.MESH
        )
    pl.semaphore_wait(barrier, 3 * groups - 1)

    down_copy = send(down_ref, down_all.at[1], down_send, down_recv, (sp, pair))
    pieces = weight_send.shape[0]
    depth = gate_ref.shape[0] // pieces

    def weight_copies(number):
        part = pl.ds(pl.multiple_of(number * depth, depth), depth)
        return [
            send(
                src.at[part],
                dst.at[1, part],
                weight_send.at[number, n],
                weight_recv.at[number, n],
                (sp, pair),
            )
            for n, (src, dst) in enumerate(((gate_ref, gate_all), (up_ref, up_all)))
        ]

    def push(number):
        for copy in weight_copies(number):
            copy.start()

    early = pieces - 1 - chips
    for number in range(early):
        push(number)

    lane = lax.broadcasted_iota(jnp.int32, (rows, lanes), 1)
    low = lane < head_size
    short = rows // 2
    short_low = low[:short]

    def turned(wide):
        return pltpu.roll(wide, head_size, 1)

    for g in range(width // lanes):
        part = slice(g * lanes, (g + 1) * lanes)
        wide = q_ref[:, part].astype(jnp.float32) * scale
        tail = turned(wide[short:])
        q_out[2 * g] = jnp.where(short_low, wide[:short], tail).astype(jnp.bfloat16)
        q_out[2 * g + 1] = jnp.where(short_low, tail, wide[:short]).astype(jnp.bfloat16)
    for s in range(1, chips):
        ask(partner(2 * s) // 2).start()

    @pl.when(lead != core)
    def _():
        ask(chip).start()

    @pl.when(lead == core)
    def _():
        q_all[chip] = q_out[chip]

    for g in range(width // lanes):
        part = slice(g * lanes, (g + 1) * lanes)
        keys = k_ref[:, part].astype(jnp.float32)
        values = turned(v_ref[:, part].astype(jnp.float32))
        kv_out[2 * g] = jnp.where(low, keys, values).astype(jnp.bfloat16)
        kv_out[2 * g + 1] = jnp.where(low, values, keys).astype(jnp.bfloat16)
    for s in range(1, chips):
        for copy in spread(partner(2 * s) // 2):
            copy.start()
    kv_all[sp] = kv_out[chip]
    gates_all[sp] = gates_ref[...]
    for copy in sideways(sp, True):
        copy.start()

    first = lax.broadcasted_iota(jnp.int32, (rows, rows), 0)
    second = lax.broadcasted_iota(jnp.int32, (rows, rows), 1)
    number = lax.broadcasted_iota(jnp.int32, (128, rows), 0)
    chosen = [index_ref[k : k + 1, :] ^ sp for k in range(topk)]
    named = jnp.zeros((128, rows), jnp.float32)
    for k in range(topk):
        named = named + jnp.where(number == chosen[k], 1.0, 0.0)
    before = jnp.dot(
        named.astype(jnp.bfloat16),
        jnp.where(first < second, 1.0, 0.0).astype(jnp.bfloat16),
        preferred_element_type=jnp.float32,
    )
    facts[...] = jnp.zeros(facts.shape, jnp.float32)
    for k in range(topk):
        rank = jnp.sum(jnp.where(number == chosen[k], before, 0.0), axis=0, keepdims=True)
        place_row_ref[k : k + 1, :] = chosen[k] * capacity + rank.astype(jnp.int32)
        facts[k : k + 1, :] = (chosen[k] * capacity).astype(jnp.float32) + rank
        facts[topk + k : topk + k + 1, :] = route_ref[k : k + 1, :]
    facts_col[...] = jnp.transpose(facts[...])
    gain_row[...] = gain_ref[...].astype(jnp.float32).reshape(1, -1)

    odd = chip % 2
    key_lane = (lane // head_size) == odd
    short_key = key_lane[:short]
    top[...] = jnp.full(top.shape, -1e30, jnp.float32)
    total[...] = jnp.zeros(total.shape, jnp.float32)
    summed[...] = jnp.zeros(summed.shape, jnp.float32)
    for n in range(chips):

        @pl.when((n != chip) | (lead != core))
        def _():
            send(
                q_out.at[0], q_all.at[n], q_send.at[0], q_recv.at[n], (sibling, tp)
            ).wait_recv()

        part = q_all[n].astype(jnp.float32)
        masked_q[n, :short] = jnp.where(short_key, part, 0.0).astype(jnp.bfloat16)
        masked_q[n, short:] = jnp.where(short_key, turned(part), 0.0).astype(jnp.bfloat16)

    def block(slot, number, offset):
        span_keys = 2 * rows
        for t in range(tiles):
            span = slice(t * tile, (t + 1) * tile)
            count = span_keys if offset is None else offset + (t + 1) * tile
            pair_kv = kv_all[pl.ds(2 * number, 2)].reshape(span_keys, lanes)[:count]
            scores = lax.dot_general(
                masked_q[slot, span],
                pair_kv,
                (((1,), (1,)), ((), ())),
                preferred_element_type=jnp.float32,
            )
            scores = scores - gate_pair[0:1, :count]
            if offset is not None:
                row = lax.broadcasted_iota(jnp.int32, (tile, count), 0) + t * tile + offset
                col = lax.broadcasted_iota(jnp.int32, (tile, count), 1)
                scores = jnp.where(col <= row, scores, -jnp.inf)
            old = top[slot, span]
            new = jnp.maximum(old, jnp.max(scores, axis=1, keepdims=True))
            raised = jnp.exp(scores - new[:, :1])
            shrink = jnp.exp(old - new)
            part = raised[:, :128]
            for c in range(128, count, 128):
                part = part + raised[:, c : c + 128]
            top[slot, span] = new
            total[slot, span] = total[slot, span] * shrink + part
            product = lax.dot_general(
                raised.astype(jnp.bfloat16),
                pair_kv,
                (((1,), (0,)), ((), ())),
                preferred_element_type=jnp.float32,
            )
            summed[slot, span] = summed[slot, span] * shrink[:, :lanes] + product

    def chip_step(s, carry):
        number = partner(2 * s) // 2
        near = 2 * number + core
        push(early + s)

        @pl.when(s > 0)
        def _():
            for copy in sideways(near):
                copy.wait_recv()
            for copy in sideways(near):
                copy.start()

        for copy in sideways(2 * number + 1 - core):
            copy.wait_recv()
        gate_pair[0:1, :rows] = gates_all[2 * number, pl.ds(chip, 1), :]
        gate_pair[0:1, rows:] = gates_all[2 * number + 1, pl.ds(chip, 1), :]

        @pl.when((number + core) % 2 == 0)
        def _():
            block(number, number, 0)

        @pl.when((number + core) % 2 == 1)
        def _():
            block(number, number, rows)

        def full_step(slot, inner):
            block(slot, number, None)
            return inner

        lax.fori_loop(number + 1, chips, full_step, 0)
        return carry

    lax.fori_loop(0, chips, chip_step, 0)

    for n in range(chips):
        result = summed[n] / jnp.sum(total[n], axis=1, keepdims=True)
        folded = jnp.where(short_key, turned(result[short:]), result[:short])
        packed[n] = folded.astype(jnp.bfloat16)

        @pl.when((n != chip) | (lead != core))
        def _():
            answer(n).start()

        @pl.when((n == chip) & (lead == core))
        def _():
            heads_in[chip] = packed[n]

    for n in range(chips):

        @pl.when((n != chip) | (lead != core))
        def _():
            send(
                packed.at[0], heads_in.at[n], head_send.at[0], head_recv.at[n], (sibling, tp)
            ).wait_recv()

    for g in range(width // lanes):
        even = heads_in[2 * g].astype(jnp.float32)
        uneven = heads_in[2 * g + 1].astype(jnp.float32)
        part = slice(g * lanes, (g + 1) * lanes)
        attended[tp, :short, part] = jnp.where(short_low, turned(even), turned(uneven)).astype(
            jnp.bfloat16
        )
        attended[tp, short:, part] = jnp.where(short_low, even, uneven).astype(jnp.bfloat16)
    direct(0).start()
    direct(1).start()

    def projected(owner):
        return jnp.dot(
            attended[owner],
            weight_ref[pl.ds(pl.multiple_of(owner * width, width), width), :],
            preferred_element_type=jnp.float32,
        )

    mixed = residual_ref[...].astype(jnp.float32) + projected(tp)
    for which, owner in ((0, beside), (1, across)):
        direct(which).wait_recv()
        relay(which).start()
        mixed = mixed + projected(owner)
    push(pieces - 1)
    down_copy.start()
    relay(0).wait_recv()
    relay(1).wait_recv()
    mixed_ref[...] = (mixed + projected((beside + 2) % 4)).astype(mixed_ref.dtype)

    def rows_for(i):
        flip = half_of(partner(i) % 2, tp)
        place = lax.broadcasted_iota(jnp.int32, (capacity, rows), 0) + flip * half
        numbers = jnp.where(place >= capacity, place - capacity, place) + i * capacity
        taken = numbers == place_row_ref[0:1, :]
        for k in range(1, topk):
            taken = taken | (numbers == place_row_ref[k : k + 1, :])
        return jnp.dot(
            jnp.where(taken, 1.0, 0.0).astype(jnp.bfloat16),
            mixed_ref[...],
            preferred_element_type=jnp.float32,
        ).astype(jnp.bfloat16)

    def fill(i, carry):
        made_rows = rows_for(i)
        outbox[i, 0] = made_rows[:half]
        outbox[i, 1] = made_rows[half:]
        dispatch(i, 0).start()
        dispatch(i, 1).start()
        return carry

    lax.fori_loop(2, groups, fill, 0)
    lax.fori_loop(1, 2, fill, 0)
    first = rows_for(0)
    full[0, 0] = first[:half]
    outbox[0, 1] = first[half:]
    dispatch(0, 1).start()
    blended[...] = mixed_ref[...].astype(jnp.float32)
    for load in loads:
        load.wait()
    for number in range(pieces):
        for copy in weight_copies(number):
            copy.wait_recv()

    def hidden(i):
        square = jnp.zeros((half, 1), jnp.float32)
        for j in range(shards):
            wide = full[i, j].astype(jnp.float32)
            square = square + jnp.sum(wide * wide, axis=1, keepdims=True)
        factor = lax.rsqrt(square / (shards * columns) + NORM_EPS)
        for j in range(shards):
            span = pl.ds(pl.multiple_of(owners[j] * columns, columns), columns)
            gain = gain_row[0:1, span]
            wide_rows[:, span] = (full[i, j].astype(jnp.float32) * factor * gain).astype(
                jnp.bfloat16
            )
        for c in range(2):
            gate_input = jnp.dot(
                wide_rows[...], gate_all[c], preferred_element_type=jnp.float32
            )
            linear_input = jnp.dot(wide_rows[...], up_all[c], preferred_element_type=jnp.float32)
            gate_cut = jnp.minimum(gate_input, CLAMP_LIMIT)
            linear_cut = jnp.clip(linear_input, -CLAMP_LIMIT, CLAMP_LIMIT)
            act[i, c] = (
                gate_cut * jax.nn.sigmoid(SILU_ALPHA * gate_cut) * (linear_cut + 1.0)
            ).astype(jnp.bfloat16)

    def output_rows(i, c):
        return jnp.dot(
            wide_rows[...], down_all[c], preferred_element_type=jnp.float32
        ).astype(jnp.bfloat16)

    def step(i, carry):
        @pl.when(i < groups)
        def _():
            b = (i + 2) % groups

            @pl.when(b > 0)
            def _():
                dispatch(b, 0).wait_recv()

            dispatch(b, 1).wait_recv()
            exchange(b, full, one_send, one_recv).start()

        @pl.when((i >= 1) & (i < groups + 1))
        def _():
            b = (i + 1) % groups
            exchange(b, full, one_send, one_recv).wait_recv()
            hidden(b)
            exchange(b, act, two_send, two_recv).start()

        @pl.when((i >= 2) & (i < groups + 2))
        def _():
            b = i % groups

            @pl.when(i == 2)
            def _():
                down_copy.wait_recv()

            exchange(b, act, two_send, two_recv).wait_recv()
            for j in range(shards):
                span = pl.ds(pl.multiple_of(owners[j] * columns, columns), columns)
                wide_rows[:, span] = act[b, j]
            made[b, 1] = output_rows(b, 1)
            give_back(b, 1).start()
            result = output_rows(b, 0)

            @pl.when(b == 0)
            def _():
                returned[0, mine] = result

            @pl.when(b > 0)
            def _():
                made[b, 0] = result
                give_back(b, 0).start()

        @pl.when(i >= 3)
        def _():
            b = (i - 1) % groups

            @pl.when(b == 0)
            def _():
                arrive_back(0, 1 - mine).wait_recv()

            @pl.when(b > 0)
            def _():
                arrive_back(b, 0).wait_recv()
                arrive_back(b, 1).wait_recv()

            numbers = lax.broadcasted_iota(jnp.int32, (rows, capacity), 1) + b * capacity
            wide_numbers = numbers.astype(jnp.float32)
            added = blended[...]
            rows_back = returned[b].reshape(capacity, columns)
            for k in range(topk):
                taken = jnp.where(wide_numbers == facts_col[:, k : k + 1], 1.0, 0.0)
                picked = jnp.dot(
                    taken.astype(jnp.bfloat16), rows_back, preferred_element_type=jnp.float32
                )
                added = added + facts_col[:, topk + k : topk + k + 1] * picked
            blended[...] = added

        return carry

    lax.fori_loop(0, groups + 3, step, 0)
    out_ref[...] = blended[...].astype(out_ref.dtype)

    def settle(i, carry):
        @pl.when(i > 0)
        def _():
            dispatch(i, 0).wait_send()
            give_back(i, 0).wait_send()

        dispatch(i, 1).wait_send()
        give_back(i, 1).wait_send()
        exchange(i, full, one_send, one_recv).wait_send()
        exchange(i, act, two_send, two_recv).wait_send()
        return carry

    lax.fori_loop(0, groups, settle, 0)
    down_copy.wait_send()

    for which in range(2):
        direct(which).wait_send()
        relay(which).wait_send()

    for s in range(1, chips):
        ask(partner(2 * s) // 2).wait_send()
        for copy in spread(partner(2 * s) // 2):
            copy.wait_send()
        for copy in sideways(2 * (partner(2 * s) // 2) + core):
            copy.wait_send()
    for copy in sideways(sp, True):
        copy.wait_send()

    @pl.when(lead != core)
    def _():
        ask(chip).wait_send()

    for n in range(chips):

        @pl.when((n != chip) | (lead != core))
        def _():
            answer(n).wait_send()

    for number in range(pieces):
        for copy in weight_copies(number):
            copy.wait_send()


def layer_fused(
    query_rows,
    key_rows,
    value_rows,
    gates,
    output_weight,
    residual,
    index,
    route_weights,
    norm_gain,
    gate_weight,
    up_weight,
    down_weight,
    capacity,
):
    rows, width = query_rows.shape
    columns = residual.shape[1]
    heads = gates.shape[0]
    groups = lax.axis_size("sp")
    shards = lax.axis_size("tp")
    lanes = min(width, 128)
    depth, units = gate_weight.shape
    half = capacity // 2
    dma = pltpu.SemaphoreType.DMA
    return pl.pallas_call(
        functools.partial(layer_kernel, heads, groups),
        out_shape=jax.ShapeDtypeStruct(residual.shape, jnp.bfloat16),
        in_specs=[pl.BlockSpec(memory_space=pltpu.VMEM)] * 9
        + [pl.BlockSpec(memory_space=pl.ANY)] * 3,
        out_specs=pl.BlockSpec(memory_space=pltpu.VMEM),
        scratch_shapes=[
            pltpu.VMEM(index.shape, jnp.int32),
            pltpu.VMEM((8, rows), jnp.float32),
            pltpu.VMEM((rows, 8), jnp.float32),
            pltpu.VMEM((1, shards * columns), jnp.float32),
            pltpu.VMEM((rows, columns), jnp.bfloat16),
            pltpu.VMEM((heads, rows, lanes), jnp.bfloat16),
            pltpu.VMEM((heads, rows // 2, lanes), jnp.bfloat16),
            pltpu.VMEM((groups, rows, lanes), jnp.bfloat16),
            pltpu.VMEM((heads, rows // 2, lanes), jnp.bfloat16),
            pltpu.VMEM((groups, heads, rows), jnp.float32),
            pltpu.VMEM((8, 2 * rows), jnp.float32),
            pltpu.VMEM((heads, rows // 2, lanes), jnp.bfloat16),
            pltpu.VMEM((heads, rows // 2, lanes), jnp.bfloat16),
            pltpu.VMEM((heads, rows, lanes), jnp.bfloat16),
            pltpu.VMEM((heads, rows, 128), jnp.float32),
            pltpu.VMEM((heads, rows, 128), jnp.float32),
            pltpu.VMEM((heads, rows, lanes), jnp.float32),
            pltpu.VMEM((4, rows, width), jnp.bfloat16),
            pltpu.VMEM((groups, 2, half, columns), jnp.bfloat16),
            pltpu.VMEM((groups, shards, half, columns), jnp.bfloat16),
            pltpu.VMEM((groups, shards, half, units), jnp.bfloat16),
            pltpu.VMEM((groups, 2, half, columns), jnp.bfloat16),
            pltpu.VMEM((groups, 2, half, columns), jnp.bfloat16),
            pltpu.VMEM((rows, columns), jnp.float32),
            pltpu.VMEM((2, depth, units), jnp.bfloat16),
            pltpu.VMEM((2, depth, units), jnp.bfloat16),
            pltpu.VMEM((2, shards * units, columns), jnp.bfloat16),
            pltpu.VMEM((half, shards * columns), jnp.bfloat16),
            dma((heads, 2)),
            dma((groups, 2)),
            dma((groups, 2)),
            dma((heads,)),
            dma((heads,)),
            dma((heads,)),
            dma((heads,)),
            dma((4,)),
            dma((4,)),
            dma((8, 2)),
            dma((8, 2)),
            dma((3,)),
            dma(()),
            dma(()),
            dma((groups, 2)),
            dma((groups, 2)),
            dma((groups,)),
            dma((groups,)),
            dma((groups,)),
            dma((groups,)),
            dma((groups, 2)),
            dma((groups, 2)),
        ],
        compiler_params=pltpu.CompilerParams(
            collective_id=1, has_side_effects=True, vmem_limit_bytes=67043328
        ),
    )(
        query_rows,
        key_rows,
        value_rows,
        gates,
        output_weight,
        residual,
        index,
        route_weights,
        norm_gain,
        gate_weight,
        up_weight,
        down_weight,
    )


def body(
    query_rows,
    key_rows,
    value_rows,
    cum_gates,
    residual,
    output_weight,
    norm_gain,
    expert_index,
    route_weights,
    gate_weight,
    up_weight,
    down_weight,
):
    rows, columns = residual.shape
    topk = expert_index.shape[1]
    local_experts = gate_weight.shape[0]
    groups = lax.axis_size("sp")
    experts = local_experts * groups
    capacity = 2 * rows * topk // experts
    heads = cum_gates.shape[1]

    if (
        lax.axis_size("tp") == 4
        and local_experts == 1
        and groups == 8
        and heads == 4
        and query_rows.shape[1] == heads * 64
    ):
        return layer_fused(
            query_rows,
            key_rows,
            value_rows,
            cum_gates.T,
            output_weight,
            residual,
            expert_index.T,
            route_weights.T,
            norm_gain,
            gate_weight[0],
            up_weight[0],
            down_weight[0],
            capacity,
        )

    both = jnp.concatenate([key_rows, value_rows], axis=1)
    kv_all = lax.all_gather(both, "sp", axis=0, tiled=True)
    gates_all = lax.all_gather(cum_gates.T, "sp", axis=0, tiled=False)

    chosen = expert_index.reshape(rows * topk)
    matches = (chosen[:, None] == jnp.arange(experts, dtype=jnp.int32)[None, :]).astype(jnp.int32)
    rank = jnp.sum((jnp.cumsum(matches, axis=0) - matches) * matches, axis=1)
    chosen, rank, gates_all = lax.optimization_barrier((chosen, rank, gates_all))

    attended = attend_local(query_rows, kv_all, gates_all)
    projected = jnp.dot(
        lax.all_gather(attended, "tp", axis=1, tiled=True),
        output_weight,
        preferred_element_type=jnp.float32,
    )
    mixed = (residual.astype(jnp.float32) + projected).astype(jnp.bfloat16)

    chunks = math.gcd(capacity, CHUNKS)
    piece = capacity // chunks
    places = chosen * piece + rank % piece
    inside = rank // piece
    blended = jnp.zeros((rows, columns), jnp.float32)
    for c in range(chunks):
        place = jnp.where(inside == c, places, -1).reshape(rows, topk)
        numbers = jnp.arange(experts * piece, dtype=jnp.int32)
        taken = numbers[:, None] == place[:, 0][None, :]
        for k in range(1, topk):
            taken = taken | (numbers[:, None] == place[:, k][None, :])
        outgoing = jnp.dot(
            taken.astype(jnp.bfloat16), mixed, preferred_element_type=jnp.float32
        ).astype(jnp.bfloat16)
        arrived = lax.all_to_all(
            outgoing.reshape(experts, piece, columns), "sp", split_axis=0, concat_axis=0, tiled=True
        )
        grouped = arrived.reshape(groups, local_experts, piece, columns)
        normed = normalize(lax.all_gather(grouped, "tp", axis=3, tiled=True), norm_gain)
        gate_input = jnp.einsum(
            "seid,edf->seif", normed, gate_weight, preferred_element_type=jnp.float32
        )
        linear_input = jnp.einsum(
            "seid,edf->seif", normed, up_weight, preferred_element_type=jnp.float32
        )
        gate_cut = jnp.minimum(gate_input, CLAMP_LIMIT)
        linear_cut = jnp.clip(linear_input, -CLAMP_LIMIT, CLAMP_LIMIT)
        activated = (gate_cut * jax.nn.sigmoid(SILU_ALPHA * gate_cut) * (linear_cut + 1.0)).astype(
            jnp.bfloat16
        )
        produced = jnp.einsum(
            "seif,efc->seic",
            lax.all_gather(activated, "tp", axis=3, tiled=True),
            down_weight,
            preferred_element_type=jnp.float32,
        ).astype(jnp.bfloat16)
        returned = lax.all_to_all(
            produced.reshape(experts, piece, columns), "sp", split_axis=0, concat_axis=0, tiled=True
        ).reshape(experts * piece, columns)
        for k in range(topk):
            picked = jnp.dot(
                (place[:, k][:, None] == numbers[None, :]).astype(jnp.bfloat16),
                returned,
                preferred_element_type=jnp.float32,
            )
            blended = blended + route_weights[:, k : k + 1] * picked
    return (mixed.astype(jnp.float32) + blended).astype(jnp.bfloat16)


def solution(mesh):
    placed = (
        P("sp", "tp"),
        P("sp", "tp"),
        P("sp", "tp"),
        P("sp", "tp"),
        P("sp", "tp"),
        P(None, "tp"),
        P(),
        P("sp", None),
        P("sp", None),
        P("sp", None, "tp"),
        P("sp", None, "tp"),
        P("sp", None, "tp"),
    )
    return jax.shard_map(body, mesh=mesh, in_specs=placed, out_specs=P("sp", "tp"), check_vma=False)
```

```python
import functools
import math

import jax
import jax.numpy as jnp
from jax import lax
from jax.experimental import pallas as pl
from jax.experimental.pallas import tpu as pltpu
from jax.sharding import PartitionSpec as P

NORM_EPS = 1e-06
CLAMP_LIMIT = 7.0
SILU_ALPHA = 1.702
CHUNKS = 1


def normalize(rows, norm_gain):
    wide = rows.astype(jnp.float32)
    factor = lax.rsqrt(jnp.mean(wide * wide, axis=-1, keepdims=True) + NORM_EPS)
    return (wide * factor * norm_gain.astype(jnp.float32)).astype(jnp.bfloat16)


def attend_kernel(heads, q_ref, kv_ref, gates_ref, out_ref, masked_q, top, total, summed):
    rows, width = q_ref.shape
    head_size = width // heads
    lanes = min(width, 128)
    tile = math.gcd(rows, 256)
    tiles = rows // tile
    me = lax.axis_index("sp")
    scale = head_size ** (-0.5)
    lane = lax.broadcasted_iota(jnp.int32, (rows, lanes), 1)
    for h in range(heads):
        group, inside = divmod(h * head_size, lanes)
        part = q_ref[:, group * lanes : (group + 1) * lanes].astype(jnp.float32) * scale
        keep = (lane >= inside) & (lane < inside + head_size)
        masked_q[h] = jnp.where(keep, part, 0.0).astype(jnp.bfloat16)
    top[...] = jnp.full(top.shape, -1e30, jnp.float32)
    total[...] = jnp.zeros(total.shape, jnp.float32)
    summed[...] = jnp.zeros(summed.shape, jnp.float32)

    def block(number, diagonal):
        base = pl.multiple_of(number * rows, rows)
        for h in range(heads):
            group = h * head_size // lanes
            keys = kv_ref[pl.ds(base, rows), group * lanes : (group + 1) * lanes]
            values = kv_ref[pl.ds(base, rows), width + group * lanes : width + (group + 1) * lanes]
            gates = gates_ref[number, h : h + 1, :]
            for t in range(tiles):
                span = slice(t * tile, (t + 1) * tile)
                count = (t + 1) * tile if diagonal else rows
                scores = lax.dot_general(
                    masked_q[h, span],
                    keys[:count],
                    (((1,), (1,)), ((), ())),
                    preferred_element_type=jnp.float32,
                )
                scores = scores - gates[:, :count]
                if diagonal:
                    row = lax.broadcasted_iota(jnp.int32, (tile, count), 0) + t * tile
                    col = lax.broadcasted_iota(jnp.int32, (tile, count), 1)
                    scores = jnp.where(col <= row, scores, -jnp.inf)
                old = top[h, span]
                new = jnp.maximum(old, jnp.max(scores, axis=1, keepdims=True))
                raised = jnp.exp(scores - new[:, :1])
                shrink = jnp.exp(old - new)
                part = raised[:, :128]
                for c in range(128, count, 128):
                    part = part + raised[:, c : c + 128]
                top[h, span] = new
                total[h, span] = total[h, span] * shrink + part
                product = lax.dot_general(
                    raised.astype(jnp.bfloat16),
                    values[:count],
                    (((1,), (0,)), ((), ())),
                    preferred_element_type=jnp.float32,
                )
                summed[h, span] = summed[h, span] * shrink[:, :lanes] + product

    def step(number, carry):
        block(number, False)
        return carry

    lax.fori_loop(0, me, step, 0)
    block(me, True)
    for g in range(width // lanes):
        result = jnp.zeros((rows, lanes), jnp.float32)
        for h in range(heads):
            if h * head_size // lanes == g:
                inside = h * head_size % lanes
                keep = (lane >= inside) & (lane < inside + head_size)
                whole = jnp.sum(total[h], axis=1, keepdims=True)
                result = jnp.where(keep, summed[h] / whole, result)
        out_ref[:, g * lanes : (g + 1) * lanes] = result.astype(out_ref.dtype)


def attend_local(query_rows, kv_all, gates_all):
    rows, width = query_rows.shape
    groups, heads, _ = gates_all.shape
    lanes = min(width, 128)
    return pl.pallas_call(
        functools.partial(attend_kernel, heads),
        out_shape=jax.ShapeDtypeStruct((rows, width), jnp.bfloat16),
        in_specs=[pl.BlockSpec(memory_space=pltpu.VMEM)] * 3,
        out_specs=pl.BlockSpec(memory_space=pltpu.VMEM),
        scratch_shapes=[
            pltpu.VMEM((heads, rows, lanes), jnp.bfloat16),
            pltpu.VMEM((heads, rows, 128), jnp.float32),
            pltpu.VMEM((heads, rows, 128), jnp.float32),
            pltpu.VMEM((heads, rows, lanes), jnp.float32),
        ],
        compiler_params=pltpu.CompilerParams(vmem_limit_bytes=48 * 2**20),
        cost_estimate=pl.CostEstimate(
            flops=4 * rows * rows * groups * width * 4,
            bytes_accessed=4 * rows * groups * width,
            transcendentals=rows * rows * groups * heads,
        ),
    )(query_rows, kv_all, gates_all)


def half_of(core, tp):
    return (1 - core) * (tp // 2) + core * (tp % 2)


def partner_of(core, tp):
    return (1 - core) * ((tp + 2) % 4) + core * (tp + 1 - 2 * (tp % 2))


def layer_kernel(
    heads,
    groups,
    q_ref,
    k_ref,
    v_ref,
    gates_ref,
    weight_ref,
    residual_ref,
    index_ref,
    route_ref,
    gain_ref,
    gate_ref,
    up_ref,
    down_ref,
    out_ref,
    place_row_ref,
    facts,
    facts_col,
    gain_row,
    mixed_ref,
    kv_out,
    q_out,
    kv_all,
    q_all,
    gates_all,
    gate_pair,
    packed,
    heads_in,
    masked_q,
    top,
    total,
    summed,
    attended,
    outbox,
    full,
    act,
    made,
    returned,
    blended,
    gate_all,
    up_all,
    down_all,
    wide_rows,
    kv_send,
    side_send,
    kv_recv,
    q_send,
    q_recv,
    head_send,
    head_recv,
    tp_send,
    tp_recv,
    weight_send,
    weight_recv,
    load_sem,
    down_send,
    down_recv,
    out_send,
    out_recv,
    one_send,
    one_recv,
    two_send,
    two_recv,
    back_send,
    back_recv,
):
    rows, width = q_ref.shape
    head_size = width // heads
    lanes = min(width, 128)
    tile = math.gcd(rows, 256)
    tiles = rows // tile
    sp = lax.axis_index("sp")
    tp = lax.axis_index("tp")
    chip = sp // 2
    core = sp % 2
    chips = groups // 2
    sibling = sp + 1 - 2 * core
    beside = tp + 1 - 2 * (tp % 2)
    across = (tp + 2) % 4
    mesh_id = pl.DeviceIdType.MESH
    scale = head_size ** (-0.5)
    lead = (sp + chip) % 2

    def direct(which):
        return pltpu.make_async_remote_copy(
            src_ref=attended.at[tp],
            dst_ref=attended.at[tp],
            send_sem=tp_send.at[which],
            recv_sem=tp_recv.at[which],
            device_id=(sp, beside if which == 0 else across),
            device_id_type=mesh_id,
        )

    def relay(which):
        owner = beside if which == 0 else across
        part = attended.at[owner, pl.ds(which * (rows // 2), rows // 2)]
        return pltpu.make_async_remote_copy(
            src_ref=part,
            dst_ref=part,
            send_sem=tp_send.at[2 + which],
            recv_sem=tp_recv.at[2 + which],
            device_id=(sp, across if which == 0 else beside),
            device_id_type=mesh_id,
        )

    topk = route_ref.shape[0]
    half, columns = outbox.shape[2:]
    capacity = 2 * half
    shards = full.shape[1]
    mine = half_of(core, tp)
    pair = partner_of(core, tp)
    peer = partner_of(1 - core, tp)
    owners = (tp, pair, peer, (beside + 2) % 4)

    def partner(number):
        found, bit = 0, 1
        while bit < groups:
            found = found + bit * (((sp // bit) % 2 + (number // bit) % 2) % 2)
            bit *= 2
        return found

    def send(src, dst, send_sem, recv_sem, device):
        return pltpu.make_async_remote_copy(
            src_ref=src,
            dst_ref=dst,
            send_sem=send_sem,
            recv_sem=recv_sem,
            device_id=device,
            device_id_type=pl.DeviceIdType.MESH,
        )

    def spread(head):
        device = (2 * head + core, tp)
        return [
            send(src, dst.at[sp], kv_send.at[head, n], kv_recv.at[sp, n], device)
            for n, (src, dst) in enumerate(((kv_out.at[head], kv_all), (gates_ref, gates_all)))
        ]

    def sideways(number, own=False):
        return [
            send(src, dst.at[number], side_send.at[number, n], kv_recv.at[number, n], (sibling, tp))
            for n, (src, dst) in enumerate(
                (
                    (kv_all.at[number], kv_all),
                    (gates_ref if own else gates_all.at[number], gates_all),
                )
            )
        ]

    def ask(head):
        return send(
            q_out.at[head],
            q_all.at[chip],
            q_send.at[head],
            q_recv.at[chip],
            (2 * head + lead, tp),
        )

    def answer(slot):
        return send(
            packed.at[slot],
            heads_in.at[chip],
            head_send.at[slot],
            head_recv.at[chip],
            (2 * slot + (slot + core) % 2, tp),
        )

    def dispatch(i, which):
        group = partner(i)
        target = tp if which == 0 else partner_of(group % 2, tp)
        return send(
            outbox.at[i, which],
            full.at[i, which],
            out_send.at[i, which],
            out_recv.at[i, which],
            (group, target),
        )

    def exchange(i, held, send_sem, recv_sem):
        return send(
            held.at[i, pl.ds(0, 2)],
            held.at[i, pl.ds(2, 2)],
            send_sem.at[i],
            recv_sem.at[i],
            (sp, peer),
        )

    def give_back(i, which):
        target = tp if which == 0 else pair
        return send(
            made.at[i, which],
            returned.at[i, mine],
            back_send.at[i, which],
            back_recv.at[i, mine],
            (partner(i), target),
        )

    def arrive_back(i, which):
        return send(
            made.at[i, 0],
            returned.at[i, which],
            back_send.at[i, 0],
            back_recv.at[i, which],
            (sp, pair),
        )

    loads = []
    for n, (src, dst) in enumerate(
        ((gate_ref, gate_all.at[0]), (up_ref, up_all.at[0]), (down_ref, down_all.at[0]))
    ):
        loads.append(pltpu.make_async_copy(src, dst, load_sem.at[n]))
    for load in loads:
        load.start()

    barrier = pltpu.get_barrier_semaphore()
    for i in range(1, groups):
        pl.semaphore_signal(
            barrier, inc=1, device_id=(partner(i), tp), device_id_type=pl.DeviceIdType.MESH
        )
        pl.semaphore_signal(
            barrier,
            inc=1,
            device_id=(partner(i), partner_of(partner(i) % 2, tp)),
            device_id_type=pl.DeviceIdType.MESH,
        )
        pl.semaphore_signal(
            barrier, inc=1, device_id=(partner(i), pair), device_id_type=pl.DeviceIdType.MESH
        )
    for other in (pair, peer):
        pl.semaphore_signal(
            barrier, inc=1, device_id=(sp, other), device_id_type=pl.DeviceIdType.MESH
        )
    pl.semaphore_wait(barrier, 3 * groups - 1)

    down_copy = send(down_ref, down_all.at[1], down_send, down_recv, (sp, pair))
    pieces = weight_send.shape[0]
    depth = gate_ref.shape[0] // pieces

    def weight_copies(number):
        part = pl.ds(pl.multiple_of(number * depth, depth), depth)
        return [
            send(
                src.at[part],
                dst.at[1, part],
                weight_send.at[number, n],
                weight_recv.at[number, n],
                (sp, pair),
            )
            for n, (src, dst) in enumerate(((gate_ref, gate_all), (up_ref, up_all)))
        ]

    def push(number):
        for copy in weight_copies(number):
            copy.start()

    early = pieces - 1 - chips
    for number in range(early):
        push(number)

    lane = lax.broadcasted_iota(jnp.int32, (rows, lanes), 1)
    low = lane < head_size
    short = rows // 2
    short_low = low[:short]

    def turned(wide):
        return pltpu.roll(wide, head_size, 1)

    for g in range(width // lanes):
        part = slice(g * lanes, (g + 1) * lanes)
        wide = q_ref[:, part].astype(jnp.float32) * scale
        tail = turned(wide[short:])
        q_out[2 * g] = jnp.where(short_low, wide[:short], tail).astype(jnp.bfloat16)
        q_out[2 * g + 1] = jnp.where(short_low, tail, wide[:short]).astype(jnp.bfloat16)
    for s in range(1, chips):
        ask(partner(2 * s) // 2).start()

    @pl.when(lead != core)
    def _():
        ask(chip).start()

    @pl.when(lead == core)
    def _():
        q_all[chip] = q_out[chip]

    for g in range(width // lanes):
        part = slice(g * lanes, (g + 1) * lanes)
        keys = k_ref[:, part].astype(jnp.float32)
        values = turned(v_ref[:, part].astype(jnp.float32))
        kv_out[2 * g] = jnp.where(low, keys, values).astype(jnp.bfloat16)
        kv_out[2 * g + 1] = jnp.where(low, values, keys).astype(jnp.bfloat16)
    for s in range(1, chips):
        for copy in spread(partner(2 * s) // 2):
            copy.start()
    kv_all[sp] = kv_out[chip]
    gates_all[sp] = gates_ref[...]
    for copy in sideways(sp, True):
        copy.start()

    first = lax.broadcasted_iota(jnp.int32, (rows, rows), 0)
    second = lax.broadcasted_iota(jnp.int32, (rows, rows), 1)
    number = lax.broadcasted_iota(jnp.int32, (128, rows), 0)
    chosen = [index_ref[k : k + 1, :] ^ sp for k in range(topk)]
    named = jnp.zeros((128, rows), jnp.float32)
    for k in range(topk):
        named = named + jnp.where(number == chosen[k], 1.0, 0.0)
    before = jnp.dot(
        named.astype(jnp.bfloat16),
        jnp.where(first < second, 1.0, 0.0).astype(jnp.bfloat16),
        preferred_element_type=jnp.float32,
    )
    facts[...] = jnp.zeros(facts.shape, jnp.float32)
    for k in range(topk):
        rank = jnp.sum(jnp.where(number == chosen[k], before, 0.0), axis=0, keepdims=True)
        place_row_ref[k : k + 1, :] = chosen[k] * capacity + rank.astype(jnp.int32)
        facts[k : k + 1, :] = (chosen[k] * capacity).astype(jnp.float32) + rank
        facts[topk + k : topk + k + 1, :] = route_ref[k : k + 1, :]
    facts_col[...] = jnp.transpose(facts[...])
    gain_row[...] = gain_ref[...].astype(jnp.float32).reshape(1, -1)

    odd = chip % 2
    key_lane = (lane // head_size) == odd
    short_key = key_lane[:short]
    top[...] = jnp.full(top.shape, -1e30, jnp.float32)
    total[...] = jnp.zeros(total.shape, jnp.float32)
    summed[...] = jnp.zeros(summed.shape, jnp.float32)
    for n in range(chips):

        @pl.when((n != chip) | (lead != core))
        def _():
            send(
                q_out.at[0], q_all.at[n], q_send.at[0], q_recv.at[n], (sibling, tp)
            ).wait_recv()

        part = q_all[n].astype(jnp.float32)
        masked_q[n, :short] = jnp.where(short_key, part, 0.0).astype(jnp.bfloat16)
        masked_q[n, short:] = jnp.where(short_key, turned(part), 0.0).astype(jnp.bfloat16)

    def block(slot, number, offset):
        span_keys = 2 * rows
        for t in range(tiles):
            span = slice(t * tile, (t + 1) * tile)
            count = span_keys if offset is None else offset + (t + 1) * tile
            pair_kv = kv_all[pl.ds(2 * number, 2)].reshape(span_keys, lanes)[:count]
            scores = lax.dot_general(
                masked_q[slot, span],
                pair_kv,
                (((1,), (1,)), ((), ())),
                preferred_element_type=jnp.float32,
            )
            scores = scores - gate_pair[0:1, :count]
            if offset is not None:
                row = lax.broadcasted_iota(jnp.int32, (tile, count), 0) + t * tile + offset
                col = lax.broadcasted_iota(jnp.int32, (tile, count), 1)
                scores = jnp.where(col <= row, scores, -jnp.inf)
            old = top[slot, span]
            new = jnp.maximum(old, jnp.max(scores, axis=1, keepdims=True))
            raised = jnp.exp(scores - new[:, :1])
            shrink = jnp.exp(old - new)
            part = raised[:, :128]
            for c in range(128, count, 128):
                part = part + raised[:, c : c + 128]
            top[slot, span] = new
            total[slot, span] = total[slot, span] * shrink + part
            product = lax.dot_general(
                raised.astype(jnp.bfloat16),
                pair_kv,
                (((1,), (0,)), ((), ())),
                preferred_element_type=jnp.float32,
            )
            summed[slot, span] = summed[slot, span] * shrink[:, :lanes] + product

    def chip_step(s, carry):
        number = partner(2 * s) // 2
        near = 2 * number + core
        push(early + s)

        @pl.when(s > 0)
        def _():
            for copy in sideways(near):
                copy.wait_recv()
            for copy in sideways(near):
                copy.start()

        for copy in sideways(2 * number + 1 - core):
            copy.wait_recv()
        gate_pair[0:1, :rows] = gates_all[2 * number, pl.ds(chip, 1), :]
        gate_pair[0:1, rows:] = gates_all[2 * number + 1, pl.ds(chip, 1), :]

        @pl.when((number + core) % 2 == 0)
        def _():
            block(number, number, 0)

        @pl.when((number + core) % 2 == 1)
        def _():
            block(number, number, rows)

        def full_step(slot, inner):
            block(slot, number, None)
            return inner

        lax.fori_loop(number + 1, chips, full_step, 0)
        return carry

    lax.fori_loop(0, chips, chip_step, 0)

    for n in range(chips):
        result = summed[n] / jnp.sum(total[n], axis=1, keepdims=True)
        folded = jnp.where(short_key, turned(result[short:]), result[:short])
        packed[n] = folded.astype(jnp.bfloat16)

        @pl.when((n != chip) | (lead != core))
        def _():
            answer(n).start()

        @pl.when((n == chip) & (lead == core))
        def _():
            heads_in[chip] = packed[n]

    for n in range(chips):

        @pl.when((n != chip) | (lead != core))
        def _():
            send(
                packed.at[0], heads_in.at[n], head_send.at[0], head_recv.at[n], (sibling, tp)
            ).wait_recv()

    for g in range(width // lanes):
        even = heads_in[2 * g].astype(jnp.float32)
        uneven = heads_in[2 * g + 1].astype(jnp.float32)
        part = slice(g * lanes, (g + 1) * lanes)
        attended[tp, :short, part] = jnp.where(short_low, turned(even), turned(uneven)).astype(
            jnp.bfloat16
        )
        attended[tp, short:, part] = jnp.where(short_low, even, uneven).astype(jnp.bfloat16)
    direct(0).start()
    direct(1).start()

    def projected(owner):
        return jnp.dot(
            attended[owner],
            weight_ref[pl.ds(pl.multiple_of(owner * width, width), width), :],
            preferred_element_type=jnp.float32,
        )

    mixed = residual_ref[...].astype(jnp.float32) + projected(tp)
    for which, owner in ((0, beside), (1, across)):
        direct(which).wait_recv()
        relay(which).start()
        mixed = mixed + projected(owner)
    for number in range(early + chips, pieces):
        push(number)
    down_copy.start()
    relay(0).wait_recv()
    relay(1).wait_recv()
    mixed_ref[...] = (mixed + projected((beside + 2) % 4)).astype(mixed_ref.dtype)

    def rows_for(i):
        flip = half_of(partner(i) % 2, tp)
        place = lax.broadcasted_iota(jnp.int32, (capacity, rows), 0) + flip * half
        numbers = jnp.where(place >= capacity, place - capacity, place) + i * capacity
        taken = numbers == place_row_ref[0:1, :]
        for k in range(1, topk):
            taken = taken | (numbers == place_row_ref[k : k + 1, :])
        return jnp.dot(
            jnp.where(taken, 1.0, 0.0).astype(jnp.bfloat16),
            mixed_ref[...],
            preferred_element_type=jnp.float32,
        ).astype(jnp.bfloat16)

    def fill(i, carry):
        made_rows = rows_for(i)
        outbox[i, 0] = made_rows[:half]
        outbox[i, 1] = made_rows[half:]
        dispatch(i, 0).start()
        dispatch(i, 1).start()
        return carry

    def label(n):
        return 2 * (lax.shift_right_logical(30, 2 * (n // 2)) % chips) + n % 2

    def fill_next(n, carry):
        return fill(label(n), carry)

    lax.fori_loop(0, groups - 2, fill_next, 0)
    lax.fori_loop(1, 2, fill, 0)
    first = rows_for(0)
    full[0, 0] = first[:half]
    outbox[0, 1] = first[half:]
    dispatch(0, 1).start()
    blended[...] = mixed_ref[...].astype(jnp.float32)

    def hidden(i):
        square = jnp.zeros((half, 1), jnp.float32)
        for j in range(shards):
            wide = full[i, j].astype(jnp.float32)
            square = square + jnp.sum(wide * wide, axis=1, keepdims=True)
        factor = lax.rsqrt(square / (shards * columns) + NORM_EPS)
        for j in range(shards):
            span = pl.ds(pl.multiple_of(owners[j] * columns, columns), columns)
            gain = gain_row[0:1, span]
            wide_rows[:, span] = (full[i, j].astype(jnp.float32) * factor * gain).astype(
                jnp.bfloat16
            )
        for c in range(2):
            gate_input = jnp.dot(
                wide_rows[...], gate_all[c], preferred_element_type=jnp.float32
            )
            linear_input = jnp.dot(wide_rows[...], up_all[c], preferred_element_type=jnp.float32)
            gate_cut = jnp.minimum(gate_input, CLAMP_LIMIT)
            linear_cut = jnp.clip(linear_input, -CLAMP_LIMIT, CLAMP_LIMIT)
            act[i, c] = (
                gate_cut * jax.nn.sigmoid(SILU_ALPHA * gate_cut) * (linear_cut + 1.0)
            ).astype(jnp.bfloat16)

    def output_rows(i, c):
        return jnp.dot(
            wide_rows[...], down_all[c], preferred_element_type=jnp.float32
        ).astype(jnp.bfloat16)

    def step(i, carry):
        @pl.when(i < groups)
        def _():
            b = label(i)

            @pl.when(b > 0)
            def _():
                dispatch(b, 0).wait_recv()

            dispatch(b, 1).wait_recv()
            exchange(b, full, one_send, one_recv).start()

        @pl.when((i >= 2) & (i < groups + 2))
        def _():
            b = label(i - 2)

            @pl.when(i == 2)
            def _():
                for load in loads:
                    load.wait()
                for number in range(pieces):
                    for copy in weight_copies(number):
                        copy.wait_recv()

            exchange(b, full, one_send, one_recv).wait_recv()
            hidden(b)
            exchange(b, act, two_send, two_recv).start()

        @pl.when((i >= 4) & (i < groups + 4))
        def _():
            b = label(i - 4)

            @pl.when(i == 4)
            def _():
                down_copy.wait_recv()

            exchange(b, act, two_send, two_recv).wait_recv()
            for j in range(shards):
                span = pl.ds(pl.multiple_of(owners[j] * columns, columns), columns)
                wide_rows[:, span] = act[b, j]
            made[b, 1] = output_rows(b, 1)
            give_back(b, 1).start()
            result = output_rows(b, 0)

            @pl.when(b == 0)
            def _():
                returned[0, mine] = result

            @pl.when(b > 0)
            def _():
                made[b, 0] = result
                give_back(b, 0).start()

        @pl.when(i >= 6)
        def _():
            b = label(i - 6)

            @pl.when(b == 0)
            def _():
                arrive_back(0, 1 - mine).wait_recv()

            @pl.when(b > 0)
            def _():
                arrive_back(b, 0).wait_recv()
                arrive_back(b, 1).wait_recv()

            numbers = lax.broadcasted_iota(jnp.int32, (rows, capacity), 1) + b * capacity
            wide_numbers = numbers.astype(jnp.float32)
            added = blended[...]
            rows_back = returned[b].reshape(capacity, columns)
            for k in range(topk):
                taken = jnp.where(wide_numbers == facts_col[:, k : k + 1], 1.0, 0.0)
                picked = jnp.dot(
                    taken.astype(jnp.bfloat16), rows_back, preferred_element_type=jnp.float32
                )
                added = added + facts_col[:, topk + k : topk + k + 1] * picked
            blended[...] = added

        return carry

    lax.fori_loop(0, groups + 6, step, 0)
    out_ref[...] = blended[...].astype(out_ref.dtype)

    def settle(i, carry):
        @pl.when(i > 0)
        def _():
            dispatch(i, 0).wait_send()
            give_back(i, 0).wait_send()

        dispatch(i, 1).wait_send()
        give_back(i, 1).wait_send()
        exchange(i, full, one_send, one_recv).wait_send()
        exchange(i, act, two_send, two_recv).wait_send()
        return carry

    lax.fori_loop(0, groups, settle, 0)
    down_copy.wait_send()

    for which in range(2):
        direct(which).wait_send()
        relay(which).wait_send()

    for s in range(1, chips):
        ask(partner(2 * s) // 2).wait_send()
        for copy in spread(partner(2 * s) // 2):
            copy.wait_send()
        for copy in sideways(2 * (partner(2 * s) // 2) + core):
            copy.wait_send()
    for copy in sideways(sp, True):
        copy.wait_send()

    @pl.when(lead != core)
    def _():
        ask(chip).wait_send()

    for n in range(chips):

        @pl.when((n != chip) | (lead != core))
        def _():
            answer(n).wait_send()

    for number in range(pieces):
        for copy in weight_copies(number):
            copy.wait_send()


def layer_fused(
    query_rows,
    key_rows,
    value_rows,
    gates,
    output_weight,
    residual,
    index,
    route_weights,
    norm_gain,
    gate_weight,
    up_weight,
    down_weight,
    capacity,
):
    rows, width = query_rows.shape
    columns = residual.shape[1]
    heads = gates.shape[0]
    groups = lax.axis_size("sp")
    shards = lax.axis_size("tp")
    lanes = min(width, 128)
    depth, units = gate_weight.shape
    half = capacity // 2
    dma = pltpu.SemaphoreType.DMA
    return pl.pallas_call(
        functools.partial(layer_kernel, heads, groups),
        out_shape=jax.ShapeDtypeStruct(residual.shape, jnp.bfloat16),
        in_specs=[pl.BlockSpec(memory_space=pltpu.VMEM)] * 9
        + [pl.BlockSpec(memory_space=pl.ANY)] * 3,
        out_specs=pl.BlockSpec(memory_space=pltpu.VMEM),
        scratch_shapes=[
            pltpu.VMEM(index.shape, jnp.int32),
            pltpu.VMEM((8, rows), jnp.float32),
            pltpu.VMEM((rows, 8), jnp.float32),
            pltpu.VMEM((1, shards * columns), jnp.float32),
            pltpu.VMEM((rows, columns), jnp.bfloat16),
            pltpu.VMEM((heads, rows, lanes), jnp.bfloat16),
            pltpu.VMEM((heads, rows // 2, lanes), jnp.bfloat16),
            pltpu.VMEM((groups, rows, lanes), jnp.bfloat16),
            pltpu.VMEM((heads, rows // 2, lanes), jnp.bfloat16),
            pltpu.VMEM((groups, heads, rows), jnp.float32),
            pltpu.VMEM((8, 2 * rows), jnp.float32),
            pltpu.VMEM((heads, rows // 2, lanes), jnp.bfloat16),
            pltpu.VMEM((heads, rows // 2, lanes), jnp.bfloat16),
            pltpu.VMEM((heads, rows, lanes), jnp.bfloat16),
            pltpu.VMEM((heads, rows, 128), jnp.float32),
            pltpu.VMEM((heads, rows, 128), jnp.float32),
            pltpu.VMEM((heads, rows, lanes), jnp.float32),
            pltpu.VMEM((4, rows, width), jnp.bfloat16),
            pltpu.VMEM((groups, 2, half, columns), jnp.bfloat16),
            pltpu.VMEM((groups, shards, half, columns), jnp.bfloat16),
            pltpu.VMEM((groups, shards, half, units), jnp.bfloat16),
            pltpu.VMEM((groups, 2, half, columns), jnp.bfloat16),
            pltpu.VMEM((groups, 2, half, columns), jnp.bfloat16),
            pltpu.VMEM((rows, columns), jnp.float32),
            pltpu.VMEM((2, depth, units), jnp.bfloat16),
            pltpu.VMEM((2, depth, units), jnp.bfloat16),
            pltpu.VMEM((2, shards * units, columns), jnp.bfloat16),
            pltpu.VMEM((half, shards * columns), jnp.bfloat16),
            dma((heads, 2)),
            dma((groups, 2)),
            dma((groups, 2)),
            dma((heads,)),
            dma((heads,)),
            dma((heads,)),
            dma((heads,)),
            dma((4,)),
            dma((4,)),
            dma((8, 2)),
            dma((8, 2)),
            dma((3,)),
            dma(()),
            dma(()),
            dma((groups, 2)),
            dma((groups, 2)),
            dma((groups,)),
            dma((groups,)),
            dma((groups,)),
            dma((groups,)),
            dma((groups, 2)),
            dma((groups, 2)),
        ],
        compiler_params=pltpu.CompilerParams(
            collective_id=1, has_side_effects=True, vmem_limit_bytes=67043328
        ),
    )(
        query_rows,
        key_rows,
        value_rows,
        gates,
        output_weight,
        residual,
        index,
        route_weights,
        norm_gain,
        gate_weight,
        up_weight,
        down_weight,
    )


def body(
    query_rows,
    key_rows,
    value_rows,
    cum_gates,
    residual,
    output_weight,
    norm_gain,
    expert_index,
    route_weights,
    gate_weight,
    up_weight,
    down_weight,
):
    rows, columns = residual.shape
    topk = expert_index.shape[1]
    local_experts = gate_weight.shape[0]
    groups = lax.axis_size("sp")
    experts = local_experts * groups
    capacity = 2 * rows * topk // experts
    heads = cum_gates.shape[1]

    if (
        lax.axis_size("tp") == 4
        and local_experts == 1
        and groups == 8
        and heads == 4
        and query_rows.shape[1] == heads * 64
    ):
        return layer_fused(
            query_rows,
            key_rows,
            value_rows,
            cum_gates.T,
            output_weight,
            residual,
            expert_index.T,
            route_weights.T,
            norm_gain,
            gate_weight[0],
            up_weight[0],
            down_weight[0],
            capacity,
        )

    both = jnp.concatenate([key_rows, value_rows], axis=1)
    kv_all = lax.all_gather(both, "sp", axis=0, tiled=True)
    gates_all = lax.all_gather(cum_gates.T, "sp", axis=0, tiled=False)

    chosen = expert_index.reshape(rows * topk)
    matches = (chosen[:, None] == jnp.arange(experts, dtype=jnp.int32)[None, :]).astype(jnp.int32)
    rank = jnp.sum((jnp.cumsum(matches, axis=0) - matches) * matches, axis=1)
    chosen, rank, gates_all = lax.optimization_barrier((chosen, rank, gates_all))

    attended = attend_local(query_rows, kv_all, gates_all)
    projected = jnp.dot(
        lax.all_gather(attended, "tp", axis=1, tiled=True),
        output_weight,
        preferred_element_type=jnp.float32,
    )
    mixed = (residual.astype(jnp.float32) + projected).astype(jnp.bfloat16)

    chunks = math.gcd(capacity, CHUNKS)
    piece = capacity // chunks
    places = chosen * piece + rank % piece
    inside = rank // piece
    blended = jnp.zeros((rows, columns), jnp.float32)
    for c in range(chunks):
        place = jnp.where(inside == c, places, -1).reshape(rows, topk)
        numbers = jnp.arange(experts * piece, dtype=jnp.int32)
        taken = numbers[:, None] == place[:, 0][None, :]
        for k in range(1, topk):
            taken = taken | (numbers[:, None] == place[:, k][None, :])
        outgoing = jnp.dot(
            taken.astype(jnp.bfloat16), mixed, preferred_element_type=jnp.float32
        ).astype(jnp.bfloat16)
        arrived = lax.all_to_all(
            outgoing.reshape(experts, piece, columns), "sp", split_axis=0, concat_axis=0, tiled=True
        )
        grouped = arrived.reshape(groups, local_experts, piece, columns)
        normed = normalize(lax.all_gather(grouped, "tp", axis=3, tiled=True), norm_gain)
        gate_input = jnp.einsum(
            "seid,edf->seif", normed, gate_weight, preferred_element_type=jnp.float32
        )
        linear_input = jnp.einsum(
            "seid,edf->seif", normed, up_weight, preferred_element_type=jnp.float32
        )
        gate_cut = jnp.minimum(gate_input, CLAMP_LIMIT)
        linear_cut = jnp.clip(linear_input, -CLAMP_LIMIT, CLAMP_LIMIT)
        activated = (gate_cut * jax.nn.sigmoid(SILU_ALPHA * gate_cut) * (linear_cut + 1.0)).astype(
            jnp.bfloat16
        )
        produced = jnp.einsum(
            "seif,efc->seic",
            lax.all_gather(activated, "tp", axis=3, tiled=True),
            down_weight,
            preferred_element_type=jnp.float32,
        ).astype(jnp.bfloat16)
        returned = lax.all_to_all(
            produced.reshape(experts, piece, columns), "sp", split_axis=0, concat_axis=0, tiled=True
        ).reshape(experts * piece, columns)
        for k in range(topk):
            picked = jnp.dot(
                (place[:, k][:, None] == numbers[None, :]).astype(jnp.bfloat16),
                returned,
                preferred_element_type=jnp.float32,
            )
            blended = blended + route_weights[:, k : k + 1] * picked
    return (mixed.astype(jnp.float32) + blended).astype(jnp.bfloat16)


def solution(mesh):
    placed = (
        P("sp", "tp"),
        P("sp", "tp"),
        P("sp", "tp"),
        P("sp", "tp"),
        P("sp", "tp"),
        P(None, "tp"),
        P(),
        P("sp", None),
        P("sp", None),
        P("sp", None, "tp"),
        P("sp", None, "tp"),
        P("sp", None, "tp"),
    )
    return jax.shard_map(body, mesh=mesh, in_specs=placed, out_specs=P("sp", "tp"), check_vma=False)
```

```python
import functools
import math

import jax
import jax.numpy as jnp
from jax import lax
from jax.experimental import pallas as pl
from jax.experimental.pallas import tpu as pltpu
from jax.sharding import PartitionSpec as P

NORM_EPS = 1e-06
CLAMP_LIMIT = 7.0
SILU_ALPHA = 1.702
CHUNKS = 1


def normalize(rows, norm_gain):
    wide = rows.astype(jnp.float32)
    factor = lax.rsqrt(jnp.mean(wide * wide, axis=-1, keepdims=True) + NORM_EPS)
    return (wide * factor * norm_gain.astype(jnp.float32)).astype(jnp.bfloat16)


def attend_kernel(heads, q_ref, kv_ref, gates_ref, out_ref, masked_q, top, total, summed):
    rows, width = q_ref.shape
    head_size = width // heads
    lanes = min(width, 128)
    tile = math.gcd(rows, 256)
    tiles = rows // tile
    me = lax.axis_index("sp")
    scale = head_size ** (-0.5)
    lane = lax.broadcasted_iota(jnp.int32, (rows, lanes), 1)
    for h in range(heads):
        group, inside = divmod(h * head_size, lanes)
        part = q_ref[:, group * lanes : (group + 1) * lanes].astype(jnp.float32) * scale
        keep = (lane >= inside) & (lane < inside + head_size)
        masked_q[h] = jnp.where(keep, part, 0.0).astype(jnp.bfloat16)
    top[...] = jnp.full(top.shape, -1e30, jnp.float32)
    total[...] = jnp.zeros(total.shape, jnp.float32)
    summed[...] = jnp.zeros(summed.shape, jnp.float32)

    def block(number, diagonal):
        base = pl.multiple_of(number * rows, rows)
        for h in range(heads):
            group = h * head_size // lanes
            keys = kv_ref[pl.ds(base, rows), group * lanes : (group + 1) * lanes]
            values = kv_ref[pl.ds(base, rows), width + group * lanes : width + (group + 1) * lanes]
            gates = gates_ref[number, h : h + 1, :]
            for t in range(tiles):
                span = slice(t * tile, (t + 1) * tile)
                count = (t + 1) * tile if diagonal else rows
                scores = lax.dot_general(
                    masked_q[h, span],
                    keys[:count],
                    (((1,), (1,)), ((), ())),
                    preferred_element_type=jnp.float32,
                )
                scores = scores - gates[:, :count]
                if diagonal:
                    row = lax.broadcasted_iota(jnp.int32, (tile, count), 0) + t * tile
                    col = lax.broadcasted_iota(jnp.int32, (tile, count), 1)
                    scores = jnp.where(col <= row, scores, -jnp.inf)
                old = top[h, span]
                new = jnp.maximum(old, jnp.max(scores, axis=1, keepdims=True))
                raised = jnp.exp(scores - new[:, :1])
                shrink = jnp.exp(old - new)
                part = raised[:, :128]
                for c in range(128, count, 128):
                    part = part + raised[:, c : c + 128]
                top[h, span] = new
                total[h, span] = total[h, span] * shrink + part
                product = lax.dot_general(
                    raised.astype(jnp.bfloat16),
                    values[:count],
                    (((1,), (0,)), ((), ())),
                    preferred_element_type=jnp.float32,
                )
                summed[h, span] = summed[h, span] * shrink[:, :lanes] + product

    def step(number, carry):
        block(number, False)
        return carry

    lax.fori_loop(0, me, step, 0)
    block(me, True)
    for g in range(width // lanes):
        result = jnp.zeros((rows, lanes), jnp.float32)
        for h in range(heads):
            if h * head_size // lanes == g:
                inside = h * head_size % lanes
                keep = (lane >= inside) & (lane < inside + head_size)
                whole = jnp.sum(total[h], axis=1, keepdims=True)
                result = jnp.where(keep, summed[h] / whole, result)
        out_ref[:, g * lanes : (g + 1) * lanes] = result.astype(out_ref.dtype)


def attend_local(query_rows, kv_all, gates_all):
    rows, width = query_rows.shape
    groups, heads, _ = gates_all.shape
    lanes = min(width, 128)
    return pl.pallas_call(
        functools.partial(attend_kernel, heads),
        out_shape=jax.ShapeDtypeStruct((rows, width), jnp.bfloat16),
        in_specs=[pl.BlockSpec(memory_space=pltpu.VMEM)] * 3,
        out_specs=pl.BlockSpec(memory_space=pltpu.VMEM),
        scratch_shapes=[
            pltpu.VMEM((heads, rows, lanes), jnp.bfloat16),
            pltpu.VMEM((heads, rows, 128), jnp.float32),
            pltpu.VMEM((heads, rows, 128), jnp.float32),
            pltpu.VMEM((heads, rows, lanes), jnp.float32),
        ],
        compiler_params=pltpu.CompilerParams(vmem_limit_bytes=48 * 2**20),
        cost_estimate=pl.CostEstimate(
            flops=4 * rows * rows * groups * width * 4,
            bytes_accessed=4 * rows * groups * width,
            transcendentals=rows * rows * groups * heads,
        ),
    )(query_rows, kv_all, gates_all)


def half_of(core, tp):
    return (1 - core) * (tp // 2) + core * (tp % 2)


def partner_of(core, tp):
    return (1 - core) * ((tp + 2) % 4) + core * (tp + 1 - 2 * (tp % 2))


def layer_kernel(
    heads,
    groups,
    q_ref,
    k_ref,
    v_ref,
    gates_ref,
    weight_ref,
    residual_ref,
    index_ref,
    route_ref,
    gain_ref,
    gate_ref,
    up_ref,
    down_ref,
    out_ref,
    place_row_ref,
    facts,
    facts_col,
    gain_row,
    mixed_ref,
    kv_out,
    q_out,
    kv_all,
    q_all,
    gates_all,
    gate_pair,
    packed,
    heads_in,
    masked_q,
    top,
    total,
    summed,
    attended,
    outbox,
    full,
    act,
    made,
    returned,
    blended,
    gate_all,
    up_all,
    down_all,
    wide_rows,
    kv_send,
    side_send,
    kv_recv,
    q_send,
    q_recv,
    head_send,
    head_recv,
    tp_send,
    tp_recv,
    weight_send,
    weight_recv,
    load_sem,
    down_send,
    down_recv,
    out_send,
    out_recv,
    one_send,
    one_recv,
    two_send,
    two_recv,
    back_send,
    back_recv,
):
    rows, width = q_ref.shape
    head_size = width // heads
    lanes = min(width, 128)
    tile = math.gcd(rows, 256)
    tiles = rows // tile
    sp = lax.axis_index("sp")
    tp = lax.axis_index("tp")
    chip = sp // 2
    core = sp % 2
    chips = groups // 2
    sibling = sp + 1 - 2 * core
    beside = tp + 1 - 2 * (tp % 2)
    across = (tp + 2) % 4
    mesh_id = pl.DeviceIdType.MESH
    scale = head_size ** (-0.5)
    lead = (sp + chip) % 2

    def direct(which):
        return pltpu.make_async_remote_copy(
            src_ref=attended.at[tp],
            dst_ref=attended.at[tp],
            send_sem=tp_send.at[which],
            recv_sem=tp_recv.at[which],
            device_id=(sp, beside if which == 0 else across),
            device_id_type=mesh_id,
        )

    def relay(which):
        owner = beside if which == 0 else across
        part = attended.at[owner, pl.ds(which * (rows // 2), rows // 2)]
        return pltpu.make_async_remote_copy(
            src_ref=part,
            dst_ref=part,
            send_sem=tp_send.at[2 + which],
            recv_sem=tp_recv.at[2 + which],
            device_id=(sp, across if which == 0 else beside),
            device_id_type=mesh_id,
        )

    topk = route_ref.shape[0]
    half, columns = outbox.shape[2:]
    capacity = 2 * half
    shards = full.shape[1]
    mine = half_of(core, tp)
    pair = partner_of(core, tp)
    peer = partner_of(1 - core, tp)
    owners = (tp, pair, peer, (beside + 2) % 4)

    def partner(number):
        found, bit = 0, 1
        while bit < groups:
            found = found + bit * (((sp // bit) % 2 + (number // bit) % 2) % 2)
            bit *= 2
        return found

    def send(src, dst, send_sem, recv_sem, device):
        return pltpu.make_async_remote_copy(
            src_ref=src,
            dst_ref=dst,
            send_sem=send_sem,
            recv_sem=recv_sem,
            device_id=device,
            device_id_type=pl.DeviceIdType.MESH,
        )

    def spread(head):
        device = (2 * head + core, tp)
        return [
            send(src, dst.at[sp], kv_send.at[head, n], kv_recv.at[sp, n], device)
            for n, (src, dst) in enumerate(((kv_out.at[head], kv_all), (gates_ref, gates_all)))
        ]

    def sideways(number, own=False):
        return [
            send(src, dst.at[number], side_send.at[number, n], kv_recv.at[number, n], (sibling, tp))
            for n, (src, dst) in enumerate(
                (
                    (kv_all.at[number], kv_all),
                    (gates_ref if own else gates_all.at[number], gates_all),
                )
            )
        ]

    def ask(head):
        return send(
            q_out.at[head],
            q_all.at[chip],
            q_send.at[head],
            q_recv.at[chip],
            (2 * head + lead, tp),
        )

    def answer(slot):
        return send(
            packed.at[slot],
            heads_in.at[chip],
            head_send.at[slot],
            head_recv.at[chip],
            (2 * slot + (slot + core) % 2, tp),
        )

    def dispatch(i, which):
        group = partner(i)
        target = tp if which == 0 else partner_of(group % 2, tp)
        return send(
            outbox.at[i, which],
            full.at[i, which],
            out_send.at[i, which],
            out_recv.at[i, which],
            (group, target),
        )

    def exchange(i, held, send_sem, recv_sem):
        return send(
            held.at[i, pl.ds(0, 2)],
            held.at[i, pl.ds(2, 2)],
            send_sem.at[i],
            recv_sem.at[i],
            (sp, peer),
        )

    def give_back(i, which):
        target = tp if which == 0 else pair
        return send(
            made.at[i, which],
            returned.at[i, mine],
            back_send.at[i, which],
            back_recv.at[i, mine],
            (partner(i), target),
        )

    def arrive_back(i, which):
        return send(
            made.at[i, 0],
            returned.at[i, which],
            back_send.at[i, 0],
            back_recv.at[i, which],
            (sp, pair),
        )

    loads = []
    for n, (src, dst) in enumerate(
        ((gate_ref, gate_all.at[0]), (up_ref, up_all.at[0]), (down_ref, down_all.at[0]))
    ):
        loads.append(pltpu.make_async_copy(src, dst, load_sem.at[n]))
    for load in loads:
        load.start()

    barrier = pltpu.get_barrier_semaphore()
    for i in range(1, groups):
        pl.semaphore_signal(
            barrier, inc=1, device_id=(partner(i), tp), device_id_type=pl.DeviceIdType.MESH
        )
        pl.semaphore_signal(
            barrier,
            inc=1,
            device_id=(partner(i), partner_of(partner(i) % 2, tp)),
            device_id_type=pl.DeviceIdType.MESH,
        )
        pl.semaphore_signal(
            barrier, inc=1, device_id=(partner(i), pair), device_id_type=pl.DeviceIdType.MESH
        )
    for other in (pair, peer):
        pl.semaphore_signal(
            barrier, inc=1, device_id=(sp, other), device_id_type=pl.DeviceIdType.MESH
        )
    pl.semaphore_wait(barrier, 3 * groups - 1)

    down_copy = send(down_ref, down_all.at[1], down_send, down_recv, (sp, pair))
    pieces = weight_send.shape[0]
    depth = gate_ref.shape[0] // pieces

    def weight_copies(number):
        part = pl.ds(pl.multiple_of(number * depth, depth), depth)
        return [
            send(
                src.at[part],
                dst.at[1, part],
                weight_send.at[number, n],
                weight_recv.at[number, n],
                (sp, pair),
            )
            for n, (src, dst) in enumerate(((gate_ref, gate_all), (up_ref, up_all)))
        ]

    def push(number):
        for copy in weight_copies(number):
            copy.start()

    early = pieces - 1 - chips
    for number in range(early):
        push(number)

    lane = lax.broadcasted_iota(jnp.int32, (rows, lanes), 1)
    low = lane < head_size
    short = rows // 2
    short_low = low[:short]

    def turned(wide):
        return pltpu.roll(wide, head_size, 1)

    for g in range(width // lanes):
        part = slice(g * lanes, (g + 1) * lanes)
        wide = q_ref[:, part].astype(jnp.float32) * scale
        tail = turned(wide[short:])
        q_out[2 * g] = jnp.where(short_low, wide[:short], tail).astype(jnp.bfloat16)
        q_out[2 * g + 1] = jnp.where(short_low, tail, wide[:short]).astype(jnp.bfloat16)
    for s in range(1, chips):
        ask(partner(2 * s) // 2).start()

    @pl.when(lead != core)
    def _():
        ask(chip).start()

    @pl.when(lead == core)
    def _():
        q_all[chip] = q_out[chip]

    for g in range(width // lanes):
        part = slice(g * lanes, (g + 1) * lanes)
        keys = k_ref[:, part].astype(jnp.float32)
        values = turned(v_ref[:, part].astype(jnp.float32))
        kv_out[2 * g] = jnp.where(low, keys, values).astype(jnp.bfloat16)
        kv_out[2 * g + 1] = jnp.where(low, values, keys).astype(jnp.bfloat16)
    for s in range(1, chips):
        for copy in spread(partner(2 * s) // 2):
            copy.start()
    kv_all[sp] = kv_out[chip]
    gates_all[sp] = gates_ref[...]
    for copy in sideways(sp, True):
        copy.start()

    first = lax.broadcasted_iota(jnp.int32, (rows, rows), 0)
    second = lax.broadcasted_iota(jnp.int32, (rows, rows), 1)
    number = lax.broadcasted_iota(jnp.int32, (128, rows), 0)
    chosen = [index_ref[k : k + 1, :] ^ sp for k in range(topk)]
    named = jnp.zeros((128, rows), jnp.float32)
    for k in range(topk):
        named = named + jnp.where(number == chosen[k], 1.0, 0.0)
    before = jnp.dot(
        named.astype(jnp.bfloat16),
        jnp.where(first < second, 1.0, 0.0).astype(jnp.bfloat16),
        preferred_element_type=jnp.float32,
    )
    facts[...] = jnp.zeros(facts.shape, jnp.float32)
    for k in range(topk):
        rank = jnp.sum(jnp.where(number == chosen[k], before, 0.0), axis=0, keepdims=True)
        place_row_ref[k : k + 1, :] = chosen[k] * capacity + rank.astype(jnp.int32)
        facts[k : k + 1, :] = (chosen[k] * capacity).astype(jnp.float32) + rank
        facts[topk + k : topk + k + 1, :] = route_ref[k : k + 1, :]
    facts_col[...] = jnp.transpose(facts[...])
    gain_row[...] = gain_ref[...].astype(jnp.float32).reshape(1, -1)

    odd = chip % 2
    key_lane = (lane // head_size) == odd
    short_key = key_lane[:short]
    top[...] = jnp.full(top.shape, -1e30, jnp.float32)
    total[...] = jnp.zeros(total.shape, jnp.float32)
    summed[...] = jnp.zeros(summed.shape, jnp.float32)
    for n in range(chips):

        @pl.when((n != chip) | (lead != core))
        def _():
            send(
                q_out.at[0], q_all.at[n], q_send.at[0], q_recv.at[n], (sibling, tp)
            ).wait_recv()

        part = q_all[n].astype(jnp.float32)
        masked_q[n, :short] = jnp.where(short_key, part, 0.0).astype(jnp.bfloat16)
        masked_q[n, short:] = jnp.where(short_key, turned(part), 0.0).astype(jnp.bfloat16)

    def block(slot, number, offset):
        span_keys = 2 * rows
        for t in range(tiles):
            span = slice(t * tile, (t + 1) * tile)
            count = span_keys if offset is None else offset + (t + 1) * tile
            pair_kv = kv_all[pl.ds(2 * number, 2)].reshape(span_keys, lanes)[:count]
            scores = lax.dot_general(
                masked_q[slot, span],
                pair_kv,
                (((1,), (1,)), ((), ())),
                preferred_element_type=jnp.float32,
            )
            scores = scores - gate_pair[0:1, :count]
            if offset is not None:
                row = lax.broadcasted_iota(jnp.int32, (tile, count), 0) + t * tile + offset
                col = lax.broadcasted_iota(jnp.int32, (tile, count), 1)
                scores = jnp.where(col <= row, scores, -jnp.inf)
            old = top[slot, span]
            new = jnp.maximum(old, jnp.max(scores, axis=1, keepdims=True))
            raised = jnp.exp(scores - new[:, :1])
            shrink = jnp.exp(old - new)
            part = raised[:, :128]
            for c in range(128, count, 128):
                part = part + raised[:, c : c + 128]
            top[slot, span] = new
            total[slot, span] = total[slot, span] * shrink + part
            product = lax.dot_general(
                raised.astype(jnp.bfloat16),
                pair_kv,
                (((1,), (0,)), ((), ())),
                preferred_element_type=jnp.float32,
            )
            summed[slot, span] = summed[slot, span] * shrink[:, :lanes] + product

    def chip_step(s, carry):
        number = partner(2 * s) // 2
        near = 2 * number + core
        push(early + s)

        @pl.when(s > 0)
        def _():
            for copy in sideways(near):
                copy.wait_recv()
            for copy in sideways(near):
                copy.start()

        for copy in sideways(2 * number + 1 - core):
            copy.wait_recv()
        gate_pair[0:1, :rows] = gates_all[2 * number, pl.ds(chip, 1), :]
        gate_pair[0:1, rows:] = gates_all[2 * number + 1, pl.ds(chip, 1), :]

        @pl.when((number + core) % 2 == 0)
        def _():
            block(number, number, 0)

        @pl.when((number + core) % 2 == 1)
        def _():
            block(number, number, rows)

        def full_step(slot, inner):
            block(slot, number, None)
            return inner

        lax.fori_loop(number + 1, chips, full_step, 0)
        return carry

    lax.fori_loop(0, chips, chip_step, 0)

    for n in range(chips):
        result = summed[n] / jnp.sum(total[n], axis=1, keepdims=True)
        folded = jnp.where(short_key, turned(result[short:]), result[:short])
        packed[n] = folded.astype(jnp.bfloat16)

        @pl.when((n != chip) | (lead != core))
        def _():
            answer(n).start()

        @pl.when((n == chip) & (lead == core))
        def _():
            heads_in[chip] = packed[n]

    for n in range(chips):

        @pl.when((n != chip) | (lead != core))
        def _():
            send(
                packed.at[0], heads_in.at[n], head_send.at[0], head_recv.at[n], (sibling, tp)
            ).wait_recv()

    for g in range(width // lanes):
        even = heads_in[2 * g].astype(jnp.float32)
        uneven = heads_in[2 * g + 1].astype(jnp.float32)
        part = slice(g * lanes, (g + 1) * lanes)
        attended[tp, :short, part] = jnp.where(short_low, turned(even), turned(uneven)).astype(
            jnp.bfloat16
        )
        attended[tp, short:, part] = jnp.where(short_low, even, uneven).astype(jnp.bfloat16)
    direct(0).start()
    direct(1).start()

    def projected(owner):
        return jnp.dot(
            attended[owner],
            weight_ref[pl.ds(pl.multiple_of(owner * width, width), width), :],
            preferred_element_type=jnp.float32,
        )

    mixed = residual_ref[...].astype(jnp.float32) + projected(tp)
    for which, owner in ((0, beside), (1, across)):
        direct(which).wait_recv()
        relay(which).start()
        mixed = mixed + projected(owner)
    for number in range(early + chips, pieces):
        push(number)
    down_copy.start()
    relay(0).wait_recv()
    relay(1).wait_recv()
    mixed_ref[...] = (mixed + projected((beside + 2) % 4)).astype(mixed_ref.dtype)

    def rows_for(i):
        flip = half_of(partner(i) % 2, tp)
        place = lax.broadcasted_iota(jnp.int32, (capacity, rows), 0) + flip * half
        numbers = jnp.where(place >= capacity, place - capacity, place) + i * capacity
        taken = numbers == place_row_ref[0:1, :]
        for k in range(1, topk):
            taken = taken | (numbers == place_row_ref[k : k + 1, :])
        return jnp.dot(
            jnp.where(taken, 1.0, 0.0).astype(jnp.bfloat16),
            mixed_ref[...],
            preferred_element_type=jnp.float32,
        ).astype(jnp.bfloat16)

    def fill(i, carry):
        made_rows = rows_for(i)
        outbox[i, 0] = made_rows[:half]
        outbox[i, 1] = made_rows[half:]
        dispatch(i, 0).start()
        dispatch(i, 1).start()
        return carry

    def label(n):
        return 2 * (lax.shift_right_logical(30, 2 * (n // 2)) % chips) + n % 2

    def fill_next(n, carry):
        return fill(label(n), carry)

    lax.fori_loop(0, groups - 2, fill_next, 0)
    lax.fori_loop(1, 2, fill, 0)
    first = rows_for(0)
    full[0, 0] = first[:half]
    outbox[0, 1] = first[half:]
    dispatch(0, 1).start()
    blended[...] = mixed_ref[...].astype(jnp.float32)

    def hidden(i):
        square = jnp.zeros((half, 1), jnp.float32)
        for j in range(shards):
            wide = full[i, j].astype(jnp.float32)
            square = square + jnp.sum(wide * wide, axis=1, keepdims=True)
        factor = lax.rsqrt(square / (shards * columns) + NORM_EPS)
        for j in range(shards):
            span = pl.ds(pl.multiple_of(owners[j] * columns, columns), columns)
            gain = gain_row[0:1, span]
            wide_rows[:, span] = (full[i, j].astype(jnp.float32) * factor * gain).astype(
                jnp.bfloat16
            )
        for c in range(2):
            gate_input = jnp.dot(
                wide_rows[...], gate_all[c], preferred_element_type=jnp.float32
            )
            linear_input = jnp.dot(wide_rows[...], up_all[c], preferred_element_type=jnp.float32)
            gate_cut = jnp.minimum(gate_input, CLAMP_LIMIT)
            linear_cut = jnp.clip(linear_input, -CLAMP_LIMIT, CLAMP_LIMIT)
            act[i, c] = (
                gate_cut * jax.nn.sigmoid(SILU_ALPHA * gate_cut) * (linear_cut + 1.0)
            ).astype(jnp.bfloat16)

    def output_rows(i, c):
        return jnp.dot(
            wide_rows[...], down_all[c], preferred_element_type=jnp.float32
        ).astype(jnp.bfloat16)

    def step(i, carry):
        @pl.when(i < groups)
        def _():
            b = label(i)

            @pl.when(b > 0)
            def _():
                dispatch(b, 0).wait_recv()

            dispatch(b, 1).wait_recv()
            exchange(b, full, one_send, one_recv).start()

        @pl.when((i >= 2) & (i < groups + 2))
        def _():
            b = label(i - 2)

            @pl.when(i == 2)
            def _():
                for load in loads:
                    load.wait()
                for number in range(pieces):
                    for copy in weight_copies(number):
                        copy.wait_recv()

            exchange(b, full, one_send, one_recv).wait_recv()
            hidden(b)
            exchange(b, act, two_send, two_recv).start()

        @pl.when((i >= 4) & (i < groups + 4))
        def _():
            b = label(i - 4)

            @pl.when(i == 4)
            def _():
                down_copy.wait_recv()

            exchange(b, act, two_send, two_recv).wait_recv()
            for j in range(shards):
                span = pl.ds(pl.multiple_of(owners[j] * columns, columns), columns)
                wide_rows[:, span] = act[b, j]
            made[b, 1] = output_rows(b, 1)
            give_back(b, 1).start()
            result = output_rows(b, 0)

            @pl.when(b == 0)
            def _():
                returned[0, mine] = result

            @pl.when(b > 0)
            def _():
                made[b, 0] = result
                give_back(b, 0).start()

        @pl.when(i >= 7)
        def _():
            b = label(i - 7)

            @pl.when(b == 0)
            def _():
                arrive_back(0, 1 - mine).wait_recv()

            @pl.when(b > 0)
            def _():
                arrive_back(b, 0).wait_recv()
                arrive_back(b, 1).wait_recv()

            numbers = lax.broadcasted_iota(jnp.int32, (rows, capacity), 1) + b * capacity
            wide_numbers = numbers.astype(jnp.float32)
            added = blended[...]
            rows_back = returned[b].reshape(capacity, columns)
            for k in range(topk):
                taken = jnp.where(wide_numbers == facts_col[:, k : k + 1], 1.0, 0.0)
                picked = jnp.dot(
                    taken.astype(jnp.bfloat16), rows_back, preferred_element_type=jnp.float32
                )
                added = added + facts_col[:, topk + k : topk + k + 1] * picked
            blended[...] = added

        return carry

    lax.fori_loop(0, groups + 7, step, 0)
    out_ref[...] = blended[...].astype(out_ref.dtype)

    def settle(i, carry):
        @pl.when(i > 0)
        def _():
            dispatch(i, 0).wait_send()
            give_back(i, 0).wait_send()

        dispatch(i, 1).wait_send()
        give_back(i, 1).wait_send()
        exchange(i, full, one_send, one_recv).wait_send()
        exchange(i, act, two_send, two_recv).wait_send()
        return carry

    lax.fori_loop(0, groups, settle, 0)
    down_copy.wait_send()

    for which in range(2):
        direct(which).wait_send()
        relay(which).wait_send()

    for s in range(1, chips):
        ask(partner(2 * s) // 2).wait_send()
        for copy in spread(partner(2 * s) // 2):
            copy.wait_send()
        for copy in sideways(2 * (partner(2 * s) // 2) + core):
            copy.wait_send()
    for copy in sideways(sp, True):
        copy.wait_send()

    @pl.when(lead != core)
    def _():
        ask(chip).wait_send()

    for n in range(chips):

        @pl.when((n != chip) | (lead != core))
        def _():
            answer(n).wait_send()

    for number in range(pieces):
        for copy in weight_copies(number):
            copy.wait_send()


def layer_fused(
    query_rows,
    key_rows,
    value_rows,
    gates,
    output_weight,
    residual,
    index,
    route_weights,
    norm_gain,
    gate_weight,
    up_weight,
    down_weight,
    capacity,
):
    rows, width = query_rows.shape
    columns = residual.shape[1]
    heads = gates.shape[0]
    groups = lax.axis_size("sp")
    shards = lax.axis_size("tp")
    lanes = min(width, 128)
    depth, units = gate_weight.shape
    half = capacity // 2
    dma = pltpu.SemaphoreType.DMA
    return pl.pallas_call(
        functools.partial(layer_kernel, heads, groups),
        out_shape=jax.ShapeDtypeStruct(residual.shape, jnp.bfloat16),
        in_specs=[pl.BlockSpec(memory_space=pltpu.VMEM)] * 9
        + [pl.BlockSpec(memory_space=pl.ANY)] * 3,
        out_specs=pl.BlockSpec(memory_space=pltpu.VMEM),
        scratch_shapes=[
            pltpu.VMEM(index.shape, jnp.int32),
            pltpu.VMEM((8, rows), jnp.float32),
            pltpu.VMEM((rows, 8), jnp.float32),
            pltpu.VMEM((1, shards * columns), jnp.float32),
            pltpu.VMEM((rows, columns), jnp.bfloat16),
            pltpu.VMEM((heads, rows, lanes), jnp.bfloat16),
            pltpu.VMEM((heads, rows // 2, lanes), jnp.bfloat16),
            pltpu.VMEM((groups, rows, lanes), jnp.bfloat16),
            pltpu.VMEM((heads, rows // 2, lanes), jnp.bfloat16),
            pltpu.VMEM((groups, heads, rows), jnp.float32),
            pltpu.VMEM((8, 2 * rows), jnp.float32),
            pltpu.VMEM((heads, rows // 2, lanes), jnp.bfloat16),
            pltpu.VMEM((heads, rows // 2, lanes), jnp.bfloat16),
            pltpu.VMEM((heads, rows, lanes), jnp.bfloat16),
            pltpu.VMEM((heads, rows, 128), jnp.float32),
            pltpu.VMEM((heads, rows, 128), jnp.float32),
            pltpu.VMEM((heads, rows, lanes), jnp.float32),
            pltpu.VMEM((4, rows, width), jnp.bfloat16),
            pltpu.VMEM((groups, 2, half, columns), jnp.bfloat16),
            pltpu.VMEM((groups, shards, half, columns), jnp.bfloat16),
            pltpu.VMEM((groups, shards, half, units), jnp.bfloat16),
            pltpu.VMEM((groups, 2, half, columns), jnp.bfloat16),
            pltpu.VMEM((groups, 2, half, columns), jnp.bfloat16),
            pltpu.VMEM((rows, columns), jnp.float32),
            pltpu.VMEM((2, depth, units), jnp.bfloat16),
            pltpu.VMEM((2, depth, units), jnp.bfloat16),
            pltpu.VMEM((2, shards * units, columns), jnp.bfloat16),
            pltpu.VMEM((half, shards * columns), jnp.bfloat16),
            dma((heads, 2)),
            dma((groups, 2)),
            dma((groups, 2)),
            dma((heads,)),
            dma((heads,)),
            dma((heads,)),
            dma((heads,)),
            dma((4,)),
            dma((4,)),
            dma((8, 2)),
            dma((8, 2)),
            dma((3,)),
            dma(()),
            dma(()),
            dma((groups, 2)),
            dma((groups, 2)),
            dma((groups,)),
            dma((groups,)),
            dma((groups,)),
            dma((groups,)),
            dma((groups, 2)),
            dma((groups, 2)),
        ],
        compiler_params=pltpu.CompilerParams(
            collective_id=1, has_side_effects=True, vmem_limit_bytes=67043328
        ),
    )(
        query_rows,
        key_rows,
        value_rows,
        gates,
        output_weight,
        residual,
        index,
        route_weights,
        norm_gain,
        gate_weight,
        up_weight,
        down_weight,
    )


def body(
    query_rows,
    key_rows,
    value_rows,
    cum_gates,
    residual,
    output_weight,
    norm_gain,
    expert_index,
    route_weights,
    gate_weight,
    up_weight,
    down_weight,
):
    rows, columns = residual.shape
    topk = expert_index.shape[1]
    local_experts = gate_weight.shape[0]
    groups = lax.axis_size("sp")
    experts = local_experts * groups
    capacity = 2 * rows * topk // experts
    heads = cum_gates.shape[1]

    if (
        lax.axis_size("tp") == 4
        and local_experts == 1
        and groups == 8
        and heads == 4
        and query_rows.shape[1] == heads * 64
    ):
        return layer_fused(
            query_rows,
            key_rows,
            value_rows,
            cum_gates.T,
            output_weight,
            residual,
            expert_index.T,
            route_weights.T,
            norm_gain,
            gate_weight[0],
            up_weight[0],
            down_weight[0],
            capacity,
        )

    both = jnp.concatenate([key_rows, value_rows], axis=1)
    kv_all = lax.all_gather(both, "sp", axis=0, tiled=True)
    gates_all = lax.all_gather(cum_gates.T, "sp", axis=0, tiled=False)

    chosen = expert_index.reshape(rows * topk)
    matches = (chosen[:, None] == jnp.arange(experts, dtype=jnp.int32)[None, :]).astype(jnp.int32)
    rank = jnp.sum((jnp.cumsum(matches, axis=0) - matches) * matches, axis=1)
    chosen, rank, gates_all = lax.optimization_barrier((chosen, rank, gates_all))

    attended = attend_local(query_rows, kv_all, gates_all)
    projected = jnp.dot(
        lax.all_gather(attended, "tp", axis=1, tiled=True),
        output_weight,
        preferred_element_type=jnp.float32,
    )
    mixed = (residual.astype(jnp.float32) + projected).astype(jnp.bfloat16)

    chunks = math.gcd(capacity, CHUNKS)
    piece = capacity // chunks
    places = chosen * piece + rank % piece
    inside = rank // piece
    blended = jnp.zeros((rows, columns), jnp.float32)
    for c in range(chunks):
        place = jnp.where(inside == c, places, -1).reshape(rows, topk)
        numbers = jnp.arange(experts * piece, dtype=jnp.int32)
        taken = numbers[:, None] == place[:, 0][None, :]
        for k in range(1, topk):
            taken = taken | (numbers[:, None] == place[:, k][None, :])
        outgoing = jnp.dot(
            taken.astype(jnp.bfloat16), mixed, preferred_element_type=jnp.float32
        ).astype(jnp.bfloat16)
        arrived = lax.all_to_all(
            outgoing.reshape(experts, piece, columns), "sp", split_axis=0, concat_axis=0, tiled=True
        )
        grouped = arrived.reshape(groups, local_experts, piece, columns)
        normed = normalize(lax.all_gather(grouped, "tp", axis=3, tiled=True), norm_gain)
        gate_input = jnp.einsum(
            "seid,edf->seif", normed, gate_weight, preferred_element_type=jnp.float32
        )
        linear_input = jnp.einsum(
            "seid,edf->seif", normed, up_weight, preferred_element_type=jnp.float32
        )
        gate_cut = jnp.minimum(gate_input, CLAMP_LIMIT)
        linear_cut = jnp.clip(linear_input, -CLAMP_LIMIT, CLAMP_LIMIT)
        activated = (gate_cut * jax.nn.sigmoid(SILU_ALPHA * gate_cut) * (linear_cut + 1.0)).astype(
            jnp.bfloat16
        )
        produced = jnp.einsum(
            "seif,efc->seic",
            lax.all_gather(activated, "tp", axis=3, tiled=True),
            down_weight,
            preferred_element_type=jnp.float32,
        ).astype(jnp.bfloat16)
        returned = lax.all_to_all(
            produced.reshape(experts, piece, columns), "sp", split_axis=0, concat_axis=0, tiled=True
        ).reshape(experts * piece, columns)
        for k in range(topk):
            picked = jnp.dot(
                (place[:, k][:, None] == numbers[None, :]).astype(jnp.bfloat16),
                returned,
                preferred_element_type=jnp.float32,
            )
            blended = blended + route_weights[:, k : k + 1] * picked
    return (mixed.astype(jnp.float32) + blended).astype(jnp.bfloat16)


def solution(mesh):
    placed = (
        P("sp", "tp"),
        P("sp", "tp"),
        P("sp", "tp"),
        P("sp", "tp"),
        P("sp", "tp"),
        P(None, "tp"),
        P(),
        P("sp", None),
        P("sp", None),
        P("sp", None, "tp"),
        P("sp", None, "tp"),
        P("sp", None, "tp"),
    )
    return jax.shard_map(body, mesh=mesh, in_specs=placed, out_specs=P("sp", "tp"), check_vma=False)
```

```python
import functools
import math

import jax
import jax.numpy as jnp
from jax import lax
from jax.experimental import pallas as pl
from jax.experimental.pallas import tpu as pltpu
from jax.sharding import PartitionSpec as P

NORM_EPS = 1e-06
CLAMP_LIMIT = 7.0
SILU_ALPHA = 1.702
CHUNKS = 1


def normalize(rows, norm_gain):
    wide = rows.astype(jnp.float32)
    factor = lax.rsqrt(jnp.mean(wide * wide, axis=-1, keepdims=True) + NORM_EPS)
    return (wide * factor * norm_gain.astype(jnp.float32)).astype(jnp.bfloat16)


def attend_kernel(heads, q_ref, kv_ref, gates_ref, out_ref, masked_q, top, total, summed):
    rows, width = q_ref.shape
    head_size = width // heads
    lanes = min(width, 128)
    tile = math.gcd(rows, 256)
    tiles = rows // tile
    me = lax.axis_index("sp")
    scale = head_size ** (-0.5)
    lane = lax.broadcasted_iota(jnp.int32, (rows, lanes), 1)
    for h in range(heads):
        group, inside = divmod(h * head_size, lanes)
        part = q_ref[:, group * lanes : (group + 1) * lanes].astype(jnp.float32) * scale
        keep = (lane >= inside) & (lane < inside + head_size)
        masked_q[h] = jnp.where(keep, part, 0.0).astype(jnp.bfloat16)
    top[...] = jnp.full(top.shape, -1e30, jnp.float32)
    total[...] = jnp.zeros(total.shape, jnp.float32)
    summed[...] = jnp.zeros(summed.shape, jnp.float32)

    def block(number, diagonal):
        base = pl.multiple_of(number * rows, rows)
        for h in range(heads):
            group = h * head_size // lanes
            keys = kv_ref[pl.ds(base, rows), group * lanes : (group + 1) * lanes]
            values = kv_ref[pl.ds(base, rows), width + group * lanes : width + (group + 1) * lanes]
            gates = gates_ref[number, h : h + 1, :]
            for t in range(tiles):
                span = slice(t * tile, (t + 1) * tile)
                count = (t + 1) * tile if diagonal else rows
                scores = lax.dot_general(
                    masked_q[h, span],
                    keys[:count],
                    (((1,), (1,)), ((), ())),
                    preferred_element_type=jnp.float32,
                )
                scores = scores - gates[:, :count]
                if diagonal:
                    row = lax.broadcasted_iota(jnp.int32, (tile, count), 0) + t * tile
                    col = lax.broadcasted_iota(jnp.int32, (tile, count), 1)
                    scores = jnp.where(col <= row, scores, -jnp.inf)
                old = top[h, span]
                new = jnp.maximum(old, jnp.max(scores, axis=1, keepdims=True))
                raised = jnp.exp(scores - new[:, :1])
                shrink = jnp.exp(old - new)
                part = raised[:, :128]
                for c in range(128, count, 128):
                    part = part + raised[:, c : c + 128]
                top[h, span] = new
                total[h, span] = total[h, span] * shrink + part
                product = lax.dot_general(
                    raised.astype(jnp.bfloat16),
                    values[:count],
                    (((1,), (0,)), ((), ())),
                    preferred_element_type=jnp.float32,
                )
                summed[h, span] = summed[h, span] * shrink[:, :lanes] + product

    def step(number, carry):
        block(number, False)
        return carry

    lax.fori_loop(0, me, step, 0)
    block(me, True)
    for g in range(width // lanes):
        result = jnp.zeros((rows, lanes), jnp.float32)
        for h in range(heads):
            if h * head_size // lanes == g:
                inside = h * head_size % lanes
                keep = (lane >= inside) & (lane < inside + head_size)
                whole = jnp.sum(total[h], axis=1, keepdims=True)
                result = jnp.where(keep, summed[h] / whole, result)
        out_ref[:, g * lanes : (g + 1) * lanes] = result.astype(out_ref.dtype)


def attend_local(query_rows, kv_all, gates_all):
    rows, width = query_rows.shape
    groups, heads, _ = gates_all.shape
    lanes = min(width, 128)
    return pl.pallas_call(
        functools.partial(attend_kernel, heads),
        out_shape=jax.ShapeDtypeStruct((rows, width), jnp.bfloat16),
        in_specs=[pl.BlockSpec(memory_space=pltpu.VMEM)] * 3,
        out_specs=pl.BlockSpec(memory_space=pltpu.VMEM),
        scratch_shapes=[
            pltpu.VMEM((heads, rows, lanes), jnp.bfloat16),
            pltpu.VMEM((heads, rows, 128), jnp.float32),
            pltpu.VMEM((heads, rows, 128), jnp.float32),
            pltpu.VMEM((heads, rows, lanes), jnp.float32),
        ],
        compiler_params=pltpu.CompilerParams(vmem_limit_bytes=48 * 2**20),
        cost_estimate=pl.CostEstimate(
            flops=4 * rows * rows * groups * width * 4,
            bytes_accessed=4 * rows * groups * width,
            transcendentals=rows * rows * groups * heads,
        ),
    )(query_rows, kv_all, gates_all)


def half_of(core, tp):
    return (1 - core) * (tp // 2) + core * (tp % 2)


def partner_of(core, tp):
    return (1 - core) * ((tp + 2) % 4) + core * (tp + 1 - 2 * (tp % 2))


def layer_kernel(
    heads,
    groups,
    gates_ref,
    index_ref,
    route_ref,
    gain_ref,
    q_source,
    k_source,
    v_source,
    weight_source,
    residual_source,
    gate_ref,
    up_ref,
    down_ref,
    out_ref,
    q_ref,
    k_ref,
    v_ref,
    weight_ref,
    residual_ref,
    place_row_ref,
    facts,
    facts_col,
    gain_row,
    mixed_ref,
    kv_out,
    q_out,
    kv_all,
    q_all,
    gates_all,
    gate_pair,
    packed,
    heads_in,
    masked_q,
    top,
    total,
    summed,
    attended,
    outbox,
    full,
    act,
    made,
    returned,
    blended,
    gate_all,
    up_all,
    down_all,
    wide_rows,
    kv_send,
    side_send,
    kv_recv,
    q_send,
    q_recv,
    head_send,
    head_recv,
    tp_send,
    tp_recv,
    weight_send,
    weight_recv,
    load_sem,
    down_send,
    down_recv,
    out_send,
    out_recv,
    one_send,
    one_recv,
    two_send,
    two_recv,
    back_send,
    back_recv,
):
    rows, width = q_ref.shape
    head_size = width // heads
    lanes = min(width, 128)
    tile = math.gcd(rows, 256)
    tiles = rows // tile
    sp = lax.axis_index("sp")
    tp = lax.axis_index("tp")
    chip = sp // 2
    core = sp % 2
    chips = groups // 2
    sibling = sp + 1 - 2 * core
    beside = tp + 1 - 2 * (tp % 2)
    across = (tp + 2) % 4
    mesh_id = pl.DeviceIdType.MESH
    scale = head_size ** (-0.5)
    lead = (sp + chip) % 2

    def direct(which):
        return pltpu.make_async_remote_copy(
            src_ref=attended.at[tp],
            dst_ref=attended.at[tp],
            send_sem=tp_send.at[which],
            recv_sem=tp_recv.at[which],
            device_id=(sp, beside if which == 0 else across),
            device_id_type=mesh_id,
        )

    def relay(which):
        owner = beside if which == 0 else across
        part = attended.at[owner, pl.ds(which * (rows // 2), rows // 2)]
        return pltpu.make_async_remote_copy(
            src_ref=part,
            dst_ref=part,
            send_sem=tp_send.at[2 + which],
            recv_sem=tp_recv.at[2 + which],
            device_id=(sp, across if which == 0 else beside),
            device_id_type=mesh_id,
        )

    topk = route_ref.shape[0]
    half, columns = outbox.shape[2:]
    capacity = 2 * half
    shards = full.shape[1]
    mine = half_of(core, tp)
    pair = partner_of(core, tp)
    peer = partner_of(1 - core, tp)
    owners = (tp, pair, peer, (beside + 2) % 4)

    def partner(number):
        found, bit = 0, 1
        while bit < groups:
            found = found + bit * (((sp // bit) % 2 + (number // bit) % 2) % 2)
            bit *= 2
        return found

    def send(src, dst, send_sem, recv_sem, device):
        return pltpu.make_async_remote_copy(
            src_ref=src,
            dst_ref=dst,
            send_sem=send_sem,
            recv_sem=recv_sem,
            device_id=device,
            device_id_type=pl.DeviceIdType.MESH,
        )

    def spread(head):
        device = (2 * head + core, tp)
        return [
            send(src, dst.at[sp], kv_send.at[head, n], kv_recv.at[sp, n], device)
            for n, (src, dst) in enumerate(((kv_out.at[head], kv_all), (gates_ref, gates_all)))
        ]

    def sideways(number, own=False):
        return [
            send(src, dst.at[number], side_send.at[number, n], kv_recv.at[number, n], (sibling, tp))
            for n, (src, dst) in enumerate(
                (
                    (kv_all.at[number], kv_all),
                    (gates_ref if own else gates_all.at[number], gates_all),
                )
            )
        ]

    def ask(head):
        return send(
            q_out.at[head],
            q_all.at[chip],
            q_send.at[head],
            q_recv.at[chip],
            (2 * head + lead, tp),
        )

    def answer(slot):
        return send(
            packed.at[slot],
            heads_in.at[chip],
            head_send.at[slot],
            head_recv.at[chip],
            (2 * slot + (slot + core) % 2, tp),
        )

    def dispatch(i, which):
        group = partner(i)
        target = tp if which == 0 else partner_of(group % 2, tp)
        return send(
            outbox.at[i, which],
            full.at[i, which],
            out_send.at[i, which],
            out_recv.at[i, which],
            (group, target),
        )

    def exchange(i, held, send_sem, recv_sem):
        return send(
            held.at[i, pl.ds(0, 2)],
            held.at[i, pl.ds(2, 2)],
            send_sem.at[i],
            recv_sem.at[i],
            (sp, peer),
        )

    def give_back(i, which):
        target = tp if which == 0 else pair
        return send(
            made.at[i, which],
            returned.at[i, mine],
            back_send.at[i, which],
            back_recv.at[i, mine],
            (partner(i), target),
        )

    def arrive_back(i, which):
        return send(
            made.at[i, 0],
            returned.at[i, which],
            back_send.at[i, 0],
            back_recv.at[i, which],
            (sp, pair),
        )

    loads = []
    for n, (src, dst) in enumerate(
        (
            (q_source, q_ref),
            (k_source, k_ref),
            (v_source, v_ref),
            (weight_source, weight_ref),
            (residual_source, residual_ref),
            (gate_ref, gate_all.at[0]),
            (up_ref, up_all.at[0]),
            (down_ref, down_all.at[0]),
        )
    ):
        loads.append(pltpu.make_async_copy(src, dst, load_sem.at[n]))
    for load in loads:
        load.start()

    barrier = pltpu.get_barrier_semaphore()
    for i in range(1, groups):
        pl.semaphore_signal(
            barrier, inc=1, device_id=(partner(i), tp), device_id_type=pl.DeviceIdType.MESH
        )
        pl.semaphore_signal(
            barrier,
            inc=1,
            device_id=(partner(i), partner_of(partner(i) % 2, tp)),
            device_id_type=pl.DeviceIdType.MESH,
        )
        pl.semaphore_signal(
            barrier, inc=1, device_id=(partner(i), pair), device_id_type=pl.DeviceIdType.MESH
        )
    for other in (pair, peer):
        pl.semaphore_signal(
            barrier, inc=1, device_id=(sp, other), device_id_type=pl.DeviceIdType.MESH
        )
    pl.semaphore_wait(barrier, 3 * groups - 1)

    down_copy = send(down_ref, down_all.at[1], down_send, down_recv, (sp, pair))
    pieces = weight_send.shape[0]
    depth = gate_ref.shape[0] // pieces

    def weight_copies(number):
        part = pl.ds(pl.multiple_of(number * depth, depth), depth)
        return [
            send(
                src.at[part],
                dst.at[1, part],
                weight_send.at[number, n],
                weight_recv.at[number, n],
                (sp, pair),
            )
            for n, (src, dst) in enumerate(((gate_ref, gate_all), (up_ref, up_all)))
        ]

    def push(number):
        for copy in weight_copies(number):
            copy.start()

    early = pieces - 1 - chips
    for number in range(early):
        push(number)

    for load in loads[:3]:
        load.wait()
    lane = lax.broadcasted_iota(jnp.int32, (rows, lanes), 1)
    low = lane < head_size
    short = rows // 2
    short_low = low[:short]

    def turned(wide):
        return pltpu.roll(wide, head_size, 1)

    for g in range(width // lanes):
        part = slice(g * lanes, (g + 1) * lanes)
        wide = q_ref[:, part].astype(jnp.float32) * scale
        tail = turned(wide[short:])
        q_out[2 * g] = jnp.where(short_low, wide[:short], tail).astype(jnp.bfloat16)
        q_out[2 * g + 1] = jnp.where(short_low, tail, wide[:short]).astype(jnp.bfloat16)
    for s in range(1, chips):
        ask(partner(2 * s) // 2).start()

    @pl.when(lead != core)
    def _():
        ask(chip).start()

    @pl.when(lead == core)
    def _():
        q_all[chip] = q_out[chip]

    for g in range(width // lanes):
        part = slice(g * lanes, (g + 1) * lanes)
        keys = k_ref[:, part].astype(jnp.float32)
        values = turned(v_ref[:, part].astype(jnp.float32))
        kv_out[2 * g] = jnp.where(low, keys, values).astype(jnp.bfloat16)
        kv_out[2 * g + 1] = jnp.where(low, values, keys).astype(jnp.bfloat16)
    for s in range(1, chips):
        for copy in spread(partner(2 * s) // 2):
            copy.start()
    kv_all[sp] = kv_out[chip]
    gates_all[sp] = gates_ref[...]
    for copy in sideways(sp, True):
        copy.start()

    first = lax.broadcasted_iota(jnp.int32, (rows, rows), 0)
    second = lax.broadcasted_iota(jnp.int32, (rows, rows), 1)
    number = lax.broadcasted_iota(jnp.int32, (128, rows), 0)
    chosen = [index_ref[k : k + 1, :] ^ sp for k in range(topk)]
    named = jnp.zeros((128, rows), jnp.float32)
    for k in range(topk):
        named = named + jnp.where(number == chosen[k], 1.0, 0.0)
    before = jnp.dot(
        named.astype(jnp.bfloat16),
        jnp.where(first < second, 1.0, 0.0).astype(jnp.bfloat16),
        preferred_element_type=jnp.float32,
    )
    facts[...] = jnp.zeros(facts.shape, jnp.float32)
    for k in range(topk):
        rank = jnp.sum(jnp.where(number == chosen[k], before, 0.0), axis=0, keepdims=True)
        place_row_ref[k : k + 1, :] = chosen[k] * capacity + rank.astype(jnp.int32)
        facts[k : k + 1, :] = (chosen[k] * capacity).astype(jnp.float32) + rank
        facts[topk + k : topk + k + 1, :] = route_ref[k : k + 1, :]
    facts_col[...] = jnp.transpose(facts[...])
    gain_row[...] = gain_ref[...].astype(jnp.float32).reshape(1, -1)

    odd = chip % 2
    key_lane = (lane // head_size) == odd
    short_key = key_lane[:short]
    top[...] = jnp.full(top.shape, -1e30, jnp.float32)
    total[...] = jnp.zeros(total.shape, jnp.float32)
    summed[...] = jnp.zeros(summed.shape, jnp.float32)
    for n in range(chips):

        @pl.when((n != chip) | (lead != core))
        def _():
            send(
                q_out.at[0], q_all.at[n], q_send.at[0], q_recv.at[n], (sibling, tp)
            ).wait_recv()

        part = q_all[n].astype(jnp.float32)
        masked_q[n, :short] = jnp.where(short_key, part, 0.0).astype(jnp.bfloat16)
        masked_q[n, short:] = jnp.where(short_key, turned(part), 0.0).astype(jnp.bfloat16)

    def block(slot, number, offset):
        span_keys = 2 * rows
        for t in range(tiles):
            span = slice(t * tile, (t + 1) * tile)
            count = span_keys if offset is None else offset + (t + 1) * tile
            pair_kv = kv_all[pl.ds(2 * number, 2)].reshape(span_keys, lanes)[:count]
            scores = lax.dot_general(
                masked_q[slot, span],
                pair_kv,
                (((1,), (1,)), ((), ())),
                preferred_element_type=jnp.float32,
            )
            scores = scores - gate_pair[0:1, :count]
            if offset is not None:
                row = lax.broadcasted_iota(jnp.int32, (tile, count), 0) + t * tile + offset
                col = lax.broadcasted_iota(jnp.int32, (tile, count), 1)
                scores = jnp.where(col <= row, scores, -jnp.inf)
            old = top[slot, span]
            new = jnp.maximum(old, jnp.max(scores, axis=1, keepdims=True))
            raised = jnp.exp(scores - new[:, :1])
            shrink = jnp.exp(old - new)
            part = raised[:, :128]
            for c in range(128, count, 128):
                part = part + raised[:, c : c + 128]
            top[slot, span] = new
            total[slot, span] = total[slot, span] * shrink + part
            product = lax.dot_general(
                raised.astype(jnp.bfloat16),
                pair_kv,
                (((1,), (0,)), ((), ())),
                preferred_element_type=jnp.float32,
            )
            summed[slot, span] = summed[slot, span] * shrink[:, :lanes] + product

    def chip_step(s, carry):
        number = partner(2 * s) // 2
        near = 2 * number + core
        push(early + s)

        @pl.when(s > 0)
        def _():
            for copy in sideways(near):
                copy.wait_recv()
            for copy in sideways(near):
                copy.start()

        for copy in sideways(2 * number + 1 - core):
            copy.wait_recv()
        gate_pair[0:1, :rows] = gates_all[2 * number, pl.ds(chip, 1), :]
        gate_pair[0:1, rows:] = gates_all[2 * number + 1, pl.ds(chip, 1), :]

        @pl.when((number + core) % 2 == 0)
        def _():
            block(number, number, 0)

        @pl.when((number + core) % 2 == 1)
        def _():
            block(number, number, rows)

        def full_step(slot, inner):
            block(slot, number, None)
            return inner

        lax.fori_loop(number + 1, chips, full_step, 0)
        return carry

    lax.fori_loop(0, chips, chip_step, 0)

    for n in range(chips):
        result = summed[n] / jnp.sum(total[n], axis=1, keepdims=True)
        folded = jnp.where(short_key, turned(result[short:]), result[:short])
        packed[n] = folded.astype(jnp.bfloat16)

        @pl.when((n != chip) | (lead != core))
        def _():
            answer(n).start()

        @pl.when((n == chip) & (lead == core))
        def _():
            heads_in[chip] = packed[n]

    for n in range(chips):

        @pl.when((n != chip) | (lead != core))
        def _():
            send(
                packed.at[0], heads_in.at[n], head_send.at[0], head_recv.at[n], (sibling, tp)
            ).wait_recv()

    for g in range(width // lanes):
        even = heads_in[2 * g].astype(jnp.float32)
        uneven = heads_in[2 * g + 1].astype(jnp.float32)
        part = slice(g * lanes, (g + 1) * lanes)
        attended[tp, :short, part] = jnp.where(short_low, turned(even), turned(uneven)).astype(
            jnp.bfloat16
        )
        attended[tp, short:, part] = jnp.where(short_low, even, uneven).astype(jnp.bfloat16)
    direct(0).start()
    direct(1).start()

    def projected(owner):
        return jnp.dot(
            attended[owner],
            weight_ref[pl.ds(pl.multiple_of(owner * width, width), width), :],
            preferred_element_type=jnp.float32,
        )

    for load in loads[3:5]:
        load.wait()
    mixed = residual_ref[...].astype(jnp.float32) + projected(tp)
    for which, owner in ((0, beside), (1, across)):
        direct(which).wait_recv()
        relay(which).start()
        mixed = mixed + projected(owner)
    for number in range(early + chips, pieces):
        push(number)
    down_copy.start()
    relay(0).wait_recv()
    relay(1).wait_recv()
    mixed_ref[...] = (mixed + projected((beside + 2) % 4)).astype(mixed_ref.dtype)

    def rows_for(i):
        flip = half_of(partner(i) % 2, tp)
        place = lax.broadcasted_iota(jnp.int32, (capacity, rows), 0) + flip * half
        numbers = jnp.where(place >= capacity, place - capacity, place) + i * capacity
        taken = numbers == place_row_ref[0:1, :]
        for k in range(1, topk):
            taken = taken | (numbers == place_row_ref[k : k + 1, :])
        return jnp.dot(
            jnp.where(taken, 1.0, 0.0).astype(jnp.bfloat16),
            mixed_ref[...],
            preferred_element_type=jnp.float32,
        ).astype(jnp.bfloat16)

    def fill(i, carry):
        made_rows = rows_for(i)
        outbox[i, 0] = made_rows[:half]
        outbox[i, 1] = made_rows[half:]
        dispatch(i, 0).start()
        dispatch(i, 1).start()
        return carry

    def label(n):
        return 2 * (lax.shift_right_logical(30, 2 * (n // 2)) % chips) + n % 2

    def fill_next(n, carry):
        return fill(label(n), carry)

    lax.fori_loop(0, groups - 2, fill_next, 0)
    lax.fori_loop(1, 2, fill, 0)
    first = rows_for(0)
    full[0, 0] = first[:half]
    outbox[0, 1] = first[half:]
    dispatch(0, 1).start()
    blended[...] = mixed_ref[...].astype(jnp.float32)

    def hidden(i):
        square = jnp.zeros((half, 1), jnp.float32)
        for j in range(shards):
            wide = full[i, j].astype(jnp.float32)
            square = square + jnp.sum(wide * wide, axis=1, keepdims=True)
        factor = lax.rsqrt(square / (shards * columns) + NORM_EPS)
        for j in range(shards):
            span = pl.ds(pl.multiple_of(owners[j] * columns, columns), columns)
            gain = gain_row[0:1, span]
            wide_rows[:, span] = (full[i, j].astype(jnp.float32) * factor * gain).astype(
                jnp.bfloat16
            )
        for c in range(2):
            gate_input = jnp.dot(
                wide_rows[...], gate_all[c], preferred_element_type=jnp.float32
            )
            linear_input = jnp.dot(wide_rows[...], up_all[c], preferred_element_type=jnp.float32)
            gate_cut = jnp.minimum(gate_input, CLAMP_LIMIT)
            linear_cut = jnp.clip(linear_input, -CLAMP_LIMIT, CLAMP_LIMIT)
            act[i, c] = (
                gate_cut * jax.nn.sigmoid(SILU_ALPHA * gate_cut) * (linear_cut + 1.0)
            ).astype(jnp.bfloat16)

    def output_rows(i, c):
        return jnp.dot(
            wide_rows[...], down_all[c], preferred_element_type=jnp.float32
        ).astype(jnp.bfloat16)

    def step(i, carry):
        @pl.when(i < groups)
        def _():
            b = label(i)

            @pl.when(b > 0)
            def _():
                dispatch(b, 0).wait_recv()

            dispatch(b, 1).wait_recv()
            exchange(b, full, one_send, one_recv).start()

        @pl.when((i >= 2) & (i < groups + 2))
        def _():
            b = label(i - 2)

            @pl.when(i == 2)
            def _():
                for load in loads[5:]:
                    load.wait()
                for number in range(pieces):
                    for copy in weight_copies(number):
                        copy.wait_recv()

            exchange(b, full, one_send, one_recv).wait_recv()
            hidden(b)
            exchange(b, act, two_send, two_recv).start()

        @pl.when((i >= 4) & (i < groups + 4))
        def _():
            b = label(i - 4)

            @pl.when(i == 4)
            def _():
                down_copy.wait_recv()

            exchange(b, act, two_send, two_recv).wait_recv()
            for j in range(shards):
                span = pl.ds(pl.multiple_of(owners[j] * columns, columns), columns)
                wide_rows[:, span] = act[b, j]
            made[b, 1] = output_rows(b, 1)
            give_back(b, 1).start()
            result = output_rows(b, 0)

            @pl.when(b == 0)
            def _():
                returned[0, mine] = result

            @pl.when(b > 0)
            def _():
                made[b, 0] = result
                give_back(b, 0).start()

        @pl.when(i >= 7)
        def _():
            b = label(i - 7)

            @pl.when(b == 0)
            def _():
                arrive_back(0, 1 - mine).wait_recv()

            @pl.when(b > 0)
            def _():
                arrive_back(b, 0).wait_recv()
                arrive_back(b, 1).wait_recv()

            numbers = lax.broadcasted_iota(jnp.int32, (rows, capacity), 1) + b * capacity
            wide_numbers = numbers.astype(jnp.float32)
            added = blended[...]
            rows_back = returned[b].reshape(capacity, columns)
            for k in range(topk):
                taken = jnp.where(wide_numbers == facts_col[:, k : k + 1], 1.0, 0.0)
                picked = jnp.dot(
                    taken.astype(jnp.bfloat16), rows_back, preferred_element_type=jnp.float32
                )
                added = added + facts_col[:, topk + k : topk + k + 1] * picked
            blended[...] = added

        return carry

    lax.fori_loop(0, groups + 7, step, 0)
    out_ref[...] = blended[...].astype(out_ref.dtype)

    def settle(i, carry):
        @pl.when(i > 0)
        def _():
            dispatch(i, 0).wait_send()
            give_back(i, 0).wait_send()

        dispatch(i, 1).wait_send()
        give_back(i, 1).wait_send()
        exchange(i, full, one_send, one_recv).wait_send()
        exchange(i, act, two_send, two_recv).wait_send()
        return carry

    lax.fori_loop(0, groups, settle, 0)
    down_copy.wait_send()

    for which in range(2):
        direct(which).wait_send()
        relay(which).wait_send()

    for s in range(1, chips):
        ask(partner(2 * s) // 2).wait_send()
        for copy in spread(partner(2 * s) // 2):
            copy.wait_send()
        for copy in sideways(2 * (partner(2 * s) // 2) + core):
            copy.wait_send()
    for copy in sideways(sp, True):
        copy.wait_send()

    @pl.when(lead != core)
    def _():
        ask(chip).wait_send()

    for n in range(chips):

        @pl.when((n != chip) | (lead != core))
        def _():
            answer(n).wait_send()

    for number in range(pieces):
        for copy in weight_copies(number):
            copy.wait_send()


def layer_fused(
    query_rows,
    key_rows,
    value_rows,
    gates,
    output_weight,
    residual,
    index,
    route_weights,
    norm_gain,
    gate_weight,
    up_weight,
    down_weight,
    capacity,
):
    rows, width = query_rows.shape
    columns = residual.shape[1]
    heads = gates.shape[0]
    groups = lax.axis_size("sp")
    shards = lax.axis_size("tp")
    lanes = min(width, 128)
    depth, units = gate_weight.shape
    half = capacity // 2
    dma = pltpu.SemaphoreType.DMA
    return pl.pallas_call(
        functools.partial(layer_kernel, heads, groups),
        out_shape=jax.ShapeDtypeStruct(residual.shape, jnp.bfloat16),
        in_specs=[pl.BlockSpec(memory_space=pltpu.VMEM)] * 4
        + [pl.BlockSpec(memory_space=pl.ANY)] * 8,
        out_specs=pl.BlockSpec(memory_space=pltpu.VMEM),
        scratch_shapes=[
            pltpu.VMEM((rows, width), jnp.bfloat16),
            pltpu.VMEM((rows, width), jnp.bfloat16),
            pltpu.VMEM((rows, width), jnp.bfloat16),
            pltpu.VMEM(output_weight.shape, jnp.bfloat16),
            pltpu.VMEM(residual.shape, jnp.bfloat16),
            pltpu.VMEM(index.shape, jnp.int32),
            pltpu.VMEM((8, rows), jnp.float32),
            pltpu.VMEM((rows, 8), jnp.float32),
            pltpu.VMEM((1, shards * columns), jnp.float32),
            pltpu.VMEM((rows, columns), jnp.bfloat16),
            pltpu.VMEM((heads, rows, lanes), jnp.bfloat16),
            pltpu.VMEM((heads, rows // 2, lanes), jnp.bfloat16),
            pltpu.VMEM((groups, rows, lanes), jnp.bfloat16),
            pltpu.VMEM((heads, rows // 2, lanes), jnp.bfloat16),
            pltpu.VMEM((groups, heads, rows), jnp.float32),
            pltpu.VMEM((8, 2 * rows), jnp.float32),
            pltpu.VMEM((heads, rows // 2, lanes), jnp.bfloat16),
            pltpu.VMEM((heads, rows // 2, lanes), jnp.bfloat16),
            pltpu.VMEM((heads, rows, lanes), jnp.bfloat16),
            pltpu.VMEM((heads, rows, 128), jnp.float32),
            pltpu.VMEM((heads, rows, 128), jnp.float32),
            pltpu.VMEM((heads, rows, lanes), jnp.float32),
            pltpu.VMEM((4, rows, width), jnp.bfloat16),
            pltpu.VMEM((groups, 2, half, columns), jnp.bfloat16),
            pltpu.VMEM((groups, shards, half, columns), jnp.bfloat16),
            pltpu.VMEM((groups, shards, half, units), jnp.bfloat16),
            pltpu.VMEM((groups, 2, half, columns), jnp.bfloat16),
            pltpu.VMEM((groups, 2, half, columns), jnp.bfloat16),
            pltpu.VMEM((rows, columns), jnp.float32),
            pltpu.VMEM((2, depth, units), jnp.bfloat16),
            pltpu.VMEM((2, depth, units), jnp.bfloat16),
            pltpu.VMEM((2, shards * units, columns), jnp.bfloat16),
            pltpu.VMEM((half, shards * columns), jnp.bfloat16),
            dma((heads, 2)),
            dma((groups, 2)),
            dma((groups, 2)),
            dma((heads,)),
            dma((heads,)),
            dma((heads,)),
            dma((heads,)),
            dma((4,)),
            dma((4,)),
            dma((8, 2)),
            dma((8, 2)),
            dma((8,)),
            dma(()),
            dma(()),
            dma((groups, 2)),
            dma((groups, 2)),
            dma((groups,)),
            dma((groups,)),
            dma((groups,)),
            dma((groups,)),
            dma((groups, 2)),
            dma((groups, 2)),
        ],
        compiler_params=pltpu.CompilerParams(
            collective_id=1, has_side_effects=True, vmem_limit_bytes=67043328
        ),
    )(
        gates,
        index,
        route_weights,
        norm_gain,
        query_rows,
        key_rows,
        value_rows,
        output_weight,
        residual,
        gate_weight,
        up_weight,
        down_weight,
    )


def body(
    query_rows,
    key_rows,
    value_rows,
    cum_gates,
    residual,
    output_weight,
    norm_gain,
    expert_index,
    route_weights,
    gate_weight,
    up_weight,
    down_weight,
):
    rows, columns = residual.shape
    topk = expert_index.shape[1]
    local_experts = gate_weight.shape[0]
    groups = lax.axis_size("sp")
    experts = local_experts * groups
    capacity = 2 * rows * topk // experts
    heads = cum_gates.shape[1]

    if (
        lax.axis_size("tp") == 4
        and local_experts == 1
        and groups == 8
        and heads == 4
        and query_rows.shape[1] == heads * 64
    ):
        return layer_fused(
            query_rows,
            key_rows,
            value_rows,
            cum_gates.T,
            output_weight,
            residual,
            expert_index.T,
            route_weights.T,
            norm_gain,
            gate_weight[0],
            up_weight[0],
            down_weight[0],
            capacity,
        )

    both = jnp.concatenate([key_rows, value_rows], axis=1)
    kv_all = lax.all_gather(both, "sp", axis=0, tiled=True)
    gates_all = lax.all_gather(cum_gates.T, "sp", axis=0, tiled=False)

    chosen = expert_index.reshape(rows * topk)
    matches = (chosen[:, None] == jnp.arange(experts, dtype=jnp.int32)[None, :]).astype(jnp.int32)
    rank = jnp.sum((jnp.cumsum(matches, axis=0) - matches) * matches, axis=1)
    chosen, rank, gates_all = lax.optimization_barrier((chosen, rank, gates_all))

    attended = attend_local(query_rows, kv_all, gates_all)
    projected = jnp.dot(
        lax.all_gather(attended, "tp", axis=1, tiled=True),
        output_weight,
        preferred_element_type=jnp.float32,
    )
    mixed = (residual.astype(jnp.float32) + projected).astype(jnp.bfloat16)

    chunks = math.gcd(capacity, CHUNKS)
    piece = capacity // chunks
    places = chosen * piece + rank % piece
    inside = rank // piece
    blended = jnp.zeros((rows, columns), jnp.float32)
    for c in range(chunks):
        place = jnp.where(inside == c, places, -1).reshape(rows, topk)
        numbers = jnp.arange(experts * piece, dtype=jnp.int32)
        taken = numbers[:, None] == place[:, 0][None, :]
        for k in range(1, topk):
            taken = taken | (numbers[:, None] == place[:, k][None, :])
        outgoing = jnp.dot(
            taken.astype(jnp.bfloat16), mixed, preferred_element_type=jnp.float32
        ).astype(jnp.bfloat16)
        arrived = lax.all_to_all(
            outgoing.reshape(experts, piece, columns), "sp", split_axis=0, concat_axis=0, tiled=True
        )
        grouped = arrived.reshape(groups, local_experts, piece, columns)
        normed = normalize(lax.all_gather(grouped, "tp", axis=3, tiled=True), norm_gain)
        gate_input = jnp.einsum(
            "seid,edf->seif", normed, gate_weight, preferred_element_type=jnp.float32
        )
        linear_input = jnp.einsum(
            "seid,edf->seif", normed, up_weight, preferred_element_type=jnp.float32
        )
        gate_cut = jnp.minimum(gate_input, CLAMP_LIMIT)
        linear_cut = jnp.clip(linear_input, -CLAMP_LIMIT, CLAMP_LIMIT)
        activated = (gate_cut * jax.nn.sigmoid(SILU_ALPHA * gate_cut) * (linear_cut + 1.0)).astype(
            jnp.bfloat16
        )
        produced = jnp.einsum(
            "seif,efc->seic",
            lax.all_gather(activated, "tp", axis=3, tiled=True),
            down_weight,
            preferred_element_type=jnp.float32,
        ).astype(jnp.bfloat16)
        returned = lax.all_to_all(
            produced.reshape(experts, piece, columns), "sp", split_axis=0, concat_axis=0, tiled=True
        ).reshape(experts * piece, columns)
        for k in range(topk):
            picked = jnp.dot(
                (place[:, k][:, None] == numbers[None, :]).astype(jnp.bfloat16),
                returned,
                preferred_element_type=jnp.float32,
            )
            blended = blended + route_weights[:, k : k + 1] * picked
    return (mixed.astype(jnp.float32) + blended).astype(jnp.bfloat16)


def solution(mesh):
    placed = (
        P("sp", "tp"),
        P("sp", "tp"),
        P("sp", "tp"),
        P("sp", "tp"),
        P("sp", "tp"),
        P(None, "tp"),
        P(),
        P("sp", None),
        P("sp", None),
        P("sp", None, "tp"),
        P("sp", None, "tp"),
        P("sp", None, "tp"),
    )
    return jax.shard_map(body, mesh=mesh, in_specs=placed, out_specs=P("sp", "tp"), check_vma=False)
```
